32 devices in a mesh: grp: 2 (over y), fs: 4 (over z), tp: 4 (over x, core).
Axes of the slice: x: 2, y: 2, z: 4, core: 2. Of those that a mesh axis runs over, the one named last changes fastest.
Arguments:
- tokens: bfloat16 [8, 384, 2048], P(('grp', 'fs'), None, 'tp'), parts along dimension 0, may hold values from -24 to 24
- input_gain: float32 [2048], replicated, may hold values from 0.1 to 1.9
- query_weight: bfloat16 [2048, 1024], P('fs', 'tp'), may hold values from -0.125 to 0.125
- key_weight: bfloat16 [2048, 1024], P('fs', 'tp'), may hold values from -0.125 to 0.125
- value_weight: bfloat16 [2048, 1024], P('fs', 'tp'), may hold values from -0.125 to 0.125
- output_gate_matrix: bfloat16 [2048, 1024], P('fs', 'tp'), may hold values from -0.125 to 0.125
- forward_decay: float32 [16], P('tp'), may hold values from -1 to 9
- backward_decay: float32 [16], P('tp'), may hold values from -1 to 9
- merge_weight: bfloat16 [1024, 2048], P('tp', 'fs'), may hold values from -0.375 to 0.375
- middle_gain: float32 [2048], replicated, may hold values from 0.1 to 1.9
- gate_weight: bfloat16 [2048, 5120], P('fs', 'tp'), may hold values from -0.125 to 0.125
- up_weight: bfloat16 [2048, 5120], P('fs', 'tp'), may hold values from -0.125 to 0.125
- down_weight: bfloat16 [5120, 2048], P('tp', 'fs'), may hold values from -0.15625 to 0.15625
Outputs:
- layer_out: bfloat16 [8, 384, 2048], P(('grp', 'fs'), None, 'tp'), parts along dimension 0
The draws below stay inside these ranges and needn't reach their ends.
There are 2 independent parts, one for each index of `grp`. The reference program is written for one: setup_inputs(seed, part) draws one part's arguments, and reference() takes and returns one part's arrays. A program takes and returns all parts, laid end to end along the dimension named above; an argument that names none is the same for every part. Nothing has to cross between parts.
All inputs are finite; a program needn't handle non-finite values.
Results may differ from the reference program's by a relative error of at most 0.019.
Values may be sent and summed in bfloat16 or wider, within the bound.
A program may use at most 64 MiB of HBM per device.

```python
import math
import jax
import jax.numpy as jnp
from jax import lax

D = 2048
HEADS = 16
FF = 5120
BLOCK = 128
LEN = 384
RET_W = 1024
SEQS = 4
N_TP = 4


def draw_tokens(key, part):
    subkeys = jax.random.split(jax.random.fold_in(key, 11), 3)
    full_shape = (SEQS, LEN, D)
    row_scale = jnp.exp(jax.random.uniform(subkeys[1], (SEQS, LEN, 1), jnp.float32, math.log(0.3), math.log(3.0)))
    column_scale = jnp.exp(jax.random.uniform(subkeys[2], (1, 1, D), jnp.float32, math.log(0.5), math.log(2.0)))
    base_values = jnp.clip(jax.random.normal(subkeys[0], full_shape, jnp.float32), -4.0, 4.0)
    return (base_values * row_scale * column_scale).astype(jnp.bfloat16)


def decay_logits(key, salt):
    subkeys = jax.random.split(jax.random.fold_in(key, salt), 3)
    slow_share = 0.5
    slow_low = 0.7
    slow_high = 2.3
    is_slow = jax.random.bernoulli(subkeys[0], slow_share, (HEADS,))
    slow_rate = -jax.random.uniform(subkeys[1], (HEADS,), jnp.float32, slow_low, slow_high) / LEN
    fast_rate = -jax.random.uniform(subkeys[2], (HEADS,), jnp.float32, 7.5, 15.0) / BLOCK
    log_rates = jnp.where(is_slow, slow_rate, fast_rate)
    return log_rates - jnp.log(-jnp.expm1(log_rates))


def draw_forward_decay(key, part):
    return decay_logits(key, 21)


def draw_backward_decay(key, part):
    return decay_logits(key, 22)


def levels(stream_key, dims, pieces, smallest, largest):
    gain, own = 1.0, jax.random.fold_in(stream_key, 6)
    for dim, blocks in pieces:
        draws = jnp.exp(jax.random.uniform(jax.random.fold_in(own, dim), (blocks,), jnp.float32, smallest / len(pieces), largest / len(pieces)))
        gain = gain * jnp.repeat(draws, dims[dim] // blocks).reshape([-1 if axis == dim else 1 for axis in range(len(dims))])
    return gain


def scatter_about(stream_key, shape, scale, bound, cuts=(), kind=jnp.bfloat16):
    level = levels(stream_key, shape, cuts, -0.22, 0.18) if cuts else 1.0
    values = jax.random.normal(stream_key, shape, jnp.float32) * scale * level
    return jnp.minimum(jnp.maximum(values, -bound), bound).astype(kind)


def setup_inputs(seed: int = 0, part: int = 0) -> dict:
    arg_keys = jax.random.split(jax.random.key(seed), 14)
    part_splits = jax.random.split(jax.random.fold_in(arg_keys[13], part), 14)
    return {
        "tokens": draw_tokens(jax.random.fold_in(jax.random.fold_in(arg_keys[13], part), 71), part),
        "input_gain": jnp.clip(1.0 + 0.18 * jax.random.normal(arg_keys[1], (D,), jnp.float32), 0.1, 1.9),
        "query_weight": scatter_about(arg_keys[2], (D, RET_W), D ** -0.5, 0.125, ((0, 4), (1, 4))),
        "key_weight": scatter_about(arg_keys[3], (D, RET_W), D ** -0.5, 0.125, ((0, 4), (1, 4))),
        "value_weight": scatter_about(arg_keys[4], (D, RET_W), D ** -0.5, 0.125, ((0, 4), (1, 4))),
        "output_gate_matrix": scatter_about(arg_keys[5], (D, RET_W), D ** -0.5, 0.125, ((0, 4), (1, 4))),
        "forward_decay": draw_forward_decay(jax.random.fold_in(arg_keys[13], 71), part),
        "backward_decay": draw_backward_decay(jax.random.fold_in(arg_keys[13], 71), part),
        "merge_weight": scatter_about(arg_keys[8], (RET_W, D), (RET_W // 4) ** -0.5, 0.375, ((0, 4), (1, 4))),
        "middle_gain": jnp.clip(1.0 + 0.18 * jax.random.normal(arg_keys[9], (D,), jnp.float32), 0.1, 1.9),
        "gate_weight": scatter_about(arg_keys[10], (D, FF), D ** -0.5, 0.125, ((0, 4), (1, 4))),
        "up_weight": scatter_about(arg_keys[11], (D, FF), D ** -0.5, 0.125, ((0, 4), (1, 4))),
        "down_weight": scatter_about(arg_keys[12], (FF, D), (FF // 4) ** -0.5, 0.15625, ((0, 4), (1, 4))),
    }


norm_eps = 1e-06
group_eps = 1e-05
rope_base = 10000.0
highest_precision = lax.Precision.HIGHEST

def rms_scale(values, gain_vector):
    widened = values.astype(jnp.float32)
    scaled = widened * lax.rsqrt(lax.optimization_barrier(jnp.mean(widened * widened, axis=-1, keepdims=True)) + norm_eps)
    return (scaled * gain_vector.astype(jnp.float32)).astype(jnp.bfloat16)

def apply_rotary_heads(values, length):
    half_dim = values.shape[-1] // 2
    inverse = rope_base ** (-jnp.arange(half_dim, dtype=jnp.float32) / half_dim)
    angles = jnp.arange(length, dtype=jnp.float32)[:, None] * inverse[None, :]
    cosine = jnp.cos(angles)[:, None, :]
    sine_part = jnp.sin(angles)[:, None, :]
    lower_half = values[..., :half_dim]
    upper_half = values[..., half_dim:]
    return jnp.concatenate([lower_half * cosine - upper_half * sine_part, upper_half * cosine + lower_half * sine_part], axis=-1)

def retain_dense(query_rows, key_rows, value_rows, gate_rows, forward_decay, backward_decay, seq_count, length):
    head_count = forward_decay.shape[0]
    head_dim = query_rows.shape[1] // head_count

    def split_heads(rows_in):
        return rows_in.astype(jnp.float32).reshape(seq_count, length, head_count, head_dim)
    queries = apply_rotary_heads(split_heads(query_rows), length)
    key_heads = apply_rotary_heads(split_heads(key_rows), length) * head_dim ** (-0.5)
    valued = split_heads(value_rows)
    rate_ahead = jax.nn.log_sigmoid(forward_decay.astype(jnp.float32))
    rate_behind = jax.nn.log_sigmoid(backward_decay.astype(jnp.float32))
    position = jnp.arange(length, dtype=jnp.float32)
    offset = position[:, None] - position[None, :]
    weight_tree = jnp.where(offset[None] >= 0, jnp.exp(rate_ahead[:, None, None] * jnp.maximum(offset, 0.0)[None]), jnp.exp(rate_behind[:, None, None] * jnp.maximum(-offset, 0.0)[None]))

    def one_sequence(operands):
        sequence_query, sequence_key, sequence_value = operands
        attention_scores = jnp.einsum('pze,rze->zpr', sequence_query, sequence_key, precision=highest_precision) * weight_tree
        return jnp.einsum('kaf,fkg->akg', attention_scores, sequence_value, precision=highest_precision)
    result = lax.map(one_sequence, (queries, key_heads, valued))
    center = lax.optimization_barrier(jnp.mean(result, axis=-1, keepdims=True))
    spread = lax.optimization_barrier(jnp.mean(jnp.square(result - center), axis=-1, keepdims=True))
    normalized = (result - center) * lax.rsqrt(spread + group_eps)
    gated = jax.nn.silu(split_heads(gate_rows)) * normalized
    return gated.reshape(seq_count * length, head_count * head_dim).astype(jnp.bfloat16)

def split_sum(left_rows, right_rows):
    group_size = left_rows.shape[1] // N_TP
    total = jnp.zeros((left_rows.shape[0], right_rows.shape[1]), jnp.float32)
    for index in range(N_TP):
        lower = index * group_size
        partial_term = jnp.dot(left_rows[:, lower:lower + group_size], right_rows[lower:lower + group_size], preferred_element_type=jnp.float32).astype(jnp.bfloat16)
        total = total + lax.optimization_barrier(partial_term).astype(jnp.float32)
    return total

def reference(tokens, input_gain, query_weight, key_weight, value_weight, output_gate_matrix, forward_decay, backward_decay, merge_weight, middle_gain, gate_weight, up_weight, down_weight):
    seq_count, length, width = tokens.shape
    row_count = seq_count * length
    flat = tokens.reshape(row_count, width)
    normed = rms_scale(flat, input_gain)
    query_rows = jnp.dot(normed, query_weight, preferred_element_type=jnp.float32).astype(jnp.bfloat16)
    key_rows = jnp.dot(normed, key_weight, preferred_element_type=jnp.float32).astype(jnp.bfloat16)
    value_rows = jnp.dot(normed, value_weight, preferred_element_type=jnp.float32).astype(jnp.bfloat16)
    gate_rows = jnp.dot(normed, output_gate_matrix, preferred_element_type=jnp.float32).astype(jnp.bfloat16)
    mixed = retain_dense(query_rows, key_rows, value_rows, gate_rows, forward_decay, backward_decay, seq_count, length)
    middle = (flat.astype(jnp.float32) + split_sum(mixed, merge_weight)).astype(jnp.bfloat16)
    normed_mid = rms_scale(middle, middle_gain)
    gate_act = jnp.dot(normed_mid, gate_weight, preferred_element_type=jnp.float32)
    up_act = jnp.dot(normed_mid, up_weight, preferred_element_type=jnp.float32)
    hidden = (jax.nn.silu(gate_act) * up_act).astype(jnp.bfloat16)
    layer_out = (middle.astype(jnp.float32) + split_sum(hidden, down_weight)).astype(jnp.bfloat16)
    return layer_out.reshape(seq_count, length, width)
```

```python
import functools

import jax
import jax.numpy as jnp
import numpy as np
from jax import lax
from jax.experimental import pallas as pl
from jax.experimental.pallas import tpu as pltpu
from jax.sharding import PartitionSpec as P

norm_eps = 1e-06
group_eps = 1e-05
rope_base = 10000.0


def turn_tables(length, head_dim, head_count):
    half_dim = head_dim // 2
    inverse = rope_base ** (-np.arange(half_dim) / half_dim)
    angles = np.arange(length)[:, None] * inverse[None, :]
    cosine, sine_part = np.cos(angles), np.sin(angles)
    return (
        np.tile(np.concatenate([cosine, cosine], axis=1), (1, head_count)).astype(np.float32),
        np.tile(np.concatenate([-sine_part, sine_part], axis=1), (1, head_count)).astype(np.float32),
    )


MESH = pl.DeviceIdType.MESH


def layer_kernel(
    sizes,
    tokens,
    input_gain,
    middle_gain,
    rate_ahead,
    rate_behind,
    cosine,
    sine_part,
    joined_shard,
    merge_shard,
    gate_shard,
    up_shard,
    down_shard,
    out,
    joined,
    merge,
    gate,
    up,
    *rest,
):
    line, copies, row = sizes["fs"], sizes["grp"], sizes["tp"]
    parts = len(rest) - 18
    downs, partial_ends, received_ends = rest[:parts], rest[-2], rest[-1]
    (
        gathered,
        gathered_mid,
        normed,
        projected,
        mixed,
        hidden,
        partial,
        received,
        own_sem,
        line_send,
        line_recv,
        pair_send,
        pair_recv,
        row_send,
        row_recv,
        self_sem,
    ) = rest[parts:-2]
    piece_width = downs[0].shape[2]
    shards = (joined_shard, merge_shard, gate_shard, up_shard) + tuple(
        down_shard if parts == 1 else down_shard.at[:, pl.ds(i * piece_width, piece_width)]
        for i in range(parts)
    )
    slots = (joined, merge, gate, up) + tuple(downs)
    count = len(slots)
    length, part_width = tokens.shape
    width = row * part_width
    seat = lax.axis_index("tp")
    place = lax.axis_index("fs")
    half = lax.axis_index("grp")

    barrier = pltpu.get_barrier_semaphore()
    for shift in (1, -1):
        there = place + shift

        @pl.when((there >= 0) & (there < line))
        def _():
            pl.semaphore_signal(barrier, inc=1, device_id={"fs": there}, device_id_type=MESH)

    for other in range(1, copies):
        pl.semaphore_signal(
            barrier,
            inc=1,
            device_id={"grp": lax.rem(half + other, copies)},
            device_id_type=MESH,
        )
    for other in range(1, row):
        pl.semaphore_signal(
            barrier,
            inc=1,
            device_id={"tp": lax.rem(seat + other, row)},
            device_id_type=MESH,
        )
    own = [pltpu.make_async_copy(shards[k], slots[k].at[place], own_sem.at[k]) for k in range(count)]
    for copy in own:
        copy.start()
    neighbours = (place > 0).astype(jnp.int32) + (place < line - 1).astype(jnp.int32)
    mine = pltpu.make_async_copy(tokens, gathered.at[seat], self_sem)
    mine.start()
    pl.semaphore_wait(barrier, neighbours + copies - 1 + row - 1)

    def piece(k, block, part):
        rows = slots[k].shape[1] // copies
        return slots[k].at[block, pl.ds(pl.multiple_of(part * rows, rows), rows), :]

    def hop(k, way, step):
        shift = 1 if way == 0 else -1
        block = place - shift * step
        return pltpu.make_async_remote_copy(
            src_ref=piece(k, block, half),
            dst_ref=piece(k, block, half),
            send_sem=line_send.at[k, way, step],
            recv_sem=line_recv.at[k, way, step],
            device_id={"fs": place + shift},
            device_id_type=MESH,
        )

    def arrival(k, way, step):
        shift = 1 if way == 0 else -1
        block = place - shift * step
        return pltpu.make_async_remote_copy(
            src_ref=piece(k, block, half),
            dst_ref=piece(k, block, half),
            send_sem=line_send.at[k, way, step - 1],
            recv_sem=line_recv.at[k, way, step - 1],
            device_id={"fs": place - shift},
            device_id_type=MESH,
        )

    def across(k, way, step, other):
        shift = 1 if way == 0 else -1
        block = place - shift * step
        return pltpu.make_async_remote_copy(
            src_ref=piece(k, block, half),
            dst_ref=piece(k, block, half),
            send_sem=pair_send.at[k, way, step - 1, other - 1],
            recv_sem=pair_recv.at[k, way, step - 1, other - 1],
            device_id={"grp": lax.rem(half + other, copies)},
            device_id_type=MESH,
        )

    def landed(k, way, step, other):
        shift = 1 if way == 0 else -1
        block = place - shift * step
        source = lax.rem(half + copies - other, copies)
        return pltpu.make_async_remote_copy(
            src_ref=piece(k, block, source),
            dst_ref=piece(k, block, source),
            send_sem=pair_send.at[k, way, step - 1, other - 1],
            recv_sem=pair_recv.at[k, way, step - 1, other - 1],
            device_id={"grp": source},
            device_id_type=MESH,
        )

    def has(way, step):
        return place >= step if way == 0 else place + step < line

    def goes(way):
        return place < line - 1 if way == 0 else place > 0

    def launch(k):
        own[k].wait()
        for way in range(2):

            @pl.when(goes(way))
            def _():
                hop(k, way, 0).start()

    def pump(k):
        for step in range(1, line):
            for way in range(2):

                @pl.when(has(way, step))
                def _():
                    arrival(k, way, step).wait_recv()
                    for other in range(1, copies):
                        across(k, way, step, other).start()

                @pl.when(has(way, step) & goes(way))
                def _():
                    hop(k, way, step).start()

    def settle(k):
        for step in range(1, line):
            for way in range(2):

                @pl.when(has(way, step))
                def _():
                    for other in range(1, copies):
                        landed(k, way, step, other).wait_recv()

    def drain(k):
        for way in range(2):
            for step in range(line):

                @pl.when((has(way, step) if step else True) & goes(way))
                def _():
                    hop(k, way, step).wait_send()

                if step:

                    @pl.when(has(way, step))
                    def _():
                        for other in range(1, copies):
                            across(k, way, step, other).wait_send()

    def spread(source, target, stage):
        return [
            pltpu.make_async_remote_copy(
                src_ref=source,
                dst_ref=target.at[seat],
                send_sem=row_send.at[stage, other - 1],
                recv_sem=row_recv.at[stage, other - 1],
                device_id={"tp": lax.rem(seat + other, row)},
                device_id_type=MESH,
            )
            for other in range(1, row)
        ]

    def spread_in(target, stage):
        sources = [lax.rem(seat + row - other, row) for other in range(1, row)]
        return [
            pltpu.make_async_remote_copy(
                src_ref=target.at[source],
                dst_ref=target.at[source],
                send_sem=row_send.at[stage, other],
                recv_sem=row_recv.at[stage, other],
                device_id={"tp": source},
                device_id_type=MESH,
            )
            for other, source in enumerate(sources)
        ]

    def scatter(source, target, stage, other):
        there = lax.rem(seat + other, row)
        return pltpu.make_async_remote_copy(
            src_ref=source.at[there],
            dst_ref=target.at[other - 1],
            send_sem=row_send.at[stage, other - 1],
            recv_sem=row_recv.at[stage, other - 1],
            device_id={"tp": there},
            device_id_type=MESH,
        )

    def normalize(source, gain_vector):
        total = jnp.zeros((length, 1), jnp.float32)
        for t in range(row):
            widened = source[t].astype(jnp.float32)
            total = total + jnp.sum(widened * widened, axis=1, keepdims=True)
        scale = lax.rsqrt(total / width + norm_eps)
        for t in range(row):
            span = slice(t * part_width, (t + 1) * part_width)
            scaled = source[t].astype(jnp.float32) * scale * gain_vector[:, span]
            normed[:, span] = scaled.astype(jnp.bfloat16)

    def times(weight, columns):
        block = weight[:, :, columns]
        return jnp.dot(
            normed[...], block.reshape(-1, block.shape[2]), preferred_element_type=jnp.float32
        )

    def shares(rows_in, weight, target):
        step = weight.shape[2]
        for block in range(line):
            term = jnp.dot(rows_in[...], weight[block], preferred_element_type=jnp.float32)
            begin = block * step
            inner = begin % part_width
            target[begin // part_width, :, inner : inner + step] = term.astype(jnp.bfloat16)

    def finish(i):
        settle(4 + i)
        if parts == 1:
            shares(hidden, downs[i], partial_ends.at[i])
        else:
            for j in range(row):
                blocks = [jnp.dot(
                    hidden[...], downs[i][j * line // row + c], preferred_element_type=jnp.float32
                ) for c in range(max(1, line // row))]
                for c, term in enumerate(blocks):
                    partial_ends[i, j, :, c * piece_width : (c + 1) * piece_width] = term.astype(
                        jnp.bfloat16
                    )
        for other in range(1, row):
            scatter(partial_ends.at[i], received_ends.at[i], 3 + i, other).start()

    def collect(i):
        span = slice(None) if parts == 1 else slice(i * piece_width, (i + 1) * piece_width)
        total = gathered_mid[seat, :, span].astype(jnp.float32)
        total = total + partial_ends[i, seat].astype(jnp.float32)
        for other in range(1, row):
            scatter(partial_ends.at[i], received_ends.at[i], 3 + i, other).wait_recv()
            total = total + received_ends[i, other - 1].astype(jnp.float32)
        out[:, span] = total.astype(jnp.bfloat16)

    launch(0)
    first = spread(tokens, gathered, 0)
    for copy in first:
        copy.start()
    launch(1)
    mine.wait()
    for copy in spread_in(gathered, 0):
        copy.wait_recv()
    normalize(gathered, input_gain)

    pump(0)
    launch(2)
    settle(0)
    ret_width = projected.shape[2]
    for t in range(4):
        projected[t] = (
            times(joined, slice(t * ret_width, (t + 1) * ret_width))
            .astype(jnp.bfloat16)
            .astype(jnp.float32)
        )
    pump(1)
    launch(3)

    head_count = rate_ahead.shape[0]
    head_dim = ret_width // head_count
    lane = lax.broadcasted_iota(jnp.int32, (length, ret_width), 1)
    in_lower = lax.rem(lane, head_dim) < head_dim // 2

    def turned(values):
        partner = jnp.where(
            in_lower,
            pltpu.roll(values, ret_width - head_dim // 2, 1),
            pltpu.roll(values, head_dim // 2, 1),
        )
        return values * cosine[...] + partner * sine_part[...]

    queries = turned(projected[0])
    key_heads = (turned(projected[1]) * head_dim ** (-0.5)).astype(jnp.bfloat16)
    valued = projected[2]
    offset = (
        lax.broadcasted_iota(jnp.int32, (length, length), 0)
        - lax.broadcasted_iota(jnp.int32, (length, length), 1)
    ).astype(jnp.float32)
    result = jnp.zeros((length, ret_width), jnp.float32)
    for h in range(head_count):
        here = (lane >= h * head_dim) & (lane < (h + 1) * head_dim)
        scores = lax.dot_general(
            jnp.where(here, queries, 0.0).astype(jnp.bfloat16),
            key_heads,
            (((1,), (1,)), ((), ())),
            preferred_element_type=jnp.float32,
        )
        decay = jnp.exp(jnp.where(offset >= 0, rate_ahead[h] * offset, -rate_behind[h] * offset))
        result = result + jnp.dot(
            (scores * decay).astype(jnp.bfloat16),
            jnp.where(here, valued, 0.0).astype(jnp.bfloat16),
            preferred_element_type=jnp.float32,
        )
    center = jnp.zeros((length, ret_width), jnp.float32)
    for h in range(head_count):
        here = (lane >= h * head_dim) & (lane < (h + 1) * head_dim)
        mean = jnp.sum(jnp.where(here, result, 0.0), axis=1, keepdims=True) / head_dim
        center = jnp.where(here, mean, center)
    centered = result - center
    squared = centered * centered
    factor = jnp.zeros((length, ret_width), jnp.float32)
    for h in range(head_count):
        here = (lane >= h * head_dim) & (lane < (h + 1) * head_dim)
        spread_h = jnp.sum(jnp.where(here, squared, 0.0), axis=1, keepdims=True) / head_dim
        factor = jnp.where(here, lax.rsqrt(spread_h + group_eps), factor)
    gates = projected[3]
    mixed[...] = (gates / (1.0 + jnp.exp(-gates)) * (centered * factor)).astype(jnp.bfloat16)

    settle(1)
    shares(mixed, merge, partial)
    for other in range(1, row):
        scatter(partial, received, 1, other).start()
    pump(2)
    total = tokens[...].astype(jnp.float32) + partial[seat].astype(jnp.float32)
    for other in range(1, row):
        scatter(partial, received, 1, other).wait_recv()
        total = total + received[other - 1].astype(jnp.float32)
    gathered_mid[seat] = total.astype(jnp.bfloat16)
    second = spread(gathered_mid.at[seat], gathered_mid, 2)
    for copy in second:
        copy.start()
    pump(3)
    launch(4)
    if parts > 1:
        launch(5)
    for copy in spread_in(gathered_mid, 2):
        copy.wait_recv()
    normalize(gathered_mid, middle_gain)
    settle(2)
    settle(3)
    hidden_width = hidden.shape[1]
    tile = 256 if hidden_width % 256 == 0 else 128

    @pl.loop(0, hidden_width // tile)
    def _(index):
        columns = pl.ds(pl.multiple_of(index * tile, tile), tile)
        gate_act = times(gate, columns)
        up_act = times(up, columns)
        hidden[:, columns] = (gate_act / (1.0 + jnp.exp(-gate_act)) * up_act).astype(jnp.bfloat16)

    for i in range(parts):
        pump(4 + i)
        if i + 2 < parts:
            launch(6 + i)
        if i:
            finish(i - 1)
    finish(parts - 1)
    for i in range(parts):
        collect(i)
    for copy in first + second:
        copy.wait_send()
    for other in range(1, row):
        scatter(partial, received, 1, other).wait_send()
        for i in range(parts):
            scatter(partial_ends.at[i], received_ends.at[i], 3 + i, other).wait_send()
    for k in range(count):
        drain(k)


def paired_kernel(
    sizes,
    tokens,
    input_gain,
    middle_gain,
    rate_ahead,
    rate_behind,
    cosine,
    sine_part,
    query_shard,
    key_shard,
    value_shard,
    output_gate_shard,
    merge_shard,
    gate_shard,
    up_shard,
    down_shard,
    out,
    joined_out,
    merge_out,
    gate_out,
    up_out,
    down_out,
    joined,
    merge,
    gate,
    up,
    down,
    gathered,
    gathered_mid,
    normed,
    projected,
    mixed,
    hidden,
    first_partial,
    first_core,
    first_row,
    first_line,
    last_partial,
    last_core,
    last_row,
    last_line,
    own_sem,
    line_send,
    line_recv,
    pair_send,
    pair_recv,
    share_send,
    share_recv,
    sum_send,
    sum_recv,
):
    line, row = sizes["fs"], sizes["tp"]
    pieces = down.shape[0]
    piece_width = down.shape[3]
    length, part_width = tokens.shape
    width = row * part_width
    seat = lax.axis_index("tp")
    place = lax.axis_index("fs")
    half = lax.axis_index("grp")
    core, column = lax.rem(seat, 2), seat // 2
    slot = lax.rem(place, 2)
    core_peer = seat + 1 - 2 * core
    row_peer = lax.rem(seat + 2, row)
    far_peer = lax.rem(core_peer + 2, row)
    line_peer = place + 1 - 2 * slot
    sign = 1 - 2 * (place // (line // 2))
    others = [lax.rem(place + sign * step + line, line) for step in range(1, line)]

    barrier = pltpu.get_barrier_semaphore()
    for there in others:
        pl.semaphore_signal(barrier, inc=1, device_id={"fs": there}, device_id_type=MESH)
    pl.semaphore_signal(barrier, inc=1, device_id={"grp": 1 - half}, device_id_type=MESH)
    for there in (core_peer, row_peer):
        pl.semaphore_signal(barrier, inc=1, device_id={"tp": there}, device_id_type=MESH)

    group = joined_out.shape[2] // 4
    quads = (query_shard, key_shard, value_shard, output_gate_shard)
    merge_rows = merge.shape[1]
    hidden_half = gate.shape[2]

    def cut(ref, axis, part, size):
        window = pl.ds(pl.multiple_of(part * size, size), size)
        return ref.at[window] if axis == 0 else ref.at[:, window]

    loads = [
        [
            (quad.at[:, p * group : (p + 1) * group], joined_out.at[p, :, i * group : (i + 1) * group])
            for p in range(2)
            for i, quad in enumerate(quads)
        ],
        [(merge_shard, merge_out)],
        [(gate_shard, gate_out)],
        [(up_shard, up_out)],
        [(down_shard, down_out)],
        [
            (cut(quad, 1, slot, group), joined.at[place, :, i * group : (i + 1) * group])
            for i, quad in enumerate(quads)
        ],
        [(cut(merge_shard, 0, slot, merge_rows), merge.at[place])],
        [(cut(gate_shard, 1, slot, hidden_half), gate.at[place])],
        [(cut(up_shard, 1, slot, hidden_half), up.at[place])],
        [
            (
                cut(down_shard, 0, slot, hidden_half).at[:, i * piece_width : (i + 1) * piece_width],
                down.at[i, place],
            )
            for i in range(pieces)
        ],
    ]
    own, index = [], 0
    for pairs in loads:
        own.append([])
        for source, target in pairs:
            own[-1].append(pltpu.make_async_copy(source, target, own_sem.at[index]))
            index += 1
    for copies in own:
        for copy in copies:
            copy.start()
    gathered[slot, seat] = tokens[...]
    pl.semaphore_wait(barrier, line - 1 + 1 + 2)

    def ready(k):
        for copy in own[k]:
            copy.wait()

    def outgoing(k, parity):
        if k == 0:
            size = joined.shape[1] // 2
            return joined_out.at[parity, pl.ds(pl.multiple_of(half * size, size), size)]
        if k == 1:
            size = merge_rows // 2
            return cut(merge_out, 0, parity * 2 + half, size)
        if k < 4:
            source = (gate_out, up_out)[k - 2]
            size = source.shape[0] // 2
            return cut(source, 0, half, size).at[
                :, pl.ds(pl.multiple_of(parity * hidden_half, hidden_half), hidden_half)
            ]
        size = hidden_half // 2
        return cut(down_out, 0, parity * 2 + half, size).at[
            :, (k - 4) * piece_width : (k - 3) * piece_width
        ]

    def landing(k, block, part):
        target = (joined, merge, gate, up)[k] if k < 4 else down.at[k - 4]
        size = target.shape[1] // 2
        return target.at[block, pl.ds(pl.multiple_of(part * size, size), size)]

    def post(k, there):
        return pltpu.make_async_remote_copy(
            src_ref=outgoing(k, lax.rem(there, 2)),
            dst_ref=landing(k, place, half),
            send_sem=line_send.at[k, there],
            recv_sem=line_recv.at[k, place],
            device_id={"fs": there},
            device_id_type=MESH,
        )

    def arrival(k, block):
        return pltpu.make_async_remote_copy(
            src_ref=landing(k, block, half),
            dst_ref=landing(k, block, half),
            send_sem=line_send.at[k, block],
            recv_sem=line_recv.at[k, block],
            device_id={"fs": block},
            device_id_type=MESH,
        )

    def across(k, block, part):
        return pltpu.make_async_remote_copy(
            src_ref=landing(k, block, part),
            dst_ref=landing(k, block, part),
            send_sem=pair_send.at[k, block],
            recv_sem=pair_recv.at[k, block],
            device_id={"grp": 1 - half},
            device_id_type=MESH,
        )

    def launch(k):
        ready(k)
        for there in others:
            post(k, there).start()

    def pump(k, block):
        arrival(k, block).wait_recv()
        across(k, block, half).start()

    def settle(k):
        for block in others:
            across(k, block, 1 - half).wait_recv()

    def handed(source, target, stage, step):
        plane = slot if step in (0, 1, 2, 3) else 1 - slot
        holder = seat if step in (0, 1, 2, 4, 5) else row_peer
        place_in = target.at[plane, holder]
        peer = {"tp": core_peer}
        if step in (1, 5):
            peer = {"tp": row_peer}
        if step == 2:
            peer = {"fs": line_peer}
        return pltpu.make_async_remote_copy(
            src_ref=source if step < 3 else place_in,
            dst_ref=place_in,
            send_sem=share_send.at[stage, step],
            recv_sem=share_recv.at[stage, step],
            device_id=peer,
            device_id_type=MESH,
        )

    def received(target, stage, step):
        plane = slot if step in (0, 1, 3) else 1 - slot
        holder = (core_peer, row_peer, seat, far_peer, core_peer, row_peer, far_peer)[step]
        place_in = target.at[plane, holder]
        return pltpu.make_async_remote_copy(
            src_ref=place_in,
            dst_ref=place_in,
            send_sem=share_send.at[stage, step],
            recv_sem=share_recv.at[stage, step],
            device_id={"tp": core_peer},
            device_id_type=MESH,
        )

    def normalize(source, gain_vector, plane):
        total = jnp.zeros((length, 1), jnp.float32)
        for t in range(row):
            widened = source[plane, t].astype(jnp.float32)
            total = total + jnp.sum(widened * widened, axis=1, keepdims=True)
        scale = lax.rsqrt(total / width + norm_eps)
        for t in range(row):
            span = slice(t * part_width, (t + 1) * part_width)
            scaled = source[plane, t].astype(jnp.float32) * scale * gain_vector[:, span]
            normed[plane, :, span] = scaled.astype(jnp.bfloat16)

    def hand_over(source, target, stage):
        return [handed(source, target, stage, step) for step in range(7)]

    def moved(source, target, peer, stage, step):
        return pltpu.make_async_remote_copy(
            src_ref=source,
            dst_ref=target,
            send_sem=sum_send.at[stage, step],
            recv_sem=sum_recv.at[stage, step],
            device_id=peer,
            device_id_type=MESH,
        )

    def reducer(partial, core_in, row_in, line_in, stage):
        return [
            moved(partial.at[1 - core], core_in, {"tp": core_peer}, stage, 0),
            moved(partial.at[core, 1 - column, 1 - slot], row_in.at[0], {"tp": row_peer}, stage, 1),
            moved(partial.at[core, 1 - column, slot], row_in.at[1], {"tp": row_peer}, stage, 2),
            moved(partial.at[core, column, 1 - slot], line_in, {"fs": line_peer}, stage, 3),
        ]

    def add_core(partial, core_in, steps):
        steps[0].wait_recv()
        for step, plane in ((1, 1 - slot), (2, slot)):
            total = partial[core, 1 - column, plane].astype(jnp.float32) + core_in[
                1 - column, plane
            ].astype(jnp.float32)
            partial[core, 1 - column, plane] = total.astype(jnp.bfloat16)
            steps[step].start()

    def add_row(partial, core_in, row_in, steps, step):
        plane = 1 - slot if step == 1 else slot
        steps[step].wait_recv()
        return (
            partial[core, column, plane].astype(jnp.float32)
            + core_in[column, plane].astype(jnp.float32)
            + row_in[step - 1].astype(jnp.float32)
        )

    def pass_line(partial, core_in, row_in, steps):
        total = add_row(partial, core_in, row_in, steps, 1)
        partial[core, column, 1 - slot] = total.astype(jnp.bfloat16)
        steps[3].start()

    first = hand_over(tokens, gathered, 0)
    for step in (2, 1, 0):
        first[step].start()
    launch(0)
    launch(1)
    launch(2)
    received(gathered, 0, 1).wait_recv()
    first[3].start()
    received(gathered, 0, 2).wait_recv()
    first[5].start()
    first[4].start()
    received(gathered, 0, 0).wait_recv()
    received(gathered, 0, 3).wait_recv()
    normalize(gathered, input_gain, slot)
    for block in others:
        pump(0, block)
    received(gathered, 0, 5).wait_recv()
    first[6].start()
    received(gathered, 0, 4).wait_recv()
    received(gathered, 0, 6).wait_recv()
    normalize(gathered, input_gain, 1 - slot)
    for block in others:
        pump(1, block)
    ready(5)
    settle(0)
    for plane in range(2):
        rows_out = jnp.dot(
            normed[plane], joined[...].reshape(width, 4 * group), preferred_element_type=jnp.float32
        )
        for i in range(4):
            projected[i, plane] = (
                rows_out[:, i * group : (i + 1) * group].astype(jnp.bfloat16).astype(jnp.float32)
            )

    head_count = rate_ahead.shape[0] // 2
    head_dim = group // head_count
    lane = lax.broadcasted_iota(jnp.int32, (length, group), 1)
    in_lower = lax.rem(lane, head_dim) < head_dim // 2

    def turned(values):
        partner = jnp.where(
            in_lower,
            pltpu.roll(values, group - head_dim // 2, 1),
            pltpu.roll(values, head_dim // 2, 1),
        )
        return values * cosine[...] + partner * sine_part[...]

    offset = (
        lax.broadcasted_iota(jnp.int32, (length, length), 0)
        - lax.broadcasted_iota(jnp.int32, (length, length), 1)
    ).astype(jnp.float32)
    decays = [
        jnp.exp(
            jnp.where(
                offset >= 0,
                rate_ahead[slot * head_count + h] * offset,
                -rate_behind[slot * head_count + h] * offset,
            )
        )
        for h in range(head_count)
    ]
    here = [(lane >= h * head_dim) & (lane < (h + 1) * head_dim) for h in range(head_count)]
    for plane in range(2):
        queries = turned(projected[0, plane])
        key_heads = (turned(projected[1, plane]) * head_dim ** (-0.5)).astype(jnp.bfloat16)
        valued = projected[2, plane]
        result = jnp.zeros((length, group), jnp.float32)
        for h in range(head_count):
            scores = lax.dot_general(
                jnp.where(here[h], queries, 0.0).astype(jnp.bfloat16),
                key_heads,
                (((1,), (1,)), ((), ())),
                preferred_element_type=jnp.float32,
            )
            result = result + jnp.dot(
                (scores * decays[h]).astype(jnp.bfloat16),
                jnp.where(here[h], valued, 0.0).astype(jnp.bfloat16),
                preferred_element_type=jnp.float32,
            )
        center = jnp.zeros((length, group), jnp.float32)
        for h in range(head_count):
            mean = jnp.sum(jnp.where(here[h], result, 0.0), axis=1, keepdims=True) / head_dim
            center = jnp.where(here[h], mean, center)
        centered = result - center
        squared = centered * centered
        factor = jnp.zeros((length, group), jnp.float32)
        for h in range(head_count):
            spread_h = jnp.sum(jnp.where(here[h], squared, 0.0), axis=1, keepdims=True) / head_dim
            factor = jnp.where(here[h], lax.rsqrt(spread_h + group_eps), factor)
        gates = projected[3, plane]
        mixed[plane] = (gates / (1.0 + jnp.exp(-gates)) * (centered * factor)).astype(jnp.bfloat16)

    ready(6)
    settle(1)

    def fill(rows_in, weight, partial, side):
        for x in range(row // 2):
            block = x * 2 + side
            for plane in range(2):
                term = jnp.dot(rows_in[plane], weight[block], preferred_element_type=jnp.float32)
                partial[side, x, plane] = term.astype(jnp.bfloat16)

    steps = reducer(first_partial, first_core, first_row, first_line, 0)
    fill(mixed, merge, first_partial, 1 - core)
    steps[0].start()
    fill(mixed, merge, first_partial, core)
    add_core(first_partial, first_core, steps)
    for block in others:
        pump(2, block)
    pass_line(first_partial, first_core, first_row, steps)
    launch(3)
    total = tokens[...].astype(jnp.float32) + add_row(
        first_partial, first_core, first_row, steps, 2
    )
    steps[3].wait_recv()
    total = total + first_line[...].astype(jnp.float32)
    gathered_mid[slot, seat] = total.astype(jnp.bfloat16)

    second = hand_over(gathered_mid.at[slot, seat], gathered_mid, 1)
    for step in (2, 1, 0):
        second[step].start()
    for i in range(pieces):
        if i == 0:
            ready(4)
        for there in others:
            post(4 + i, there).start()
    received(gathered_mid, 1, 1).wait_recv()
    second[3].start()
    received(gathered_mid, 1, 2).wait_recv()
    second[5].start()
    second[4].start()
    received(gathered_mid, 1, 0).wait_recv()
    received(gathered_mid, 1, 3).wait_recv()
    normalize(gathered_mid, middle_gain, slot)
    for block in others:
        pump(3, block)
    received(gathered_mid, 1, 5).wait_recv()
    second[6].start()
    received(gathered_mid, 1, 4).wait_recv()
    received(gathered_mid, 1, 6).wait_recv()
    normalize(gathered_mid, middle_gain, 1 - slot)
    ready(7)
    ready(8)
    settle(2)
    settle(3)
    tile = 256

    @pl.loop(0, 2)
    def _(plane):
        for begin in range(0, hidden_half, tile):
            columns = slice(begin, min(begin + tile, hidden_half))
            gate_act, up_act = [
                jnp.dot(
                    normed[plane],
                    weight[:, :, columns].reshape(width, -1),
                    preferred_element_type=jnp.float32,
                )
                for weight in (gate, up)
            ]
            hidden[plane, :, columns] = (gate_act / (1.0 + jnp.exp(-gate_act)) * up_act).astype(
                jnp.bfloat16
            )

    ready(9)
    ends = [
        reducer(last_partial.at[i], last_core.at[i], last_row.at[i], last_line.at[i], 1 + i)
        for i in range(pieces)
    ]

    def finish(i):
        span = slice(i * piece_width, (i + 1) * piece_width)
        total = gathered_mid[slot, seat, :, span].astype(jnp.float32) + add_row(
            last_partial.at[i], last_core.at[i], last_row.at[i], ends[i], 2
        )
        ends[i][3].wait_recv()
        out[:, span] = (total + last_line[i].astype(jnp.float32)).astype(jnp.bfloat16)

    for i in range(pieces):
        for block in others:
            pump(4 + i, block)
        settle(4 + i)
        fill(hidden, down.at[i], last_partial.at[i], 1 - core)
        ends[i][0].start()
        fill(hidden, down.at[i], last_partial.at[i], core)
        add_core(last_partial.at[i], last_core.at[i], ends[i])
        if i:
            pass_line(last_partial.at[i - 1], last_core.at[i - 1], last_row.at[i - 1], ends[i - 1])
    pass_line(last_partial.at[pieces - 1], last_core.at[pieces - 1], last_row.at[pieces - 1], ends[pieces - 1])
    for i in range(pieces):
        finish(i)

    for copy in first + second + steps:
        copy.wait_send()
    for group_steps in ends:
        for copy in group_steps:
            copy.wait_send()
    for k in range(4 + pieces):
        for there in others:
            post(k, there).wait_send()
            across(k, there, half).wait_send()


def paired_call(
    sizes, flat, input_gain, middle_gain, rates, tables, quads, merge_weight, gate_weight, up_weight, down_weight
):
    line, row = sizes["fs"], sizes["tp"]
    bf16 = jnp.bfloat16
    length, part_width = flat.shape
    depth, ret_width = quads[0].shape
    hidden_half, group = gate_weight.shape[1] // 2, ret_width // 2
    pieces = 2
    piece_width = down_weight.shape[1] // pieces
    kinds = 4 + pieces
    in_vmem = pl.BlockSpec(memory_space=pltpu.VMEM)
    in_smem = pl.BlockSpec(memory_space=pltpu.SMEM)

    def sums(lead, columns):
        return [
            pltpu.VMEM(lead + (2, row // 2, 2, length, columns), bf16),
            pltpu.VMEM(lead + (row // 2, 2, length, columns), bf16),
            pltpu.VMEM(lead + (2, length, columns), bf16),
            pltpu.VMEM(lead + (length, columns), bf16),
        ]

    dma = pltpu.SemaphoreType.DMA
    return pl.pallas_call(
        functools.partial(paired_kernel, sizes),
        out_shape=jax.ShapeDtypeStruct(flat.shape, bf16),
        in_specs=[in_vmem] * 3
        + [in_smem] * 2
        + [in_vmem] * 2
        + [pl.BlockSpec(memory_space=pl.ANY)] * 8,
        out_specs=in_vmem,
        scratch_shapes=[
            pltpu.VMEM((2, depth, 4 * group), bf16),
            pltpu.VMEM(merge_weight.shape, bf16),
            pltpu.VMEM(gate_weight.shape, bf16),
            pltpu.VMEM(up_weight.shape, bf16),
            pltpu.VMEM(down_weight.shape, bf16),
            pltpu.VMEM((line, depth, 4 * group), bf16),
            pltpu.VMEM((line, merge_weight.shape[0] // 2, part_width), bf16),
            pltpu.VMEM((line, depth, hidden_half), bf16),
            pltpu.VMEM((line, depth, hidden_half), bf16),
            pltpu.VMEM((pieces, line, hidden_half, piece_width), bf16),
            pltpu.VMEM((2, row, length, part_width), bf16),
            pltpu.VMEM((2, row, length, part_width), bf16),
            pltpu.VMEM((2, length, row * part_width), bf16),
            pltpu.VMEM((4, 2, length, group), jnp.float32),
            pltpu.VMEM((2, length, group), bf16),
            pltpu.VMEM((2, length, hidden_half), bf16),
        ]
        + sums((), part_width)
        + sums((pieces,), piece_width)
        + [
            dma((20 + pieces,)),
            dma((kinds, line)),
            dma((kinds, line)),
            dma((kinds, line)),
            dma((kinds, line)),
            dma((2, 7)),
            dma((2, 7)),
            dma((1 + pieces, 4)),
            dma((1 + pieces, 4)),
        ],
        compiler_params=pltpu.CompilerParams(
            collective_id=0, has_side_effects=True, vmem_limit_bytes=60 << 20
        ),
    )(
        flat,
        input_gain[None, :],
        middle_gain[None, :],
        *rates,
        *tables,
        *quads,
        merge_weight,
        gate_weight,
        up_weight,
        down_weight,
    )


def on_device(
    sizes,
    tokens,
    input_gain,
    query_weight,
    key_weight,
    value_weight,
    output_gate_matrix,
    forward_decay,
    backward_decay,
    merge_weight,
    middle_gain,
    gate_weight,
    up_weight,
    down_weight,
):
    seq_count, length, part_width = tokens.shape
    flat = tokens.reshape(seq_count * length, part_width)
    quads = (query_weight, key_weight, value_weight, output_gate_matrix)
    paired = (
        sizes["grp"] == 2
        and sizes["fs"] == sizes["tp"] == 4
        and seq_count == 1
        and query_weight.shape[1] % 256 == 0
        and forward_decay.shape[0] % 2 == 0
        and gate_weight.shape[1] % 256 == 0
        and down_weight.shape[1] == part_width
        and part_width % 256 == 0
    )
    if paired:
        head_count = forward_decay.shape[0] // 2
        head_dim = query_weight.shape[1] // (2 * head_count)
        layer_out = paired_call(
            sizes,
            flat,
            input_gain,
            middle_gain,
            (jax.nn.log_sigmoid(forward_decay), jax.nn.log_sigmoid(backward_decay)),
            turn_tables(length, head_dim, head_count),
            quads,
            merge_weight,
            gate_weight,
            up_weight,
            down_weight,
        )
        return layer_out.reshape(seq_count, length, part_width)
    joined = jnp.concatenate(quads, axis=1)
    shards = (joined, merge_weight, gate_weight, up_weight, down_weight)
    line, copies, row = sizes["fs"], sizes["grp"], sizes["tp"]
    down_width = down_weight.shape[1]
    parts = down_width // 256 if line == row and down_width % 256 == 0 else 1
    down_piece = jax.ShapeDtypeStruct((down_weight.shape[0], down_width // parts), jnp.bfloat16)
    landing = shards[:4] + (down_piece,) * parts
    count = len(landing)
    width, ret_width, hidden_width = row * part_width, query_weight.shape[1], gate_weight.shape[1]
    head_count = forward_decay.shape[0]
    tables = turn_tables(length, ret_width // head_count, head_count)
    in_vmem = pl.BlockSpec(memory_space=pltpu.VMEM)
    in_smem = pl.BlockSpec(memory_space=pltpu.SMEM)
    bf16 = jnp.bfloat16
    layer_out = pl.pallas_call(
        functools.partial(layer_kernel, sizes),
        out_shape=jax.ShapeDtypeStruct(flat.shape, bf16),
        in_specs=[in_vmem] * 3
        + [in_smem] * 2
        + [in_vmem] * 2
        + [pl.BlockSpec(memory_space=pl.ANY)] * len(shards),
        out_specs=in_vmem,
        scratch_shapes=[pltpu.VMEM((line,) + w.shape, w.dtype) for w in landing]
        + [
            pltpu.VMEM((row, length, part_width), bf16),
            pltpu.VMEM((row, length, part_width), bf16),
            pltpu.VMEM((length, width), bf16),
            pltpu.VMEM((4, length, ret_width), jnp.float32),
            pltpu.VMEM((length, ret_width), bf16),
            pltpu.VMEM((length, hidden_width), bf16),
            pltpu.VMEM((row, length, part_width), bf16),
            pltpu.VMEM((row - 1, length, part_width), bf16),
            pltpu.SemaphoreType.DMA((count,)),
            pltpu.SemaphoreType.DMA((count, 2, line)),
            pltpu.SemaphoreType.DMA((count, 2, line)),
            pltpu.SemaphoreType.DMA((count, 2, line, copies - 1)),
            pltpu.SemaphoreType.DMA((count, 2, line, copies - 1)),
            pltpu.SemaphoreType.DMA((3 + parts, row - 1)),
            pltpu.SemaphoreType.DMA((3 + parts, row - 1)),
            pltpu.SemaphoreType.DMA,
            pltpu.VMEM((parts, row, length, part_width // parts), bf16),
            pltpu.VMEM((parts, row - 1, length, part_width // parts), bf16),
        ],
        compiler_params=pltpu.CompilerParams(
            collective_id=0, has_side_effects=True, vmem_limit_bytes=58 << 20
        ),
    )(
        flat,
        input_gain[None, :],
        middle_gain[None, :],
        jax.nn.log_sigmoid(forward_decay),
        jax.nn.log_sigmoid(backward_decay),
        *tables,
        *shards,
    )
    return layer_out.reshape(seq_count, length, part_width)


def solution(mesh):
    placed = (
        P(("grp", "fs"), None, "tp"),
        P(),
        P("fs", "tp"),
        P("fs", "tp"),
        P("fs", "tp"),
        P("fs", "tp"),
        P("tp"),
        P("tp"),
        P("tp", "fs"),
        P(),
        P("fs", "tp"),
        P("fs", "tp"),
        P("tp", "fs"),
    )
    return jax.shard_map(
        functools.partial(on_device, dict(mesh.shape)),
        mesh=mesh,
        in_specs=placed,
        out_specs=P(("grp", "fs"), None, "tp"),
        check_vma=False,
    )
```

```python
import functools

import jax
import jax.numpy as jnp
import numpy as np
from jax import lax
from jax.experimental import pallas as pl
from jax.experimental.pallas import tpu as pltpu
from jax.sharding import PartitionSpec as P

norm_eps = 1e-06
group_eps = 1e-05
rope_base = 10000.0


def turn_tables(length, head_dim, head_count):
    half_dim = head_dim // 2
    inverse = rope_base ** (-np.arange(half_dim) / half_dim)
    angles = np.arange(length)[:, None] * inverse[None, :]
    cosine, sine_part = np.cos(angles), np.sin(angles)
    return (
        np.tile(np.concatenate([cosine, cosine], axis=1), (1, head_count)).astype(np.float32),
        np.tile(np.concatenate([-sine_part, sine_part], axis=1), (1, head_count)).astype(np.float32),
    )


MESH = pl.DeviceIdType.MESH


def layer_kernel(
    sizes,
    tokens,
    input_gain,
    middle_gain,
    rate_ahead,
    rate_behind,
    cosine,
    sine_part,
    joined_shard,
    merge_shard,
    gate_shard,
    up_shard,
    down_shard,
    out,
    joined,
    merge,
    gate,
    up,
    *rest,
):
    line, copies, row = sizes["fs"], sizes["grp"], sizes["tp"]
    parts = len(rest) - 18
    downs, partial_ends, received_ends = rest[:parts], rest[-2], rest[-1]
    (
        gathered,
        gathered_mid,
        normed,
        projected,
        mixed,
        hidden,
        partial,
        received,
        own_sem,
        line_send,
        line_recv,
        pair_send,
        pair_recv,
        row_send,
        row_recv,
        self_sem,
    ) = rest[parts:-2]
    piece_width = downs[0].shape[2]
    shards = (joined_shard, merge_shard, gate_shard, up_shard) + tuple(
        down_shard if parts == 1 else down_shard.at[:, pl.ds(i * piece_width, piece_width)]
        for i in range(parts)
    )
    slots = (joined, merge, gate, up) + tuple(downs)
    count = len(slots)
    length, part_width = tokens.shape
    width = row * part_width
    seat = lax.axis_index("tp")
    place = lax.axis_index("fs")
    half = lax.axis_index("grp")

    barrier = pltpu.get_barrier_semaphore()
    for shift in (1, -1):
        there = place + shift

        @pl.when((there >= 0) & (there < line))
        def _():
            pl.semaphore_signal(barrier, inc=1, device_id={"fs": there}, device_id_type=MESH)

    for other in range(1, copies):
        pl.semaphore_signal(
            barrier,
            inc=1,
            device_id={"grp": lax.rem(half + other, copies)},
            device_id_type=MESH,
        )
    for other in range(1, row):
        pl.semaphore_signal(
            barrier,
            inc=1,
            device_id={"tp": lax.rem(seat + other, row)},
            device_id_type=MESH,
        )
    own = [pltpu.make_async_copy(shards[k], slots[k].at[place], own_sem.at[k]) for k in range(count)]
    for copy in own:
        copy.start()
    neighbours = (place > 0).astype(jnp.int32) + (place < line - 1).astype(jnp.int32)
    mine = pltpu.make_async_copy(tokens, gathered.at[seat], self_sem)
    mine.start()
    pl.semaphore_wait(barrier, neighbours + copies - 1 + row - 1)

    def piece(k, block, part):
        rows = slots[k].shape[1] // copies
        return slots[k].at[block, pl.ds(pl.multiple_of(part * rows, rows), rows), :]

    def hop(k, way, step):
        shift = 1 if way == 0 else -1
        block = place - shift * step
        return pltpu.make_async_remote_copy(
            src_ref=piece(k, block, half),
            dst_ref=piece(k, block, half),
            send_sem=line_send.at[k, way, step],
            recv_sem=line_recv.at[k, way, step],
            device_id={"fs": place + shift},
            device_id_type=MESH,
        )

    def arrival(k, way, step):
        shift = 1 if way == 0 else -1
        block = place - shift * step
        return pltpu.make_async_remote_copy(
            src_ref=piece(k, block, half),
            dst_ref=piece(k, block, half),
            send_sem=line_send.at[k, way, step - 1],
            recv_sem=line_recv.at[k, way, step - 1],
            device_id={"fs": place - shift},
            device_id_type=MESH,
        )

    def across(k, way, step, other):
        shift = 1 if way == 0 else -1
        block = place - shift * step
        return pltpu.make_async_remote_copy(
            src_ref=piece(k, block, half),
            dst_ref=piece(k, block, half),
            send_sem=pair_send.at[k, way, step - 1, other - 1],
            recv_sem=pair_recv.at[k, way, step - 1, other - 1],
            device_id={"grp": lax.rem(half + other, copies)},
            device_id_type=MESH,
        )

    def landed(k, way, step, other):
        shift = 1 if way == 0 else -1
        block = place - shift * step
        source = lax.rem(half + copies - other, copies)
        return pltpu.make_async_remote_copy(
            src_ref=piece(k, block, source),
            dst_ref=piece(k, block, source),
            send_sem=pair_send.at[k, way, step - 1, other - 1],
            recv_sem=pair_recv.at[k, way, step - 1, other - 1],
            device_id={"grp": source},
            device_id_type=MESH,
        )

    def has(way, step):
        return place >= step if way == 0 else place + step < line

    def goes(way):
        return place < line - 1 if way == 0 else place > 0

    def launch(k):
        own[k].wait()
        for way in range(2):

            @pl.when(goes(way))
            def _():
                hop(k, way, 0).start()

    def pump(k):
        for step in range(1, line):
            for way in range(2):

                @pl.when(has(way, step))
                def _():
                    arrival(k, way, step).wait_recv()
                    for other in range(1, copies):
                        across(k, way, step, other).start()

                @pl.when(has(way, step) & goes(way))
                def _():
                    hop(k, way, step).start()

    def settle(k):
        for step in range(1, line):
            for way in range(2):

                @pl.when(has(way, step))
                def _():
                    for other in range(1, copies):
                        landed(k, way, step, other).wait_recv()

    def drain(k):
        for way in range(2):
            for step in range(line):

                @pl.when((has(way, step) if step else True) & goes(way))
                def _():
                    hop(k, way, step).wait_send()

                if step:

                    @pl.when(has(way, step))
                    def _():
                        for other in range(1, copies):
                            across(k, way, step, other).wait_send()

    def spread(source, target, stage):
        return [
            pltpu.make_async_remote_copy(
                src_ref=source,
                dst_ref=target.at[seat],
                send_sem=row_send.at[stage, other - 1],
                recv_sem=row_recv.at[stage, other - 1],
                device_id={"tp": lax.rem(seat + other, row)},
                device_id_type=MESH,
            )
            for other in range(1, row)
        ]

    def spread_in(target, stage):
        sources = [lax.rem(seat + row - other, row) for other in range(1, row)]
        return [
            pltpu.make_async_remote_copy(
                src_ref=target.at[source],
                dst_ref=target.at[source],
                send_sem=row_send.at[stage, other],
                recv_sem=row_recv.at[stage, other],
                device_id={"tp": source},
                device_id_type=MESH,
            )
            for other, source in enumerate(sources)
        ]

    def scatter(source, target, stage, other):
        there = lax.rem(seat + other, row)
        return pltpu.make_async_remote_copy(
            src_ref=source.at[there],
            dst_ref=target.at[other - 1],
            send_sem=row_send.at[stage, other - 1],
            recv_sem=row_recv.at[stage, other - 1],
            device_id={"tp": there},
            device_id_type=MESH,
        )

    def normalize(source, gain_vector):
        total = jnp.zeros((length, 1), jnp.float32)
        for t in range(row):
            widened = source[t].astype(jnp.float32)
            total = total + jnp.sum(widened * widened, axis=1, keepdims=True)
        scale = lax.rsqrt(total / width + norm_eps)
        for t in range(row):
            span = slice(t * part_width, (t + 1) * part_width)
            scaled = source[t].astype(jnp.float32) * scale * gain_vector[:, span]
            normed[:, span] = scaled.astype(jnp.bfloat16)

    def times(weight, columns):
        block = weight[:, :, columns]
        return jnp.dot(
            normed[...], block.reshape(-1, block.shape[2]), preferred_element_type=jnp.float32
        )

    def shares(rows_in, weight, target):
        step = weight.shape[2]
        for block in range(line):
            term = jnp.dot(rows_in[...], weight[block], preferred_element_type=jnp.float32)
            begin = block * step
            inner = begin % part_width
            target[begin // part_width, :, inner : inner + step] = term.astype(jnp.bfloat16)

    def finish(i):
        settle(4 + i)
        if parts == 1:
            shares(hidden, downs[i], partial_ends.at[i])
        else:
            for j in range(row):
                blocks = [jnp.dot(
                    hidden[...], downs[i][j * line // row + c], preferred_element_type=jnp.float32
                ) for c in range(max(1, line // row))]
                for c, term in enumerate(blocks):
                    partial_ends[i, j, :, c * piece_width : (c + 1) * piece_width] = term.astype(
                        jnp.bfloat16
                    )
        for other in range(1, row):
            scatter(partial_ends.at[i], received_ends.at[i], 3 + i, other).start()

    def collect(i):
        span = slice(None) if parts == 1 else slice(i * piece_width, (i + 1) * piece_width)
        total = gathered_mid[seat, :, span].astype(jnp.float32)
        total = total + partial_ends[i, seat].astype(jnp.float32)
        for other in range(1, row):
            scatter(partial_ends.at[i], received_ends.at[i], 3 + i, other).wait_recv()
            total = total + received_ends[i, other - 1].astype(jnp.float32)
        out[:, span] = total.astype(jnp.bfloat16)

    launch(0)
    first = spread(tokens, gathered, 0)
    for copy in first:
        copy.start()
    launch(1)
    mine.wait()
    for copy in spread_in(gathered, 0):
        copy.wait_recv()
    normalize(gathered, input_gain)

    pump(0)
    launch(2)
    settle(0)
    ret_width = projected.shape[2]
    for t in range(4):
        projected[t] = (
            times(joined, slice(t * ret_width, (t + 1) * ret_width))
            .astype(jnp.bfloat16)
            .astype(jnp.float32)
        )
    pump(1)
    launch(3)

    head_count = rate_ahead.shape[0]
    head_dim = ret_width // head_count
    lane = lax.broadcasted_iota(jnp.int32, (length, ret_width), 1)
    in_lower = lax.rem(lane, head_dim) < head_dim // 2

    def turned(values):
        partner = jnp.where(
            in_lower,
            pltpu.roll(values, ret_width - head_dim // 2, 1),
            pltpu.roll(values, head_dim // 2, 1),
        )
        return values * cosine[...] + partner * sine_part[...]

    queries = turned(projected[0])
    key_heads = (turned(projected[1]) * head_dim ** (-0.5)).astype(jnp.bfloat16)
    valued = projected[2]
    offset = (
        lax.broadcasted_iota(jnp.int32, (length, length), 0)
        - lax.broadcasted_iota(jnp.int32, (length, length), 1)
    ).astype(jnp.float32)
    result = jnp.zeros((length, ret_width), jnp.float32)
    for h in range(head_count):
        here = (lane >= h * head_dim) & (lane < (h + 1) * head_dim)
        scores = lax.dot_general(
            jnp.where(here, queries, 0.0).astype(jnp.bfloat16),
            key_heads,
            (((1,), (1,)), ((), ())),
            preferred_element_type=jnp.float32,
        )
        decay = jnp.exp(jnp.where(offset >= 0, rate_ahead[h] * offset, -rate_behind[h] * offset))
        result = result + jnp.dot(
            (scores * decay).astype(jnp.bfloat16),
            jnp.where(here, valued, 0.0).astype(jnp.bfloat16),
            preferred_element_type=jnp.float32,
        )
    center = jnp.zeros((length, ret_width), jnp.float32)
    for h in range(head_count):
        here = (lane >= h * head_dim) & (lane < (h + 1) * head_dim)
        mean = jnp.sum(jnp.where(here, result, 0.0), axis=1, keepdims=True) / head_dim
        center = jnp.where(here, mean, center)
    centered = result - center
    squared = centered * centered
    factor = jnp.zeros((length, ret_width), jnp.float32)
    for h in range(head_count):
        here = (lane >= h * head_dim) & (lane < (h + 1) * head_dim)
        spread_h = jnp.sum(jnp.where(here, squared, 0.0), axis=1, keepdims=True) / head_dim
        factor = jnp.where(here, lax.rsqrt(spread_h + group_eps), factor)
    gates = projected[3]
    mixed[...] = (gates / (1.0 + jnp.exp(-gates)) * (centered * factor)).astype(jnp.bfloat16)

    settle(1)
    shares(mixed, merge, partial)
    for other in range(1, row):
        scatter(partial, received, 1, other).start()
    pump(2)
    total = tokens[...].astype(jnp.float32) + partial[seat].astype(jnp.float32)
    for other in range(1, row):
        scatter(partial, received, 1, other).wait_recv()
        total = total + received[other - 1].astype(jnp.float32)
    gathered_mid[seat] = total.astype(jnp.bfloat16)
    second = spread(gathered_mid.at[seat], gathered_mid, 2)
    for copy in second:
        copy.start()
    pump(3)
    launch(4)
    if parts > 1:
        launch(5)
    for copy in spread_in(gathered_mid, 2):
        copy.wait_recv()
    normalize(gathered_mid, middle_gain)
    settle(2)
    settle(3)
    hidden_width = hidden.shape[1]
    tile = 256 if hidden_width % 256 == 0 else 128

    @pl.loop(0, hidden_width // tile)
    def _(index):
        columns = pl.ds(pl.multiple_of(index * tile, tile), tile)
        gate_act = times(gate, columns)
        up_act = times(up, columns)
        hidden[:, columns] = (gate_act / (1.0 + jnp.exp(-gate_act)) * up_act).astype(jnp.bfloat16)

    for i in range(parts):
        pump(4 + i)
        if i + 2 < parts:
            launch(6 + i)
        if i:
            finish(i - 1)
    finish(parts - 1)
    for i in range(parts):
        collect(i)
    for copy in first + second:
        copy.wait_send()
    for other in range(1, row):
        scatter(partial, received, 1, other).wait_send()
        for i in range(parts):
            scatter(partial_ends.at[i], received_ends.at[i], 3 + i, other).wait_send()
    for k in range(count):
        drain(k)


def paired_kernel(
    sizes,
    tokens,
    input_gain,
    middle_gain,
    rate_ahead,
    rate_behind,
    cosine,
    sine_part,
    query_shard,
    key_shard,
    value_shard,
    output_gate_shard,
    merge_shard,
    gate_shard,
    up_shard,
    down_shard,
    out,
    joined_out,
    merge_out,
    gate_out,
    up_out,
    down_out,
    joined,
    merge,
    gate,
    up,
    down,
    gathered,
    gathered_mid,
    normed,
    projected,
    mixed,
    hidden,
    first_partial,
    first_core,
    first_row,
    first_line,
    last_partial,
    last_core,
    last_row,
    last_line,
    own_sem,
    line_send,
    line_recv,
    pair_send,
    pair_recv,
    share_send,
    share_recv,
    sum_send,
    sum_recv,
):
    line, row = sizes["fs"], sizes["tp"]
    pieces = down.shape[0]
    piece_width = down.shape[3]
    length, part_width = tokens.shape
    width = row * part_width
    seat = lax.axis_index("tp")
    place = lax.axis_index("fs")
    half = lax.axis_index("grp")
    core, column = lax.rem(seat, 2), seat // 2
    slot = lax.rem(place, 2)
    core_peer = seat + 1 - 2 * core
    row_peer = lax.rem(seat + 2, row)
    far_peer = lax.rem(core_peer + 2, row)
    line_peer = place + 1 - 2 * slot
    sign = 1 - 2 * (place // (line // 2))
    others = [lax.rem(place + sign * step + line, line) for step in range(1, line)]

    barrier = pltpu.get_barrier_semaphore()
    for there in others:
        pl.semaphore_signal(barrier, inc=1, device_id={"fs": there}, device_id_type=MESH)
    pl.semaphore_signal(barrier, inc=1, device_id={"grp": 1 - half}, device_id_type=MESH)
    for there in (core_peer, row_peer):
        pl.semaphore_signal(barrier, inc=1, device_id={"tp": there}, device_id_type=MESH)

    group = joined_out.shape[2] // 4
    quads = (query_shard, key_shard, value_shard, output_gate_shard)
    merge_rows = merge.shape[1]
    hidden_half = gate.shape[2]

    def cut(ref, axis, part, size):
        window = pl.ds(pl.multiple_of(part * size, size), size)
        return ref.at[window] if axis == 0 else ref.at[:, window]

    loads = [
        [
            (quad.at[:, p * group : (p + 1) * group], joined_out.at[p, :, i * group : (i + 1) * group])
            for p in range(2)
            for i, quad in enumerate(quads)
        ],
        [(merge_shard, merge_out)],
        [(gate_shard, gate_out)],
        [(up_shard, up_out)],
        [(down_shard, down_out)],
        [
            (cut(quad, 1, slot, group), joined.at[place, :, i * group : (i + 1) * group])
            for i, quad in enumerate(quads)
        ],
        [(cut(merge_shard, 0, slot, merge_rows), merge.at[place])],
        [(cut(gate_shard, 1, slot, hidden_half), gate.at[place])],
        [(cut(up_shard, 1, slot, hidden_half), up.at[place])],
        [
            (
                cut(down_shard, 0, slot, hidden_half).at[:, i * piece_width : (i + 1) * piece_width],
                down.at[i, place],
            )
            for i in range(pieces)
        ],
    ]
    own, index = [], 0
    for pairs in loads:
        own.append([])
        for source, target in pairs:
            own[-1].append(pltpu.make_async_copy(source, target, own_sem.at[index]))
            index += 1
    for copies in own:
        for copy in copies:
            copy.start()
    gathered[slot, seat] = tokens[...]
    pl.semaphore_wait(barrier, line - 1 + 1 + 2)

    def ready(k):
        for copy in own[k]:
            copy.wait()

    def outgoing(k, parity):
        if k == 0:
            size = joined.shape[1] // 2
            return joined_out.at[parity, pl.ds(pl.multiple_of(half * size, size), size)]
        if k == 1:
            size = merge_rows // 2
            return cut(merge_out, 0, parity * 2 + half, size)
        if k < 4:
            source = (gate_out, up_out)[k - 2]
            size = source.shape[0] // 2
            return cut(source, 0, half, size).at[
                :, pl.ds(pl.multiple_of(parity * hidden_half, hidden_half), hidden_half)
            ]
        size = hidden_half // 2
        return cut(down_out, 0, parity * 2 + half, size).at[
            :, (k - 4) * piece_width : (k - 3) * piece_width
        ]

    def landing(k, block, part):
        target = (joined, merge, gate, up)[k] if k < 4 else down.at[k - 4]
        size = target.shape[1] // 2
        return target.at[block, pl.ds(pl.multiple_of(part * size, size), size)]

    def post(k, there):
        return pltpu.make_async_remote_copy(
            src_ref=outgoing(k, lax.rem(there, 2)),
            dst_ref=landing(k, place, half),
            send_sem=line_send.at[k, there],
            recv_sem=line_recv.at[k, place],
            device_id={"fs": there},
            device_id_type=MESH,
        )

    def arrival(k, block):
        return pltpu.make_async_remote_copy(
            src_ref=landing(k, block, half),
            dst_ref=landing(k, block, half),
            send_sem=line_send.at[k, block],
            recv_sem=line_recv.at[k, block],
            device_id={"fs": block},
            device_id_type=MESH,
        )

    def across(k, block, part):
        return pltpu.make_async_remote_copy(
            src_ref=landing(k, block, part),
            dst_ref=landing(k, block, part),
            send_sem=pair_send.at[k, block],
            recv_sem=pair_recv.at[k, block],
            device_id={"grp": 1 - half},
            device_id_type=MESH,
        )

    def launch(k):
        ready(k)
        for there in others:
            post(k, there).start()

    def pump(k, block):
        arrival(k, block).wait_recv()
        across(k, block, half).start()

    def settle(k):
        for block in others:
            across(k, block, 1 - half).wait_recv()

    def handed(source, target, stage, step):
        plane = slot if step in (0, 1, 2, 3) else 1 - slot
        holder = seat if step in (0, 1, 2, 4, 5) else row_peer
        place_in = target.at[plane, holder]
        peer = {"tp": core_peer}
        if step in (1, 5):
            peer = {"tp": row_peer}
        if step == 2:
            peer = {"fs": line_peer}
        return pltpu.make_async_remote_copy(
            src_ref=source if step < 3 else place_in,
            dst_ref=place_in,
            send_sem=share_send.at[stage, step],
            recv_sem=share_recv.at[stage, step],
            device_id=peer,
            device_id_type=MESH,
        )

    def received(target, stage, step):
        plane = slot if step in (0, 1, 3) else 1 - slot
        holder = (core_peer, row_peer, seat, far_peer, core_peer, row_peer, far_peer)[step]
        place_in = target.at[plane, holder]
        return pltpu.make_async_remote_copy(
            src_ref=place_in,
            dst_ref=place_in,
            send_sem=share_send.at[stage, step],
            recv_sem=share_recv.at[stage, step],
            device_id={"tp": core_peer},
            device_id_type=MESH,
        )

    def normalize(source, gain_vector, plane):
        total = jnp.zeros((length, 1), jnp.float32)
        for t in range(row):
            widened = source[plane, t].astype(jnp.float32)
            total = total + jnp.sum(widened * widened, axis=1, keepdims=True)
        scale = lax.rsqrt(total / width + norm_eps)
        for t in range(row):
            span = slice(t * part_width, (t + 1) * part_width)
            scaled = source[plane, t].astype(jnp.float32) * scale * gain_vector[:, span]
            normed[plane, :, span] = scaled.astype(jnp.bfloat16)

    def hand_over(source, target, stage):
        return [handed(source, target, stage, step) for step in range(7)]

    def moved(source, target, peer, stage, step):
        return pltpu.make_async_remote_copy(
            src_ref=source,
            dst_ref=target,
            send_sem=sum_send.at[stage, step],
            recv_sem=sum_recv.at[stage, step],
            device_id=peer,
            device_id_type=MESH,
        )

    def share_mid(step):
        plane, kind = step % 2, step // 2
        spot = gathered_mid.at[plane, row_peer if kind == 2 else seat]
        return pltpu.make_async_remote_copy(
            src_ref=spot,
            dst_ref=spot,
            send_sem=share_send.at[1, step],
            recv_sem=share_recv.at[1, step],
            device_id={"tp": core_peer if kind else row_peer},
            device_id_type=MESH,
        )

    def shared_mid(step):
        plane, kind = step % 2, step // 2
        spot = gathered_mid.at[plane, (row_peer, core_peer, far_peer)[kind]]
        return pltpu.make_async_remote_copy(
            src_ref=spot,
            dst_ref=spot,
            send_sem=share_send.at[1, step],
            recv_sem=share_recv.at[1, step],
            device_id={"tp": core_peer},
            device_id_type=MESH,
        )

    def reducer(partial, core_in, row_in, stage):
        order = (0, 1) if stage == 0 else (1 - slot, slot)
        return [moved(partial.at[1 - core], core_in, {"tp": core_peer}, stage, 0)] + [
            moved(
                partial.at[core, 1 - column, plane],
                row_in.at[step],
                {"tp": row_peer},
                stage,
                1 + step,
            )
            for step, plane in enumerate(order)
        ]

    def add_core(partial, core_in, steps, order):
        steps[0].wait_recv()
        for step, plane in enumerate(order):
            total = partial[core, 1 - column, plane].astype(jnp.float32) + core_in[
                1 - column, plane
            ].astype(jnp.float32)
            partial[core, 1 - column, plane] = total.astype(jnp.bfloat16)
            steps[1 + step].start()

    def add_row(partial, core_in, row_in, steps, step, plane):
        steps[1 + step].wait_recv()
        return (
            partial[core, column, plane].astype(jnp.float32)
            + core_in[column, plane].astype(jnp.float32)
            + row_in[step].astype(jnp.float32)
        )

    first = hand_over(tokens, gathered, 0)
    for step in (2, 1, 0):
        first[step].start()
    launch(0)
    launch(1)
    launch(2)
    received(gathered, 0, 1).wait_recv()
    first[3].start()
    received(gathered, 0, 2).wait_recv()
    first[5].start()
    first[4].start()
    received(gathered, 0, 0).wait_recv()
    received(gathered, 0, 3).wait_recv()
    normalize(gathered, input_gain, slot)
    for block in others:
        pump(0, block)
    received(gathered, 0, 5).wait_recv()
    first[6].start()
    received(gathered, 0, 4).wait_recv()
    received(gathered, 0, 6).wait_recv()
    normalize(gathered, input_gain, 1 - slot)
    for block in others:
        pump(1, block)
    ready(5)
    settle(0)
    for plane in range(2):
        rows_out = jnp.dot(
            normed[plane], joined[...].reshape(width, 4 * group), preferred_element_type=jnp.float32
        )
        for i in range(4):
            projected[i, plane] = (
                rows_out[:, i * group : (i + 1) * group].astype(jnp.bfloat16).astype(jnp.float32)
            )

    head_count = rate_ahead.shape[0] // 2
    head_dim = group // head_count
    lane = lax.broadcasted_iota(jnp.int32, (length, group), 1)
    in_lower = lax.rem(lane, head_dim) < head_dim // 2

    def turned(values):
        partner = jnp.where(
            in_lower,
            pltpu.roll(values, group - head_dim // 2, 1),
            pltpu.roll(values, head_dim // 2, 1),
        )
        return values * cosine[...] + partner * sine_part[...]

    offset = (
        lax.broadcasted_iota(jnp.int32, (length, length), 0)
        - lax.broadcasted_iota(jnp.int32, (length, length), 1)
    ).astype(jnp.float32)
    decays = [
        jnp.exp(
            jnp.where(
                offset >= 0,
                rate_ahead[slot * head_count + h] * offset,
                -rate_behind[slot * head_count + h] * offset,
            )
        )
        for h in range(head_count)
    ]
    here = [(lane >= h * head_dim) & (lane < (h + 1) * head_dim) for h in range(head_count)]
    for plane in range(2):
        queries = turned(projected[0, plane])
        key_heads = (turned(projected[1, plane]) * head_dim ** (-0.5)).astype(jnp.bfloat16)
        valued = projected[2, plane]
        result = jnp.zeros((length, group), jnp.float32)
        for h in range(head_count):
            scores = lax.dot_general(
                jnp.where(here[h], queries, 0.0).astype(jnp.bfloat16),
                key_heads,
                (((1,), (1,)), ((), ())),
                preferred_element_type=jnp.float32,
            )
            result = result + jnp.dot(
                (scores * decays[h]).astype(jnp.bfloat16),
                jnp.where(here[h], valued, 0.0).astype(jnp.bfloat16),
                preferred_element_type=jnp.float32,
            )
        center = jnp.zeros((length, group), jnp.float32)
        for h in range(head_count):
            mean = jnp.sum(jnp.where(here[h], result, 0.0), axis=1, keepdims=True) / head_dim
            center = jnp.where(here[h], mean, center)
        centered = result - center
        squared = centered * centered
        factor = jnp.zeros((length, group), jnp.float32)
        for h in range(head_count):
            spread_h = jnp.sum(jnp.where(here[h], squared, 0.0), axis=1, keepdims=True) / head_dim
            factor = jnp.where(here[h], lax.rsqrt(spread_h + group_eps), factor)
        gates = projected[3, plane]
        mixed[plane] = (gates / (1.0 + jnp.exp(-gates)) * (centered * factor)).astype(jnp.bfloat16)

    ready(6)
    settle(1)

    def fill(rows_in, weight, partial, side):
        for x in range(row // 2):
            block = x * 2 + side
            for plane in range(2):
                term = jnp.dot(rows_in[plane], weight[block], preferred_element_type=jnp.float32)
                partial[side, x, plane] = term.astype(jnp.bfloat16)

    steps = reducer(first_partial, first_core, first_row, 0) + [
        moved(first_partial.at[core, column, plane], first_line.at[plane], {"fs": line_peer}, 0, 3 + plane)
        for plane in range(2)
    ]
    fill(mixed, merge, first_partial, 1 - core)
    steps[0].start()
    pump(2, others[0])
    fill(mixed, merge, first_partial, core)
    pump(2, others[1])
    add_core(first_partial, first_core, steps, (0, 1))
    pump(2, others[2])
    for plane in range(2):
        total = add_row(first_partial, first_core, first_row, steps, plane, plane)
        first_partial[core, column, plane] = total.astype(jnp.bfloat16)
        steps[3 + plane].start()
    launch(3)
    ready(4)
    for i in range(pieces):
        for there in others:
            post(4 + i, there).start()

    second = [share_mid(step) for step in range(6)]
    for plane in range(2):
        steps[3 + plane].wait_recv()
        total = gathered[plane, seat].astype(jnp.float32) + (
            first_partial[core, column, plane].astype(jnp.float32)
            + first_line[plane].astype(jnp.float32)
        )
        gathered_mid[plane, seat] = total.astype(jnp.bfloat16)
        second[plane].start()
        second[2 + plane].start()
    for plane in range(2):
        pump(3, others[plane])
        shared_mid(plane).wait_recv()
        second[4 + plane].start()
    pump(3, others[2])
    for plane in range(2):
        shared_mid(2 + plane).wait_recv()
        shared_mid(4 + plane).wait_recv()
        normalize(gathered_mid, middle_gain, plane)
        pump(4, others[plane])
    ready(7)
    ready(8)
    settle(2)
    settle(3)
    tile = 256
    for plane in range(2):
        for begin in range(0, hidden_half, tile):
            columns = slice(begin, min(begin + tile, hidden_half))
            gate_act, up_act = [
                jnp.dot(
                    normed[plane],
                    weight[:, :, columns].reshape(width, -1),
                    preferred_element_type=jnp.float32,
                )
                for weight in (gate, up)
            ]
            hidden[plane, :, columns] = (gate_act / (1.0 + jnp.exp(-gate_act)) * up_act).astype(
                jnp.bfloat16
            )
        pump(4 + plane, others[2 * (1 - plane)])

    ready(9)
    ends = [
        reducer(last_partial.at[i], last_core.at[i], last_row.at[i], 1 + i)
        + [
            moved(
                last_partial.at[i, core, column, 1 - slot],
                last_line.at[i],
                {"fs": line_peer},
                1 + i,
                3,
            )
        ]
        for i in range(pieces)
    ]

    def pass_line(i):
        total = add_row(
            last_partial.at[i], last_core.at[i], last_row.at[i], ends[i], 0, 1 - slot
        )
        last_partial[i, core, column, 1 - slot] = total.astype(jnp.bfloat16)
        ends[i][3].start()

    def finish(i):
        span = slice(i * piece_width, (i + 1) * piece_width)
        total = gathered_mid[slot, seat, :, span].astype(jnp.float32) + add_row(
            last_partial.at[i], last_core.at[i], last_row.at[i], ends[i], 1, slot
        )
        ends[i][3].wait_recv()
        out[:, span] = (total + last_line[i].astype(jnp.float32)).astype(jnp.bfloat16)

    for i in range(pieces):
        if i:
            for block in others[1:] if i == 1 else others:
                pump(4 + i, block)
        settle(4 + i)
        fill(hidden, down.at[i], last_partial.at[i], 1 - core)
        ends[i][0].start()
        fill(hidden, down.at[i], last_partial.at[i], core)
        add_core(last_partial.at[i], last_core.at[i], ends[i], (1 - slot, slot))
        if i:
            pass_line(i - 1)
    pass_line(pieces - 1)
    for i in range(pieces):
        finish(i)

    for copy in first + second + steps:
        copy.wait_send()
    for group_steps in ends:
        for copy in group_steps:
            copy.wait_send()
    for k in range(4 + pieces):
        for there in others:
            post(k, there).wait_send()
            across(k, there, half).wait_send()


def paired_call(
    sizes, flat, input_gain, middle_gain, rates, tables, quads, merge_weight, gate_weight, up_weight, down_weight
):
    line, row = sizes["fs"], sizes["tp"]
    bf16 = jnp.bfloat16
    length, part_width = flat.shape
    depth, ret_width = quads[0].shape
    hidden_half, group = gate_weight.shape[1] // 2, ret_width // 2
    pieces = 2
    piece_width = down_weight.shape[1] // pieces
    kinds = 4 + pieces
    in_vmem = pl.BlockSpec(memory_space=pltpu.VMEM)
    in_smem = pl.BlockSpec(memory_space=pltpu.SMEM)

    def sums(lead, columns, last):
        return [
            pltpu.VMEM(lead + (2, row // 2, 2, length, columns), bf16),
            pltpu.VMEM(lead + (row // 2, 2, length, columns), bf16),
            pltpu.VMEM(lead + (2, length, columns), bf16),
            pltpu.VMEM(lead + last + (length, columns), bf16),
        ]

    dma = pltpu.SemaphoreType.DMA
    return pl.pallas_call(
        functools.partial(paired_kernel, sizes),
        out_shape=jax.ShapeDtypeStruct(flat.shape, bf16),
        in_specs=[in_vmem] * 3
        + [in_smem] * 2
        + [in_vmem] * 2
        + [pl.BlockSpec(memory_space=pl.ANY)] * 8,
        out_specs=in_vmem,
        scratch_shapes=[
            pltpu.VMEM((2, depth, 4 * group), bf16),
            pltpu.VMEM(merge_weight.shape, bf16),
            pltpu.VMEM(gate_weight.shape, bf16),
            pltpu.VMEM(up_weight.shape, bf16),
            pltpu.VMEM(down_weight.shape, bf16),
            pltpu.VMEM((line, depth, 4 * group), bf16),
            pltpu.VMEM((line, merge_weight.shape[0] // 2, part_width), bf16),
            pltpu.VMEM((line, depth, hidden_half), bf16),
            pltpu.VMEM((line, depth, hidden_half), bf16),
            pltpu.VMEM((pieces, line, hidden_half, piece_width), bf16),
            pltpu.VMEM((2, row, length, part_width), bf16),
            pltpu.VMEM((2, row, length, part_width), bf16),
            pltpu.VMEM((2, length, row * part_width), bf16),
            pltpu.VMEM((4, 2, length, group), jnp.float32),
            pltpu.VMEM((2, length, group), bf16),
            pltpu.VMEM((2, length, hidden_half), bf16),
        ]
        + sums((), part_width, (2,))
        + sums((pieces,), piece_width, ())
        + [
            dma((20 + pieces,)),
            dma((kinds, line)),
            dma((kinds, line)),
            dma((kinds, line)),
            dma((kinds, line)),
            dma((2, 7)),
            dma((2, 7)),
            dma((1 + pieces, 5)),
            dma((1 + pieces, 5)),
        ],
        compiler_params=pltpu.CompilerParams(
            collective_id=0, has_side_effects=True, vmem_limit_bytes=60 << 20
        ),
    )(
        flat,
        input_gain[None, :],
        middle_gain[None, :],
        *rates,
        *tables,
        *quads,
        merge_weight,
        gate_weight,
        up_weight,
        down_weight,
    )


def on_device(
    sizes,
    tokens,
    input_gain,
    query_weight,
    key_weight,
    value_weight,
    output_gate_matrix,
    forward_decay,
    backward_decay,
    merge_weight,
    middle_gain,
    gate_weight,
    up_weight,
    down_weight,
):
    seq_count, length, part_width = tokens.shape
    flat = tokens.reshape(seq_count * length, part_width)
    quads = (query_weight, key_weight, value_weight, output_gate_matrix)
    paired = (
        sizes["grp"] == 2
        and sizes["fs"] == sizes["tp"] == 4
        and seq_count == 1
        and query_weight.shape[1] % 256 == 0
        and forward_decay.shape[0] % 2 == 0
        and gate_weight.shape[1] % 256 == 0
        and down_weight.shape[1] == part_width
        and part_width % 256 == 0
    )
    if paired:
        head_count = forward_decay.shape[0] // 2
        head_dim = query_weight.shape[1] // (2 * head_count)
        layer_out = paired_call(
            sizes,
            flat,
            input_gain,
            middle_gain,
            (jax.nn.log_sigmoid(forward_decay), jax.nn.log_sigmoid(backward_decay)),
            turn_tables(length, head_dim, head_count),
            quads,
            merge_weight,
            gate_weight,
            up_weight,
            down_weight,
        )
        return layer_out.reshape(seq_count, length, part_width)
    joined = jnp.concatenate(quads, axis=1)
    shards = (joined, merge_weight, gate_weight, up_weight, down_weight)
    line, copies, row = sizes["fs"], sizes["grp"], sizes["tp"]
    down_width = down_weight.shape[1]
    parts = down_width // 256 if line == row and down_width % 256 == 0 else 1
    down_piece = jax.ShapeDtypeStruct((down_weight.shape[0], down_width // parts), jnp.bfloat16)
    landing = shards[:4] + (down_piece,) * parts
    count = len(landing)
    width, ret_width, hidden_width = row * part_width, query_weight.shape[1], gate_weight.shape[1]
    head_count = forward_decay.shape[0]
    tables = turn_tables(length, ret_width // head_count, head_count)
    in_vmem = pl.BlockSpec(memory_space=pltpu.VMEM)
    in_smem = pl.BlockSpec(memory_space=pltpu.SMEM)
    bf16 = jnp.bfloat16
    layer_out = pl.pallas_call(
        functools.partial(layer_kernel, sizes),
        out_shape=jax.ShapeDtypeStruct(flat.shape, bf16),
        in_specs=[in_vmem] * 3
        + [in_smem] * 2
        + [in_vmem] * 2
        + [pl.BlockSpec(memory_space=pl.ANY)] * len(shards),
        out_specs=in_vmem,
        scratch_shapes=[pltpu.VMEM((line,) + w.shape, w.dtype) for w in landing]
        + [
            pltpu.VMEM((row, length, part_width), bf16),
            pltpu.VMEM((row, length, part_width), bf16),
            pltpu.VMEM((length, width), bf16),
            pltpu.VMEM((4, length, ret_width), jnp.float32),
            pltpu.VMEM((length, ret_width), bf16),
            pltpu.VMEM((length, hidden_width), bf16),
            pltpu.VMEM((row, length, part_width), bf16),
            pltpu.VMEM((row - 1, length, part_width), bf16),
            pltpu.SemaphoreType.DMA((count,)),
            pltpu.SemaphoreType.DMA((count, 2, line)),
            pltpu.SemaphoreType.DMA((count, 2, line)),
            pltpu.SemaphoreType.DMA((count, 2, line, copies - 1)),
            pltpu.SemaphoreType.DMA((count, 2, line, copies - 1)),
            pltpu.SemaphoreType.DMA((3 + parts, row - 1)),
            pltpu.SemaphoreType.DMA((3 + parts, row - 1)),
            pltpu.SemaphoreType.DMA,
            pltpu.VMEM((parts, row, length, part_width // parts), bf16),
            pltpu.VMEM((parts, row - 1, length, part_width // parts), bf16),
        ],
        compiler_params=pltpu.CompilerParams(
            collective_id=0, has_side_effects=True, vmem_limit_bytes=58 << 20
        ),
    )(
        flat,
        input_gain[None, :],
        middle_gain[None, :],
        jax.nn.log_sigmoid(forward_decay),
        jax.nn.log_sigmoid(backward_decay),
        *tables,
        *shards,
    )
    return layer_out.reshape(seq_count, length, part_width)


def solution(mesh):
    placed = (
        P(("grp", "fs"), None, "tp"),
        P(),
        P("fs", "tp"),
        P("fs", "tp"),
        P("fs", "tp"),
        P("fs", "tp"),
        P("tp"),
        P("tp"),
        P("tp", "fs"),
        P(),
        P("fs", "tp"),
        P("fs", "tp"),
        P("tp", "fs"),
    )
    return jax.shard_map(
        functools.partial(on_device, dict(mesh.shape)),
        mesh=mesh,
        in_specs=placed,
        out_specs=P(("grp", "fs"), None, "tp"),
        check_vma=False,
    )
```

```python
import functools

import jax
import jax.numpy as jnp
import numpy as np
from jax import lax
from jax.experimental import pallas as pl
from jax.experimental.pallas import tpu as pltpu
from jax.sharding import PartitionSpec as P

norm_eps = 1e-06
group_eps = 1e-05
rope_base = 10000.0


def turn_tables(length, head_dim, head_count):
    half_dim = head_dim // 2
    inverse = rope_base ** (-np.arange(half_dim) / half_dim)
    angles = np.arange(length)[:, None] * inverse[None, :]
    cosine, sine_part = np.cos(angles), np.sin(angles)
    return (
        np.tile(np.concatenate([cosine, cosine], axis=1), (1, head_count)).astype(np.float32),
        np.tile(np.concatenate([-sine_part, sine_part], axis=1), (1, head_count)).astype(np.float32),
    )


MESH = pl.DeviceIdType.MESH


def layer_kernel(
    sizes,
    tokens,
    input_gain,
    middle_gain,
    rate_ahead,
    rate_behind,
    cosine,
    sine_part,
    joined_shard,
    merge_shard,
    gate_shard,
    up_shard,
    down_shard,
    out,
    joined,
    merge,
    gate,
    up,
    *rest,
):
    line, copies, row = sizes["fs"], sizes["grp"], sizes["tp"]
    parts = len(rest) - 18
    downs, partial_ends, received_ends = rest[:parts], rest[-2], rest[-1]
    (
        gathered,
        gathered_mid,
        normed,
        projected,
        mixed,
        hidden,
        partial,
        received,
        own_sem,
        line_send,
        line_recv,
        pair_send,
        pair_recv,
        row_send,
        row_recv,
        self_sem,
    ) = rest[parts:-2]
    piece_width = downs[0].shape[2]
    shards = (joined_shard, merge_shard, gate_shard, up_shard) + tuple(
        down_shard if parts == 1 else down_shard.at[:, pl.ds(i * piece_width, piece_width)]
        for i in range(parts)
    )
    slots = (joined, merge, gate, up) + tuple(downs)
    count = len(slots)
    length, part_width = tokens.shape
    width = row * part_width
    seat = lax.axis_index("tp")
    place = lax.axis_index("fs")
    half = lax.axis_index("grp")

    barrier = pltpu.get_barrier_semaphore()
    for shift in (1, -1):
        there = place + shift

        @pl.when((there >= 0) & (there < line))
        def _():
            pl.semaphore_signal(barrier, inc=1, device_id={"fs": there}, device_id_type=MESH)

    for other in range(1, copies):
        pl.semaphore_signal(
            barrier,
            inc=1,
            device_id={"grp": lax.rem(half + other, copies)},
            device_id_type=MESH,
        )
    for other in range(1, row):
        pl.semaphore_signal(
            barrier,
            inc=1,
            device_id={"tp": lax.rem(seat + other, row)},
            device_id_type=MESH,
        )
    own = [pltpu.make_async_copy(shards[k], slots[k].at[place], own_sem.at[k]) for k in range(count)]
    for copy in own:
        copy.start()
    neighbours = (place > 0).astype(jnp.int32) + (place < line - 1).astype(jnp.int32)
    mine = pltpu.make_async_copy(tokens, gathered.at[seat], self_sem)
    mine.start()
    pl.semaphore_wait(barrier, neighbours + copies - 1 + row - 1)

    def piece(k, block, part):
        rows = slots[k].shape[1] // copies
        return slots[k].at[block, pl.ds(pl.multiple_of(part * rows, rows), rows), :]

    def hop(k, way, step):
        shift = 1 if way == 0 else -1
        block = place - shift * step
        return pltpu.make_async_remote_copy(
            src_ref=piece(k, block, half),
            dst_ref=piece(k, block, half),
            send_sem=line_send.at[k, way, step],
            recv_sem=line_recv.at[k, way, step],
            device_id={"fs": place + shift},
            device_id_type=MESH,
        )

    def arrival(k, way, step):
        shift = 1 if way == 0 else -1
        block = place - shift * step
        return pltpu.make_async_remote_copy(
            src_ref=piece(k, block, half),
            dst_ref=piece(k, block, half),
            send_sem=line_send.at[k, way, step - 1],
            recv_sem=line_recv.at[k, way, step - 1],
            device_id={"fs": place - shift},
            device_id_type=MESH,
        )

    def across(k, way, step, other):
        shift = 1 if way == 0 else -1
        block = place - shift * step
        return pltpu.make_async_remote_copy(
            src_ref=piece(k, block, half),
            dst_ref=piece(k, block, half),
            send_sem=pair_send.at[k, way, step - 1, other - 1],
            recv_sem=pair_recv.at[k, way, step - 1, other - 1],
            device_id={"grp": lax.rem(half + other, copies)},
            device_id_type=MESH,
        )

    def landed(k, way, step, other):
        shift = 1 if way == 0 else -1
        block = place - shift * step
        source = lax.rem(half + copies - other, copies)
        return pltpu.make_async_remote_copy(
            src_ref=piece(k, block, source),
            dst_ref=piece(k, block, source),
            send_sem=pair_send.at[k, way, step - 1, other - 1],
            recv_sem=pair_recv.at[k, way, step - 1, other - 1],
            device_id={"grp": source},
            device_id_type=MESH,
        )

    def has(way, step):
        return place >= step if way == 0 else place + step < line

    def goes(way):
        return place < line - 1 if way == 0 else place > 0

    def launch(k):
        own[k].wait()
        for way in range(2):

            @pl.when(goes(way))
            def _():
                hop(k, way, 0).start()

    def pump(k):
        for step in range(1, line):
            for way in range(2):

                @pl.when(has(way, step))
                def _():
                    arrival(k, way, step).wait_recv()
                    for other in range(1, copies):
                        across(k, way, step, other).start()

                @pl.when(has(way, step) & goes(way))
                def _():
                    hop(k, way, step).start()

    def settle(k):
        for step in range(1, line):
            for way in range(2):

                @pl.when(has(way, step))
                def _():
                    for other in range(1, copies):
                        landed(k, way, step, other).wait_recv()

    def drain(k):
        for way in range(2):
            for step in range(line):

                @pl.when((has(way, step) if step else True) & goes(way))
                def _():
                    hop(k, way, step).wait_send()

                if step:

                    @pl.when(has(way, step))
                    def _():
                        for other in range(1, copies):
                            across(k, way, step, other).wait_send()

    def spread(source, target, stage):
        return [
            pltpu.make_async_remote_copy(
                src_ref=source,
                dst_ref=target.at[seat],
                send_sem=row_send.at[stage, other - 1],
                recv_sem=row_recv.at[stage, other - 1],
                device_id={"tp": lax.rem(seat + other, row)},
                device_id_type=MESH,
            )
            for other in range(1, row)
        ]

    def spread_in(target, stage):
        sources = [lax.rem(seat + row - other, row) for other in range(1, row)]
        return [
            pltpu.make_async_remote_copy(
                src_ref=target.at[source],
                dst_ref=target.at[source],
                send_sem=row_send.at[stage, other],
                recv_sem=row_recv.at[stage, other],
                device_id={"tp": source},
                device_id_type=MESH,
            )
            for other, source in enumerate(sources)
        ]

    def scatter(source, target, stage, other):
        there = lax.rem(seat + other, row)
        return pltpu.make_async_remote_copy(
            src_ref=source.at[there],
            dst_ref=target.at[other - 1],
            send_sem=row_send.at[stage, other - 1],
            recv_sem=row_recv.at[stage, other - 1],
            device_id={"tp": there},
            device_id_type=MESH,
        )

    def normalize(source, gain_vector):
        total = jnp.zeros((length, 1), jnp.float32)
        for t in range(row):
            widened = source[t].astype(jnp.float32)
            total = total + jnp.sum(widened * widened, axis=1, keepdims=True)
        scale = lax.rsqrt(total / width + norm_eps)
        for t in range(row):
            span = slice(t * part_width, (t + 1) * part_width)
            scaled = source[t].astype(jnp.float32) * scale * gain_vector[:, span]
            normed[:, span] = scaled.astype(jnp.bfloat16)

    def times(weight, columns):
        block = weight[:, :, columns]
        return jnp.dot(
            normed[...], block.reshape(-1, block.shape[2]), preferred_element_type=jnp.float32
        )

    def shares(rows_in, weight, target):
        step = weight.shape[2]
        for block in range(line):
            term = jnp.dot(rows_in[...], weight[block], preferred_element_type=jnp.float32)
            begin = block * step
            inner = begin % part_width
            target[begin // part_width, :, inner : inner + step] = term.astype(jnp.bfloat16)

    def finish(i):
        settle(4 + i)
        if parts == 1:
            shares(hidden, downs[i], partial_ends.at[i])
        else:
            for j in range(row):
                blocks = [jnp.dot(
                    hidden[...], downs[i][j * line // row + c], preferred_element_type=jnp.float32
                ) for c in range(max(1, line // row))]
                for c, term in enumerate(blocks):
                    partial_ends[i, j, :, c * piece_width : (c + 1) * piece_width] = term.astype(
                        jnp.bfloat16
                    )
        for other in range(1, row):
            scatter(partial_ends.at[i], received_ends.at[i], 3 + i, other).start()

    def collect(i):
        span = slice(None) if parts == 1 else slice(i * piece_width, (i + 1) * piece_width)
        total = gathered_mid[seat, :, span].astype(jnp.float32)
        total = total + partial_ends[i, seat].astype(jnp.float32)
        for other in range(1, row):
            scatter(partial_ends.at[i], received_ends.at[i], 3 + i, other).wait_recv()
            total = total + received_ends[i, other - 1].astype(jnp.float32)
        out[:, span] = total.astype(jnp.bfloat16)

    launch(0)
    first = spread(tokens, gathered, 0)
    for copy in first:
        copy.start()
    launch(1)
    mine.wait()
    for copy in spread_in(gathered, 0):
        copy.wait_recv()
    normalize(gathered, input_gain)

    pump(0)
    launch(2)
    settle(0)
    ret_width = projected.shape[2]
    for t in range(4):
        projected[t] = (
            times(joined, slice(t * ret_width, (t + 1) * ret_width))
            .astype(jnp.bfloat16)
            .astype(jnp.float32)
        )
    pump(1)
    launch(3)

    head_count = rate_ahead.shape[0]
    head_dim = ret_width // head_count
    lane = lax.broadcasted_iota(jnp.int32, (length, ret_width), 1)
    in_lower = lax.rem(lane, head_dim) < head_dim // 2

    def turned(values):
        partner = jnp.where(
            in_lower,
            pltpu.roll(values, ret_width - head_dim // 2, 1),
            pltpu.roll(values, head_dim // 2, 1),
        )
        return values * cosine[...] + partner * sine_part[...]

    queries = turned(projected[0])
    key_heads = (turned(projected[1]) * head_dim ** (-0.5)).astype(jnp.bfloat16)
    valued = projected[2]
    offset = (
        lax.broadcasted_iota(jnp.int32, (length, length), 0)
        - lax.broadcasted_iota(jnp.int32, (length, length), 1)
    ).astype(jnp.float32)
    result = jnp.zeros((length, ret_width), jnp.float32)
    for h in range(head_count):
        here = (lane >= h * head_dim) & (lane < (h + 1) * head_dim)
        scores = lax.dot_general(
            jnp.where(here, queries, 0.0).astype(jnp.bfloat16),
            key_heads,
            (((1,), (1,)), ((), ())),
            preferred_element_type=jnp.float32,
        )
        decay = jnp.exp(jnp.where(offset >= 0, rate_ahead[h] * offset, -rate_behind[h] * offset))
        result = result + jnp.dot(
            (scores * decay).astype(jnp.bfloat16),
            jnp.where(here, valued, 0.0).astype(jnp.bfloat16),
            preferred_element_type=jnp.float32,
        )
    center = jnp.zeros((length, ret_width), jnp.float32)
    for h in range(head_count):
        here = (lane >= h * head_dim) & (lane < (h + 1) * head_dim)
        mean = jnp.sum(jnp.where(here, result, 0.0), axis=1, keepdims=True) / head_dim
        center = jnp.where(here, mean, center)
    centered = result - center
    squared = centered * centered
    factor = jnp.zeros((length, ret_width), jnp.float32)
    for h in range(head_count):
        here = (lane >= h * head_dim) & (lane < (h + 1) * head_dim)
        spread_h = jnp.sum(jnp.where(here, squared, 0.0), axis=1, keepdims=True) / head_dim
        factor = jnp.where(here, lax.rsqrt(spread_h + group_eps), factor)
    gates = projected[3]
    mixed[...] = (gates / (1.0 + jnp.exp(-gates)) * (centered * factor)).astype(jnp.bfloat16)

    settle(1)
    shares(mixed, merge, partial)
    for other in range(1, row):
        scatter(partial, received, 1, other).start()
    pump(2)
    total = tokens[...].astype(jnp.float32) + partial[seat].astype(jnp.float32)
    for other in range(1, row):
        scatter(partial, received, 1, other).wait_recv()
        total = total + received[other - 1].astype(jnp.float32)
    gathered_mid[seat] = total.astype(jnp.bfloat16)
    second = spread(gathered_mid.at[seat], gathered_mid, 2)
    for copy in second:
        copy.start()
    pump(3)
    launch(4)
    if parts > 1:
        launch(5)
    for copy in spread_in(gathered_mid, 2):
        copy.wait_recv()
    normalize(gathered_mid, middle_gain)
    settle(2)
    settle(3)
    hidden_width = hidden.shape[1]
    tile = 256 if hidden_width % 256 == 0 else 128

    @pl.loop(0, hidden_width // tile)
    def _(index):
        columns = pl.ds(pl.multiple_of(index * tile, tile), tile)
        gate_act = times(gate, columns)
        up_act = times(up, columns)
        hidden[:, columns] = (gate_act / (1.0 + jnp.exp(-gate_act)) * up_act).astype(jnp.bfloat16)

    for i in range(parts):
        pump(4 + i)
        if i + 2 < parts:
            launch(6 + i)
        if i:
            finish(i - 1)
    finish(parts - 1)
    for i in range(parts):
        collect(i)
    for copy in first + second:
        copy.wait_send()
    for other in range(1, row):
        scatter(partial, received, 1, other).wait_send()
        for i in range(parts):
            scatter(partial_ends.at[i], received_ends.at[i], 3 + i, other).wait_send()
    for k in range(count):
        drain(k)


def paired_kernel(
    sizes,
    tokens,
    input_gain,
    middle_gain,
    rate_ahead,
    rate_behind,
    cosine,
    sine_part,
    query_shard,
    key_shard,
    value_shard,
    output_gate_shard,
    merge_shard,
    gate_shard,
    up_shard,
    down_shard,
    out,
    joined_out,
    merge_out,
    gate_out,
    up_out,
    down_out,
    joined,
    merge,
    gate,
    up,
    down,
    gathered,
    gathered_mid,
    normed,
    projected,
    mixed,
    hidden,
    first_partial,
    first_core,
    first_row,
    first_line,
    last_partial,
    last_core,
    last_row,
    last_line,
    own_sem,
    line_send,
    line_recv,
    pair_send,
    pair_recv,
    share_send,
    share_recv,
    sum_send,
    sum_recv,
):
    line, row = sizes["fs"], sizes["tp"]
    pieces = down.shape[0]
    piece_width = down.shape[3]
    length, part_width = tokens.shape
    width = row * part_width
    seat = lax.axis_index("tp")
    place = lax.axis_index("fs")
    half = lax.axis_index("grp")
    core, column = lax.rem(seat, 2), seat // 2
    slot = lax.rem(place, 2)
    core_peer = seat + 1 - 2 * core
    row_peer = lax.rem(seat + 2, row)
    far_peer = lax.rem(core_peer + 2, row)
    line_peer = place + 1 - 2 * slot
    sign = 1 - 2 * (place // (line // 2))
    others = [lax.rem(place + sign * step + line, line) for step in range(1, line)]

    barrier = pltpu.get_barrier_semaphore()
    for there in others:
        pl.semaphore_signal(barrier, inc=1, device_id={"fs": there}, device_id_type=MESH)
    pl.semaphore_signal(barrier, inc=1, device_id={"grp": 1 - half}, device_id_type=MESH)
    for there in (core_peer, row_peer):
        pl.semaphore_signal(barrier, inc=1, device_id={"tp": there}, device_id_type=MESH)

    group = joined_out.shape[2] // 4
    quads = (query_shard, key_shard, value_shard, output_gate_shard)
    merge_rows = merge.shape[1]
    hidden_half = gate.shape[2]

    def cut(ref, axis, part, size):
        window = pl.ds(pl.multiple_of(part * size, size), size)
        return ref.at[window] if axis == 0 else ref.at[:, window]

    loads = [
        [
            (quad.at[:, p * group : (p + 1) * group], joined_out.at[p, :, i * group : (i + 1) * group])
            for p in range(2)
            for i, quad in enumerate(quads)
        ],
        [(merge_shard, merge_out)],
        [(gate_shard, gate_out)],
        [(up_shard, up_out)],
        [(down_shard, down_out)],
        [
            (cut(quad, 1, slot, group), joined.at[place, :, i * group : (i + 1) * group])
            for i, quad in enumerate(quads)
        ],
        [(cut(merge_shard, 0, slot, merge_rows), merge.at[place])],
        [(cut(gate_shard, 1, slot, hidden_half), gate.at[place])],
        [(cut(up_shard, 1, slot, hidden_half), up.at[place])],
        [
            (
                cut(down_shard, 0, slot, hidden_half).at[:, i * piece_width : (i + 1) * piece_width],
                down.at[i, place],
            )
            for i in range(pieces)
        ],
    ]
    own, index = [], 0
    for pairs in loads:
        own.append([])
        for source, target in pairs:
            own[-1].append(pltpu.make_async_copy(source, target, own_sem.at[index]))
            index += 1
    for copies in own:
        for copy in copies:
            copy.start()
    gathered[slot, seat] = tokens[...]
    pl.semaphore_wait(barrier, line - 1 + 1 + 2)

    def ready(k):
        for copy in own[k]:
            copy.wait()

    def outgoing(k, parity):
        if k == 0:
            size = joined.shape[1] // 2
            return joined_out.at[parity, pl.ds(pl.multiple_of(half * size, size), size)]
        if k == 1:
            size = merge_rows // 2
            return cut(merge_out, 0, parity * 2 + half, size)
        if k < 4:
            source = (gate_out, up_out)[k - 2]
            size = source.shape[0] // 2
            return cut(source, 0, half, size).at[
                :, pl.ds(pl.multiple_of(parity * hidden_half, hidden_half), hidden_half)
            ]
        size = hidden_half // 2
        return cut(down_out, 0, parity * 2 + half, size).at[
            :, (k - 4) * piece_width : (k - 3) * piece_width
        ]

    def landing(k, block, part):
        target = (joined, merge, gate, up)[k] if k < 4 else down.at[k - 4]
        size = target.shape[1] // 2
        return target.at[block, pl.ds(pl.multiple_of(part * size, size), size)]

    def post(k, there):
        return pltpu.make_async_remote_copy(
            src_ref=outgoing(k, lax.rem(there, 2)),
            dst_ref=landing(k, place, half),
            send_sem=line_send.at[k, there],
            recv_sem=line_recv.at[k, place],
            device_id={"fs": there},
            device_id_type=MESH,
        )

    def arrival(k, block):
        return pltpu.make_async_remote_copy(
            src_ref=landing(k, block, half),
            dst_ref=landing(k, block, half),
            send_sem=line_send.at[k, block],
            recv_sem=line_recv.at[k, block],
            device_id={"fs": block},
            device_id_type=MESH,
        )

    def across(k, block, part):
        return pltpu.make_async_remote_copy(
            src_ref=landing(k, block, part),
            dst_ref=landing(k, block, part),
            send_sem=pair_send.at[k, block],
            recv_sem=pair_recv.at[k, block],
            device_id={"grp": 1 - half},
            device_id_type=MESH,
        )

    def launch(k):
        ready(k)
        for there in others:
            post(k, there).start()

    def pump(k, block):
        arrival(k, block).wait_recv()
        across(k, block, half).start()

    def settle(k):
        for block in others:
            across(k, block, 1 - half).wait_recv()

    def handed(source, target, stage, step):
        plane = slot if step in (0, 1, 2, 3) else 1 - slot
        holder = seat if step in (0, 1, 2, 4, 5) else row_peer
        place_in = target.at[plane, holder]
        peer = {"tp": core_peer}
        if step in (1, 5):
            peer = {"tp": row_peer}
        if step == 2:
            peer = {"fs": line_peer}
        return pltpu.make_async_remote_copy(
            src_ref=source if step < 3 else place_in,
            dst_ref=place_in,
            send_sem=share_send.at[stage, step],
            recv_sem=share_recv.at[stage, step],
            device_id=peer,
            device_id_type=MESH,
        )

    def received(target, stage, step):
        plane = slot if step in (0, 1, 3) else 1 - slot
        holder = (core_peer, row_peer, seat, far_peer, core_peer, row_peer, far_peer)[step]
        place_in = target.at[plane, holder]
        return pltpu.make_async_remote_copy(
            src_ref=place_in,
            dst_ref=place_in,
            send_sem=share_send.at[stage, step],
            recv_sem=share_recv.at[stage, step],
            device_id={"tp": core_peer},
            device_id_type=MESH,
        )

    def normalize(source, gain_vector, plane):
        total = jnp.zeros((length, 1), jnp.float32)
        for t in range(row):
            widened = source[plane, t].astype(jnp.float32)
            total = total + jnp.sum(widened * widened, axis=1, keepdims=True)
        scale = lax.rsqrt(total / width + norm_eps)
        for t in range(row):
            span = slice(t * part_width, (t + 1) * part_width)
            scaled = source[plane, t].astype(jnp.float32) * scale * gain_vector[:, span]
            normed[plane, :, span] = scaled.astype(jnp.bfloat16)

    def hand_over(source, target, stage):
        return [handed(source, target, stage, step) for step in range(7)]

    def moved(source, target, peer, stage, step):
        return pltpu.make_async_remote_copy(
            src_ref=source,
            dst_ref=target,
            send_sem=sum_send.at[stage, step],
            recv_sem=sum_recv.at[stage, step],
            device_id=peer,
            device_id_type=MESH,
        )

    def share_mid(step):
        plane, kind = step % 2, step // 2
        spot = gathered_mid.at[plane, row_peer if kind == 2 else seat]
        return pltpu.make_async_remote_copy(
            src_ref=spot,
            dst_ref=spot,
            send_sem=share_send.at[1, step],
            recv_sem=share_recv.at[1, step],
            device_id={"tp": core_peer if kind else row_peer},
            device_id_type=MESH,
        )

    def shared_mid(step):
        plane, kind = step % 2, step // 2
        spot = gathered_mid.at[plane, (row_peer, core_peer, far_peer)[kind]]
        return pltpu.make_async_remote_copy(
            src_ref=spot,
            dst_ref=spot,
            send_sem=share_send.at[1, step],
            recv_sem=share_recv.at[1, step],
            device_id={"tp": core_peer},
            device_id_type=MESH,
        )

    def reducer(partial, core_in, row_in, stage):
        order = (0, 1) if stage == 0 else (1 - slot, slot)
        return [moved(partial.at[1 - core], core_in, {"tp": core_peer}, stage, 0)] + [
            moved(
                partial.at[core, 1 - column, plane],
                row_in.at[step],
                {"tp": row_peer},
                stage,
                1 + step,
            )
            for step, plane in enumerate(order)
        ]

    def add_core(partial, core_in, steps, order):
        steps[0].wait_recv()
        for step, plane in enumerate(order):
            total = partial[core, 1 - column, plane].astype(jnp.float32) + core_in[
                1 - column, plane
            ].astype(jnp.float32)
            partial[core, 1 - column, plane] = total.astype(jnp.bfloat16)
            steps[1 + step].start()

    def add_row(partial, core_in, row_in, steps, step, plane):
        steps[1 + step].wait_recv()
        return (
            partial[core, column, plane].astype(jnp.float32)
            + core_in[column, plane].astype(jnp.float32)
            + row_in[step].astype(jnp.float32)
        )

    first = hand_over(tokens, gathered, 0)
    for step in (2, 1, 0):
        first[step].start()
    launch(0)
    launch(1)
    launch(2)
    launch(3)
    received(gathered, 0, 1).wait_recv()
    first[3].start()
    received(gathered, 0, 2).wait_recv()
    first[5].start()
    first[4].start()
    received(gathered, 0, 0).wait_recv()
    received(gathered, 0, 3).wait_recv()
    normalize(gathered, input_gain, slot)
    for block in others:
        pump(0, block)
    received(gathered, 0, 5).wait_recv()
    first[6].start()
    received(gathered, 0, 4).wait_recv()
    received(gathered, 0, 6).wait_recv()
    normalize(gathered, input_gain, 1 - slot)
    for block in others:
        pump(1, block)
    ready(5)
    settle(0)
    for plane in range(2):
        rows_out = jnp.dot(
            normed[plane], joined[...].reshape(width, 4 * group), preferred_element_type=jnp.float32
        )
        for i in range(4):
            projected[i, plane] = (
                rows_out[:, i * group : (i + 1) * group].astype(jnp.bfloat16).astype(jnp.float32)
            )

    head_count = rate_ahead.shape[0] // 2
    head_dim = group // head_count
    lane = lax.broadcasted_iota(jnp.int32, (length, group), 1)
    in_lower = lax.rem(lane, head_dim) < head_dim // 2

    def turned(values):
        partner = jnp.where(
            in_lower,
            pltpu.roll(values, group - head_dim // 2, 1),
            pltpu.roll(values, head_dim // 2, 1),
        )
        return values * cosine[...] + partner * sine_part[...]

    offset = (
        lax.broadcasted_iota(jnp.int32, (length, length), 0)
        - lax.broadcasted_iota(jnp.int32, (length, length), 1)
    ).astype(jnp.float32)
    decays = [
        jnp.exp(
            jnp.where(
                offset >= 0,
                rate_ahead[slot * head_count + h] * offset,
                -rate_behind[slot * head_count + h] * offset,
            )
        )
        for h in range(head_count)
    ]
    here = [(lane >= h * head_dim) & (lane < (h + 1) * head_dim) for h in range(head_count)]
    for plane in range(2):
        queries = turned(projected[0, plane])
        key_heads = (turned(projected[1, plane]) * head_dim ** (-0.5)).astype(jnp.bfloat16)
        valued = projected[2, plane]
        result = jnp.zeros((length, group), jnp.float32)
        for h in range(head_count):
            scores = lax.dot_general(
                jnp.where(here[h], queries, 0.0).astype(jnp.bfloat16),
                key_heads,
                (((1,), (1,)), ((), ())),
                preferred_element_type=jnp.float32,
            )
            result = result + jnp.dot(
                (scores * decays[h]).astype(jnp.bfloat16),
                jnp.where(here[h], valued, 0.0).astype(jnp.bfloat16),
                preferred_element_type=jnp.float32,
            )
        center = jnp.zeros((length, group), jnp.float32)
        for h in range(head_count):
            mean = jnp.sum(jnp.where(here[h], result, 0.0), axis=1, keepdims=True) / head_dim
            center = jnp.where(here[h], mean, center)
        centered = result - center
        squared = centered * centered
        factor = jnp.zeros((length, group), jnp.float32)
        for h in range(head_count):
            spread_h = jnp.sum(jnp.where(here[h], squared, 0.0), axis=1, keepdims=True) / head_dim
            factor = jnp.where(here[h], lax.rsqrt(spread_h + group_eps), factor)
        gates = projected[3, plane]
        mixed[plane] = (gates / (1.0 + jnp.exp(-gates)) * (centered * factor)).astype(jnp.bfloat16)

    ready(6)
    settle(1)

    def fill(rows_in, weight, partial, side):
        for x in range(row // 2):
            block = x * 2 + side
            for plane in range(2):
                term = jnp.dot(rows_in[plane], weight[block], preferred_element_type=jnp.float32)
                partial[side, x, plane] = term.astype(jnp.bfloat16)

    steps = reducer(first_partial, first_core, first_row, 0) + [
        moved(first_partial.at[core, column, plane], first_line.at[plane], {"fs": line_peer}, 0, 3 + plane)
        for plane in range(2)
    ]
    fill(mixed, merge, first_partial, 1 - core)
    steps[0].start()
    fill(mixed, merge, first_partial, core)
    add_core(first_partial, first_core, steps, (0, 1))
    for block in others:
        pump(2, block)
    for plane in range(2):
        total = add_row(first_partial, first_core, first_row, steps, plane, plane)
        first_partial[core, column, plane] = total.astype(jnp.bfloat16)
        steps[3 + plane].start()
    ready(4)
    for i in range(pieces):
        for there in others:
            post(4 + i, there).start()

    second = [share_mid(step) for step in range(6)]
    pump(3, others[0])
    for plane in range(2):
        steps[3 + plane].wait_recv()
        total = gathered[plane, seat].astype(jnp.float32) + (
            first_partial[core, column, plane].astype(jnp.float32)
            + first_line[plane].astype(jnp.float32)
        )
        gathered_mid[plane, seat] = total.astype(jnp.bfloat16)
        second[plane].start()
        second[2 + plane].start()
        pump(3, others[1 + plane])
    queue = [(4 + i, block) for i in range(pieces) for block in others]

    def pump_next(count):
        for _ in range(count):
            pump(*queue.pop(0))

    for plane in range(2):
        shared_mid(plane).wait_recv()
        second[4 + plane].start()
    for plane in range(2):
        shared_mid(2 + plane).wait_recv()
        shared_mid(4 + plane).wait_recv()
        normalize(gathered_mid, middle_gain, plane)
    pump_next(len(others))
    ready(7)
    ready(8)
    settle(2)
    settle(3)
    tile = 256
    for plane in range(2):
        for begin in range(0, hidden_half, tile):
            columns = slice(begin, min(begin + tile, hidden_half))
            gate_act, up_act = [
                jnp.dot(
                    normed[plane],
                    weight[:, :, columns].reshape(width, -1),
                    preferred_element_type=jnp.float32,
                )
                for weight in (gate, up)
            ]
            hidden[plane, :, columns] = (gate_act / (1.0 + jnp.exp(-gate_act)) * up_act).astype(
                jnp.bfloat16
            )
    pump_next(len(others))

    ready(9)
    ends = [
        reducer(last_partial.at[i], last_core.at[i], last_row.at[i], 1 + i)
        + [
            moved(
                last_partial.at[i, core, column, 1 - slot],
                last_line.at[i],
                {"fs": line_peer},
                1 + i,
                3,
            )
        ]
        for i in range(pieces)
    ]

    def pass_line(i):
        total = add_row(
            last_partial.at[i], last_core.at[i], last_row.at[i], ends[i], 0, 1 - slot
        )
        last_partial[i, core, column, 1 - slot] = total.astype(jnp.bfloat16)
        ends[i][3].start()

    def finish(i):
        span = slice(i * piece_width, (i + 1) * piece_width)
        total = gathered_mid[slot, seat, :, span].astype(jnp.float32) + add_row(
            last_partial.at[i], last_core.at[i], last_row.at[i], ends[i], 1, slot
        )
        ends[i][3].wait_recv()
        out[:, span] = (total + last_line[i].astype(jnp.float32)).astype(jnp.bfloat16)

    for i in range(pieces):
        if i + 1 < pieces and queue and queue[0][0] == 5 + i:
            pump_next(len(others))
        settle(4 + i)
        fill(hidden, down.at[i], last_partial.at[i], 1 - core)
        ends[i][0].start()
        fill(hidden, down.at[i], last_partial.at[i], core)
        add_core(last_partial.at[i], last_core.at[i], ends[i], (1 - slot, slot))
        if i:
            pass_line(i - 1)
    pass_line(pieces - 1)
    for i in range(pieces):
        finish(i)

    for copy in first + second + steps:
        copy.wait_send()
    for group_steps in ends:
        for copy in group_steps:
            copy.wait_send()
    for k in range(4 + pieces):
        for there in others:
            post(k, there).wait_send()
            across(k, there, half).wait_send()


def paired_call(
    sizes, flat, input_gain, middle_gain, rates, tables, quads, merge_weight, gate_weight, up_weight, down_weight
):
    line, row = sizes["fs"], sizes["tp"]
    bf16 = jnp.bfloat16
    length, part_width = flat.shape
    depth, ret_width = quads[0].shape
    hidden_half, group = gate_weight.shape[1] // 2, ret_width // 2
    pieces = 4
    piece_width = down_weight.shape[1] // pieces
    kinds = 4 + pieces
    in_vmem = pl.BlockSpec(memory_space=pltpu.VMEM)
    in_smem = pl.BlockSpec(memory_space=pltpu.SMEM)

    def sums(lead, columns, last):
        return [
            pltpu.VMEM(lead + (2, row // 2, 2, length, columns), bf16),
            pltpu.VMEM(lead + (row // 2, 2, length, columns), bf16),
            pltpu.VMEM(lead + (2, length, columns), bf16),
            pltpu.VMEM(lead + last + (length, columns), bf16),
        ]

    dma = pltpu.SemaphoreType.DMA
    return pl.pallas_call(
        functools.partial(paired_kernel, sizes),
        out_shape=jax.ShapeDtypeStruct(flat.shape, bf16),
        in_specs=[in_vmem] * 3
        + [in_smem] * 2
        + [in_vmem] * 2
        + [pl.BlockSpec(memory_space=pl.ANY)] * 8,
        out_specs=in_vmem,
        scratch_shapes=[
            pltpu.VMEM((2, depth, 4 * group), bf16),
            pltpu.VMEM(merge_weight.shape, bf16),
            pltpu.VMEM(gate_weight.shape, bf16),
            pltpu.VMEM(up_weight.shape, bf16),
            pltpu.VMEM(down_weight.shape, bf16),
            pltpu.VMEM((line, depth, 4 * group), bf16),
            pltpu.VMEM((line, merge_weight.shape[0] // 2, part_width), bf16),
            pltpu.VMEM((line, depth, hidden_half), bf16),
            pltpu.VMEM((line, depth, hidden_half), bf16),
            pltpu.VMEM((pieces, line, hidden_half, piece_width), bf16),
            pltpu.VMEM((2, row, length, part_width), bf16),
            pltpu.VMEM((2, row, length, part_width), bf16),
            pltpu.VMEM((2, length, row * part_width), bf16),
            pltpu.VMEM((4, 2, length, group), jnp.float32),
            pltpu.VMEM((2, length, group), bf16),
            pltpu.VMEM((2, length, hidden_half), bf16),
        ]
        + sums((), part_width, (2,))
        + sums((pieces,), piece_width, ())
        + [
            dma((20 + pieces,)),
            dma((kinds, line)),
            dma((kinds, line)),
            dma((kinds, line)),
            dma((kinds, line)),
            dma((2, 7)),
            dma((2, 7)),
            dma((1 + pieces, 5)),
            dma((1 + pieces, 5)),
        ],
        compiler_params=pltpu.CompilerParams(
            collective_id=0, has_side_effects=True, vmem_limit_bytes=60 << 20
        ),
    )(
        flat,
        input_gain[None, :],
        middle_gain[None, :],
        *rates,
        *tables,
        *quads,
        merge_weight,
        gate_weight,
        up_weight,
        down_weight,
    )


def on_device(
    sizes,
    tokens,
    input_gain,
    query_weight,
    key_weight,
    value_weight,
    output_gate_matrix,
    forward_decay,
    backward_decay,
    merge_weight,
    middle_gain,
    gate_weight,
    up_weight,
    down_weight,
):
    seq_count, length, part_width = tokens.shape
    flat = tokens.reshape(seq_count * length, part_width)
    quads = (query_weight, key_weight, value_weight, output_gate_matrix)
    paired = (
        sizes["grp"] == 2
        and sizes["fs"] == sizes["tp"] == 4
        and seq_count == 1
        and query_weight.shape[1] % 256 == 0
        and forward_decay.shape[0] % 2 == 0
        and gate_weight.shape[1] % 256 == 0
        and down_weight.shape[1] == part_width
        and part_width % 256 == 0
    )
    if paired:
        head_count = forward_decay.shape[0] // 2
        head_dim = query_weight.shape[1] // (2 * head_count)
        layer_out = paired_call(
            sizes,
            flat,
            input_gain,
            middle_gain,
            (jax.nn.log_sigmoid(forward_decay), jax.nn.log_sigmoid(backward_decay)),
            turn_tables(length, head_dim, head_count),
            quads,
            merge_weight,
            gate_weight,
            up_weight,
            down_weight,
        )
        return layer_out.reshape(seq_count, length, part_width)
    joined = jnp.concatenate(quads, axis=1)
    shards = (joined, merge_weight, gate_weight, up_weight, down_weight)
    line, copies, row = sizes["fs"], sizes["grp"], sizes["tp"]
    down_width = down_weight.shape[1]
    parts = down_width // 256 if line == row and down_width % 256 == 0 else 1
    down_piece = jax.ShapeDtypeStruct((down_weight.shape[0], down_width // parts), jnp.bfloat16)
    landing = shards[:4] + (down_piece,) * parts
    count = len(landing)
    width, ret_width, hidden_width = row * part_width, query_weight.shape[1], gate_weight.shape[1]
    head_count = forward_decay.shape[0]
    tables = turn_tables(length, ret_width // head_count, head_count)
    in_vmem = pl.BlockSpec(memory_space=pltpu.VMEM)
    in_smem = pl.BlockSpec(memory_space=pltpu.SMEM)
    bf16 = jnp.bfloat16
    layer_out = pl.pallas_call(
        functools.partial(layer_kernel, sizes),
        out_shape=jax.ShapeDtypeStruct(flat.shape, bf16),
        in_specs=[in_vmem] * 3
        + [in_smem] * 2
        + [in_vmem] * 2
        + [pl.BlockSpec(memory_space=pl.ANY)] * len(shards),
        out_specs=in_vmem,
        scratch_shapes=[pltpu.VMEM((line,) + w.shape, w.dtype) for w in landing]
        + [
            pltpu.VMEM((row, length, part_width), bf16),
            pltpu.VMEM((row, length, part_width), bf16),
            pltpu.VMEM((length, width), bf16),
            pltpu.VMEM((4, length, ret_width), jnp.float32),
            pltpu.VMEM((length, ret_width), bf16),
            pltpu.VMEM((length, hidden_width), bf16),
            pltpu.VMEM((row, length, part_width), bf16),
            pltpu.VMEM((row - 1, length, part_width), bf16),
            pltpu.SemaphoreType.DMA((count,)),
            pltpu.SemaphoreType.DMA((count, 2, line)),
            pltpu.SemaphoreType.DMA((count, 2, line)),
            pltpu.SemaphoreType.DMA((count, 2, line, copies - 1)),
            pltpu.SemaphoreType.DMA((count, 2, line, copies - 1)),
            pltpu.SemaphoreType.DMA((3 + parts, row - 1)),
            pltpu.SemaphoreType.DMA((3 + parts, row - 1)),
            pltpu.SemaphoreType.DMA,
            pltpu.VMEM((parts, row, length, part_width // parts), bf16),
            pltpu.VMEM((parts, row - 1, length, part_width // parts), bf16),
        ],
        compiler_params=pltpu.CompilerParams(
            collective_id=0, has_side_effects=True, vmem_limit_bytes=58 << 20
        ),
    )(
        flat,
        input_gain[None, :],
        middle_gain[None, :],
        jax.nn.log_sigmoid(forward_decay),
        jax.nn.log_sigmoid(backward_decay),
        *tables,
        *shards,
    )
    return layer_out.reshape(seq_count, length, part_width)


def solution(mesh):
    placed = (
        P(("grp", "fs"), None, "tp"),
        P(),
        P("fs", "tp"),
        P("fs", "tp"),
        P("fs", "tp"),
        P("fs", "tp"),
        P("tp"),
        P("tp"),
        P("tp", "fs"),
        P(),
        P("fs", "tp"),
        P("fs", "tp"),
        P("tp", "fs"),
    )
    return jax.shard_map(
        functools.partial(on_device, dict(mesh.shape)),
        mesh=mesh,
        in_specs=placed,
        out_specs=P(("grp", "fs"), None, "tp"),
        check_vma=False,
    )
```

```python
import functools

import jax
import jax.numpy as jnp
import numpy as np
from jax import lax
from jax.experimental import pallas as pl
from jax.experimental.pallas import tpu as pltpu
from jax.sharding import PartitionSpec as P

norm_eps = 1e-06
group_eps = 1e-05
rope_base = 10000.0


def turn_tables(length, head_dim, head_count):
    half_dim = head_dim // 2
    inverse = rope_base ** (-np.arange(half_dim) / half_dim)
    angles = np.arange(length)[:, None] * inverse[None, :]
    cosine, sine_part = np.cos(angles), np.sin(angles)
    return (
        np.tile(np.concatenate([cosine, cosine], axis=1), (1, head_count)).astype(np.float32),
        np.tile(np.concatenate([-sine_part, sine_part], axis=1), (1, head_count)).astype(np.float32),
    )


MESH = pl.DeviceIdType.MESH


def layer_kernel(
    sizes,
    tokens,
    input_gain,
    middle_gain,
    rate_ahead,
    rate_behind,
    cosine,
    sine_part,
    joined_shard,
    merge_shard,
    gate_shard,
    up_shard,
    down_shard,
    out,
    joined,
    merge,
    gate,
    up,
    *rest,
):
    line, copies, row = sizes["fs"], sizes["grp"], sizes["tp"]
    parts = len(rest) - 18
    downs, partial_ends, received_ends = rest[:parts], rest[-2], rest[-1]
    (
        gathered,
        gathered_mid,
        normed,
        projected,
        mixed,
        hidden,
        partial,
        received,
        own_sem,
        line_send,
        line_recv,
        pair_send,
        pair_recv,
        row_send,
        row_recv,
        self_sem,
    ) = rest[parts:-2]
    piece_width = downs[0].shape[2]
    shards = (joined_shard, merge_shard, gate_shard, up_shard) + tuple(
        down_shard if parts == 1 else down_shard.at[:, pl.ds(i * piece_width, piece_width)]
        for i in range(parts)
    )
    slots = (joined, merge, gate, up) + tuple(downs)
    count = len(slots)
    length, part_width = tokens.shape
    width = row * part_width
    seat = lax.axis_index("tp")
    place = lax.axis_index("fs")
    half = lax.axis_index("grp")

    barrier = pltpu.get_barrier_semaphore()
    for shift in (1, -1):
        there = place + shift

        @pl.when((there >= 0) & (there < line))
        def _():
            pl.semaphore_signal(barrier, inc=1, device_id={"fs": there}, device_id_type=MESH)

    for other in range(1, copies):
        pl.semaphore_signal(
            barrier,
            inc=1,
            device_id={"grp": lax.rem(half + other, copies)},
            device_id_type=MESH,
        )
    for other in range(1, row):
        pl.semaphore_signal(
            barrier,
            inc=1,
            device_id={"tp": lax.rem(seat + other, row)},
            device_id_type=MESH,
        )
    own = [pltpu.make_async_copy(shards[k], slots[k].at[place], own_sem.at[k]) for k in range(count)]
    for copy in own:
        copy.start()
    neighbours = (place > 0).astype(jnp.int32) + (place < line - 1).astype(jnp.int32)
    mine = pltpu.make_async_copy(tokens, gathered.at[seat], self_sem)
    mine.start()
    pl.semaphore_wait(barrier, neighbours + copies - 1 + row - 1)

    def piece(k, block, part):
        rows = slots[k].shape[1] // copies
        return slots[k].at[block, pl.ds(pl.multiple_of(part * rows, rows), rows), :]

    def hop(k, way, step):
        shift = 1 if way == 0 else -1
        block = place - shift * step
        return pltpu.make_async_remote_copy(
            src_ref=piece(k, block, half),
            dst_ref=piece(k, block, half),
            send_sem=line_send.at[k, way, step],
            recv_sem=line_recv.at[k, way, step],
            device_id={"fs": place + shift},
            device_id_type=MESH,
        )

    def arrival(k, way, step):
        shift = 1 if way == 0 else -1
        block = place - shift * step
        return pltpu.make_async_remote_copy(
            src_ref=piece(k, block, half),
            dst_ref=piece(k, block, half),
            send_sem=line_send.at[k, way, step - 1],
            recv_sem=line_recv.at[k, way, step - 1],
            device_id={"fs": place - shift},
            device_id_type=MESH,
        )

    def across(k, way, step, other):
        shift = 1 if way == 0 else -1
        block = place - shift * step
        return pltpu.make_async_remote_copy(
            src_ref=piece(k, block, half),
            dst_ref=piece(k, block, half),
            send_sem=pair_send.at[k, way, step - 1, other - 1],
            recv_sem=pair_recv.at[k, way, step - 1, other - 1],
            device_id={"grp": lax.rem(half + other, copies)},
            device_id_type=MESH,
        )

    def landed(k, way, step, other):
        shift = 1 if way == 0 else -1
        block = place - shift * step
        source = lax.rem(half + copies - other, copies)
        return pltpu.make_async_remote_copy(
            src_ref=piece(k, block, source),
            dst_ref=piece(k, block, source),
            send_sem=pair_send.at[k, way, step - 1, other - 1],
            recv_sem=pair_recv.at[k, way, step - 1, other - 1],
            device_id={"grp": source},
            device_id_type=MESH,
        )

    def has(way, step):
        return place >= step if way == 0 else place + step < line

    def goes(way):
        return place < line - 1 if way == 0 else place > 0

    def launch(k):
        own[k].wait()
        for way in range(2):

            @pl.when(goes(way))
            def _():
                hop(k, way, 0).start()

    def pump(k):
        for step in range(1, line):
            for way in range(2):

                @pl.when(has(way, step))
                def _():
                    arrival(k, way, step).wait_recv()
                    for other in range(1, copies):
                        across(k, way, step, other).start()

                @pl.when(has(way, step) & goes(way))
                def _():
                    hop(k, way, step).start()

    def settle(k):
        for step in range(1, line):
            for way in range(2):

                @pl.when(has(way, step))
                def _():
                    for other in range(1, copies):
                        landed(k, way, step, other).wait_recv()

    def drain(k):
        for way in range(2):
            for step in range(line):

                @pl.when((has(way, step) if step else True) & goes(way))
                def _():
                    hop(k, way, step).wait_send()

                if step:

                    @pl.when(has(way, step))
                    def _():
                        for other in range(1, copies):
                            across(k, way, step, other).wait_send()

    def spread(source, target, stage):
        return [
            pltpu.make_async_remote_copy(
                src_ref=source,
                dst_ref=target.at[seat],
                send_sem=row_send.at[stage, other - 1],
                recv_sem=row_recv.at[stage, other - 1],
                device_id={"tp": lax.rem(seat + other, row)},
                device_id_type=MESH,
            )
            for other in range(1, row)
        ]

    def spread_in(target, stage):
        sources = [lax.rem(seat + row - other, row) for other in range(1, row)]
        return [
            pltpu.make_async_remote_copy(
                src_ref=target.at[source],
                dst_ref=target.at[source],
                send_sem=row_send.at[stage, other],
                recv_sem=row_recv.at[stage, other],
                device_id={"tp": source},
                device_id_type=MESH,
            )
            for other, source in enumerate(sources)
        ]

    def scatter(source, target, stage, other):
        there = lax.rem(seat + other, row)
        return pltpu.make_async_remote_copy(
            src_ref=source.at[there],
            dst_ref=target.at[other - 1],
            send_sem=row_send.at[stage, other - 1],
            recv_sem=row_recv.at[stage, other - 1],
            device_id={"tp": there},
            device_id_type=MESH,
        )

    def normalize(source, gain_vector):
        total = jnp.zeros((length, 1), jnp.float32)
        for t in range(row):
            widened = source[t].astype(jnp.float32)
            total = total + jnp.sum(widened * widened, axis=1, keepdims=True)
        scale = lax.rsqrt(total / width + norm_eps)
        for t in range(row):
            span = slice(t * part_width, (t + 1) * part_width)
            scaled = source[t].astype(jnp.float32) * scale * gain_vector[:, span]
            normed[:, span] = scaled.astype(jnp.bfloat16)

    def times(weight, columns):
        block = weight[:, :, columns]
        return jnp.dot(
            normed[...], block.reshape(-1, block.shape[2]), preferred_element_type=jnp.float32
        )

    def shares(rows_in, weight, target):
        step = weight.shape[2]
        for block in range(line):
            term = jnp.dot(rows_in[...], weight[block], preferred_element_type=jnp.float32)
            begin = block * step
            inner = begin % part_width
            target[begin // part_width, :, inner : inner + step] = term.astype(jnp.bfloat16)

    def finish(i):
        settle(4 + i)
        if parts == 1:
            shares(hidden, downs[i], partial_ends.at[i])
        else:
            for j in range(row):
                blocks = [jnp.dot(
                    hidden[...], downs[i][j * line // row + c], preferred_element_type=jnp.float32
                ) for c in range(max(1, line // row))]
                for c, term in enumerate(blocks):
                    partial_ends[i, j, :, c * piece_width : (c + 1) * piece_width] = term.astype(
                        jnp.bfloat16
                    )
        for other in range(1, row):
            scatter(partial_ends.at[i], received_ends.at[i], 3 + i, other).start()

    def collect(i):
        span = slice(None) if parts == 1 else slice(i * piece_width, (i + 1) * piece_width)
        total = gathered_mid[seat, :, span].astype(jnp.float32)
        total = total + partial_ends[i, seat].astype(jnp.float32)
        for other in range(1, row):
            scatter(partial_ends.at[i], received_ends.at[i], 3 + i, other).wait_recv()
            total = total + received_ends[i, other - 1].astype(jnp.float32)
        out[:, span] = total.astype(jnp.bfloat16)

    launch(0)
    first = spread(tokens, gathered, 0)
    for copy in first:
        copy.start()
    launch(1)
    mine.wait()
    for copy in spread_in(gathered, 0):
        copy.wait_recv()
    normalize(gathered, input_gain)

    pump(0)
    launch(2)
    settle(0)
    ret_width = projected.shape[2]
    for t in range(4):
        projected[t] = (
            times(joined, slice(t * ret_width, (t + 1) * ret_width))
            .astype(jnp.bfloat16)
            .astype(jnp.float32)
        )
    pump(1)
    launch(3)

    head_count = rate_ahead.shape[0]
    head_dim = ret_width // head_count
    lane = lax.broadcasted_iota(jnp.int32, (length, ret_width), 1)
    in_lower = lax.rem(lane, head_dim) < head_dim // 2

    def turned(values):
        partner = jnp.where(
            in_lower,
            pltpu.roll(values, ret_width - head_dim // 2, 1),
            pltpu.roll(values, head_dim // 2, 1),
        )
        return values * cosine[...] + partner * sine_part[...]

    queries = turned(projected[0])
    key_heads = (turned(projected[1]) * head_dim ** (-0.5)).astype(jnp.bfloat16)
    valued = projected[2]
    offset = (
        lax.broadcasted_iota(jnp.int32, (length, length), 0)
        - lax.broadcasted_iota(jnp.int32, (length, length), 1)
    ).astype(jnp.float32)
    result = jnp.zeros((length, ret_width), jnp.float32)
    for h in range(head_count):
        here = (lane >= h * head_dim) & (lane < (h + 1) * head_dim)
        scores = lax.dot_general(
            jnp.where(here, queries, 0.0).astype(jnp.bfloat16),
            key_heads,
            (((1,), (1,)), ((), ())),
            preferred_element_type=jnp.float32,
        )
        decay = jnp.exp(jnp.where(offset >= 0, rate_ahead[h] * offset, -rate_behind[h] * offset))
        result = result + jnp.dot(
            (scores * decay).astype(jnp.bfloat16),
            jnp.where(here, valued, 0.0).astype(jnp.bfloat16),
            preferred_element_type=jnp.float32,
        )
    center = jnp.zeros((length, ret_width), jnp.float32)
    for h in range(head_count):
        here = (lane >= h * head_dim) & (lane < (h + 1) * head_dim)
        mean = jnp.sum(jnp.where(here, result, 0.0), axis=1, keepdims=True) / head_dim
        center = jnp.where(here, mean, center)
    centered = result - center
    squared = centered * centered
    factor = jnp.zeros((length, ret_width), jnp.float32)
    for h in range(head_count):
        here = (lane >= h * head_dim) & (lane < (h + 1) * head_dim)
        spread_h = jnp.sum(jnp.where(here, squared, 0.0), axis=1, keepdims=True) / head_dim
        factor = jnp.where(here, lax.rsqrt(spread_h + group_eps), factor)
    gates = projected[3]
    mixed[...] = (gates / (1.0 + jnp.exp(-gates)) * (centered * factor)).astype(jnp.bfloat16)

    settle(1)
    shares(mixed, merge, partial)
    for other in range(1, row):
        scatter(partial, received, 1, other).start()
    pump(2)
    total = tokens[...].astype(jnp.float32) + partial[seat].astype(jnp.float32)
    for other in range(1, row):
        scatter(partial, received, 1, other).wait_recv()
        total = total + received[other - 1].astype(jnp.float32)
    gathered_mid[seat] = total.astype(jnp.bfloat16)
    second = spread(gathered_mid.at[seat], gathered_mid, 2)
    for copy in second:
        copy.start()
    pump(3)
    launch(4)
    if parts > 1:
        launch(5)
    for copy in spread_in(gathered_mid, 2):
        copy.wait_recv()
    normalize(gathered_mid, middle_gain)
    settle(2)
    settle(3)
    hidden_width = hidden.shape[1]
    tile = 256 if hidden_width % 256 == 0 else 128

    @pl.loop(0, hidden_width // tile)
    def _(index):
        columns = pl.ds(pl.multiple_of(index * tile, tile), tile)
        gate_act = times(gate, columns)
        up_act = times(up, columns)
        hidden[:, columns] = (gate_act / (1.0 + jnp.exp(-gate_act)) * up_act).astype(jnp.bfloat16)

    for i in range(parts):
        pump(4 + i)
        if i + 2 < parts:
            launch(6 + i)
        if i:
            finish(i - 1)
    finish(parts - 1)
    for i in range(parts):
        collect(i)
    for copy in first + second:
        copy.wait_send()
    for other in range(1, row):
        scatter(partial, received, 1, other).wait_send()
        for i in range(parts):
            scatter(partial_ends.at[i], received_ends.at[i], 3 + i, other).wait_send()
    for k in range(count):
        drain(k)


def paired_kernel(
    sizes,
    tokens,
    input_gain_in,
    middle_gain_in,
    ahead,
    behind,
    cosine_in,
    sine_in,
    query_shard,
    key_shard,
    value_shard,
    output_gate_shard,
    merge_shard,
    gate_shard,
    up_shard,
    down_shard,
    out,
    input_gain,
    middle_gain,
    cosine,
    sine_part,
    finished,
    joined_out,
    merge_out,
    gate_out,
    up_out,
    down_out,
    joined,
    merge,
    gate,
    up,
    down,
    gathered,
    gathered_mid,
    normed,
    projected,
    mixed,
    hidden,
    first_partial,
    first_core,
    first_row,
    first_line,
    last_partial,
    last_core,
    last_row,
    last_line,
    own_sem,
    line_send,
    line_recv,
    pair_send,
    pair_recv,
    share_send,
    share_recv,
    sum_send,
    sum_recv,
    out_sem,
):
    line, row = sizes["fs"], sizes["tp"]
    pieces = down.shape[0]
    piece_width = down.shape[3]
    length, part_width = tokens.shape
    width = row * part_width
    seat = lax.axis_index("tp")
    place = lax.axis_index("fs")
    half = lax.axis_index("grp")
    core, column = lax.rem(seat, 2), seat // 2
    slot = lax.rem(place, 2)
    core_peer = seat + 1 - 2 * core
    row_peer = lax.rem(seat + 2, row)
    far_peer = lax.rem(core_peer + 2, row)
    line_peer = place + 1 - 2 * slot
    sign = 1 - 2 * (place // (line // 2))
    others = [lax.rem(place + sign * step + line, line) for step in range(1, line)]
    facing = jnp.where(place < line // 2, line // 2, line // 2 - 1)
    sources = [facing, line_peer] + [
        facing + sign * step for step in range(1, line // 2)
    ]

    barrier = pltpu.get_barrier_semaphore()
    for there in others:
        pl.semaphore_signal(barrier, inc=1, device_id={"fs": there}, device_id_type=MESH)
    pl.semaphore_signal(barrier, inc=1, device_id={"grp": 1 - half}, device_id_type=MESH)
    for there in (core_peer, row_peer):
        pl.semaphore_signal(barrier, inc=1, device_id={"tp": there}, device_id_type=MESH)

    group = joined_out.shape[2] // 4
    quads = (query_shard, key_shard, value_shard, output_gate_shard)
    merge_rows = merge.shape[1]
    hidden_half = gate.shape[2]

    def cut(ref, axis, part, size):
        window = pl.ds(pl.multiple_of(part * size, size), size)
        return ref.at[window] if axis == 0 else ref.at[:, window]

    loads = [
        [
            (quad.at[:, p * group : (p + 1) * group], joined_out.at[p, :, i * group : (i + 1) * group])
            for p in range(2)
            for i, quad in enumerate(quads)
        ],
        [(merge_shard, merge_out)],
        [(gate_shard, gate_out)],
        [(up_shard, up_out)],
        [(down_shard, down_out)],
        [
            (cut(quad, 1, slot, group), joined.at[place, :, i * group : (i + 1) * group])
            for i, quad in enumerate(quads)
        ],
        [(cut(merge_shard, 0, slot, merge_rows), merge.at[place])],
        [(cut(gate_shard, 1, slot, hidden_half), gate.at[place])],
        [(cut(up_shard, 1, slot, hidden_half), up.at[place])],
        [
            (
                cut(down_shard, 0, slot, hidden_half).at[:, i * piece_width : (i + 1) * piece_width],
                down.at[i, place],
            )
            for i in range(pieces)
        ],
        [(tokens, gathered.at[slot, seat])],
        [
            (input_gain_in, input_gain),
            (middle_gain_in, middle_gain),
            (cosine_in, cosine),
            (sine_in, sine_part),
        ],
    ]
    own, index = [], 0
    for pairs in loads:
        own.append([])
        for source, target in pairs:
            own[-1].append(pltpu.make_async_copy(source, target, own_sem.at[index]))
            index += 1
    for copies in (own[-2], *own[:-2], own[-1]):
        for copy in copies:
            copy.start()
    pl.semaphore_wait(barrier, line - 1 + 1 + 2)

    def ready(k):
        for copy in own[k]:
            copy.wait()

    def outgoing(k, parity):
        if k == 0:
            size = joined.shape[1] // 2
            return joined_out.at[parity, pl.ds(pl.multiple_of(half * size, size), size)]
        if k == 1:
            size = merge_rows // 2
            return cut(merge_out, 0, parity * 2 + half, size)
        if k < 4:
            source = (gate_out, up_out)[k - 2]
            size = source.shape[0] // 2
            return cut(source, 0, half, size).at[
                :, pl.ds(pl.multiple_of(parity * hidden_half, hidden_half), hidden_half)
            ]
        size = hidden_half // 2
        return cut(down_out, 0, parity * 2 + half, size).at[
            :, (k - 4) * piece_width : (k - 3) * piece_width
        ]

    def landing(k, block, part):
        target = (joined, merge, gate, up)[k] if k < 4 else down.at[k - 4]
        size = target.shape[1] // 2
        return target.at[block, pl.ds(pl.multiple_of(part * size, size), size)]

    def post(k, there):
        return pltpu.make_async_remote_copy(
            src_ref=outgoing(k, lax.rem(there, 2)),
            dst_ref=landing(k, place, half),
            send_sem=line_send.at[k, there],
            recv_sem=line_recv.at[k, place],
            device_id={"fs": there},
            device_id_type=MESH,
        )

    def arrival(k, block):
        return pltpu.make_async_remote_copy(
            src_ref=landing(k, block, half),
            dst_ref=landing(k, block, half),
            send_sem=line_send.at[k, block],
            recv_sem=line_recv.at[k, block],
            device_id={"fs": block},
            device_id_type=MESH,
        )

    def across(k, block, part):
        return pltpu.make_async_remote_copy(
            src_ref=landing(k, block, part),
            dst_ref=landing(k, block, part),
            send_sem=pair_send.at[k, block],
            recv_sem=pair_recv.at[k, block],
            device_id={"grp": 1 - half},
            device_id_type=MESH,
        )

    def launch(k):
        ready(k)
        for there in others:
            post(k, there).start()

    def pump(k, block):
        arrival(k, block).wait_recv()
        across(k, block, half).start()

    def settle(k):
        for block in sources:
            across(k, block, 1 - half).wait_recv()

    def handed(target, stage, step):
        plane = slot if step in (0, 1, 2, 3) else 1 - slot
        holder = seat if step in (0, 1, 2, 4, 5) else row_peer
        place_in = target.at[plane, holder]
        peer = {"tp": core_peer}
        if step in (1, 5):
            peer = {"tp": row_peer}
        if step == 2:
            peer = {"fs": line_peer}
        return pltpu.make_async_remote_copy(
            src_ref=place_in,
            dst_ref=place_in,
            send_sem=share_send.at[stage, step],
            recv_sem=share_recv.at[stage, step],
            device_id=peer,
            device_id_type=MESH,
        )

    def received(target, stage, step):
        plane = slot if step in (0, 1, 3) else 1 - slot
        holder = (core_peer, row_peer, seat, far_peer, core_peer, row_peer, far_peer)[step]
        place_in = target.at[plane, holder]
        return pltpu.make_async_remote_copy(
            src_ref=place_in,
            dst_ref=place_in,
            send_sem=share_send.at[stage, step],
            recv_sem=share_recv.at[stage, step],
            device_id={"tp": core_peer},
            device_id_type=MESH,
        )

    def normalize(source, gain_vector, plane):
        total = jnp.zeros((length, 1), jnp.float32)
        for t in range(row):
            widened = source[plane, t].astype(jnp.float32)
            total = total + jnp.sum(widened * widened, axis=1, keepdims=True)
        scale = lax.rsqrt(total / width + norm_eps)
        for t in range(row):
            span = slice(t * part_width, (t + 1) * part_width)
            scaled = source[plane, t].astype(jnp.float32) * scale * gain_vector[:, span]
            normed[plane, :, span] = scaled.astype(jnp.bfloat16)

    def hand_over(target, stage):
        return [handed(target, stage, step) for step in range(7)]

    def moved(source, target, peer, stage, step):
        return pltpu.make_async_remote_copy(
            src_ref=source,
            dst_ref=target,
            send_sem=sum_send.at[stage, step],
            recv_sem=sum_recv.at[stage, step],
            device_id=peer,
            device_id_type=MESH,
        )

    def share_mid(step):
        plane, kind = step % 2, step // 2
        spot = gathered_mid.at[plane, row_peer if kind == 2 else seat]
        return pltpu.make_async_remote_copy(
            src_ref=spot,
            dst_ref=spot,
            send_sem=share_send.at[1, step],
            recv_sem=share_recv.at[1, step],
            device_id={"tp": core_peer if kind else row_peer},
            device_id_type=MESH,
        )

    def shared_mid(step):
        plane, kind = step % 2, step // 2
        spot = gathered_mid.at[plane, (row_peer, core_peer, far_peer)[kind]]
        return pltpu.make_async_remote_copy(
            src_ref=spot,
            dst_ref=spot,
            send_sem=share_send.at[1, step],
            recv_sem=share_recv.at[1, step],
            device_id={"tp": core_peer},
            device_id_type=MESH,
        )

    def reducer(partial, core_in, row_in, stage):
        order = (0, 1) if stage == 0 else (1 - slot, slot)
        return [moved(partial.at[1 - core], core_in, {"tp": core_peer}, stage, 0)] + [
            moved(
                partial.at[core, 1 - column, plane],
                row_in.at[step],
                {"tp": row_peer},
                stage,
                1 + step,
            )
            for step, plane in enumerate(order)
        ]

    def add_core(partial, core_in, steps, order):
        steps[0].wait_recv()
        for step, plane in enumerate(order):
            total = partial[core, 1 - column, plane].astype(jnp.float32) + core_in[
                1 - column, plane
            ].astype(jnp.float32)
            partial[core, 1 - column, plane] = total.astype(jnp.bfloat16)
            steps[1 + step].start()

    def add_row(partial, core_in, row_in, steps, step, plane):
        steps[1 + step].wait_recv()
        return (
            partial[core, column, plane].astype(jnp.float32)
            + core_in[column, plane].astype(jnp.float32)
            + row_in[step].astype(jnp.float32)
        )

    first = hand_over(gathered, 0)
    ready(10)
    for step in (2, 1, 0):
        first[step].start()
    launch(0)
    launch(1)
    launch(2)
    launch(3)
    received(gathered, 0, 1).wait_recv()
    first[3].start()
    pump(0, sources[0])
    received(gathered, 0, 2).wait_recv()
    first[5].start()
    first[4].start()
    pump(0, sources[1])
    received(gathered, 0, 0).wait_recv()
    received(gathered, 0, 3).wait_recv()
    ready(11)
    normalize(gathered, input_gain, slot)
    pump(0, sources[2])
    received(gathered, 0, 5).wait_recv()
    first[6].start()
    received(gathered, 0, 4).wait_recv()
    received(gathered, 0, 6).wait_recv()
    normalize(gathered, input_gain, 1 - slot)
    ready(5)
    settle(0)
    for block in sources:
        pump(1, block)
    for plane in range(2):
        rows_out = jnp.dot(
            normed[plane], joined[...].reshape(width, 4 * group), preferred_element_type=jnp.float32
        )
        for i in range(4):
            projected[i, plane] = (
                rows_out[:, i * group : (i + 1) * group].astype(jnp.bfloat16).astype(jnp.float32)
            )

    head_count = ahead.shape[0] // 2
    head_dim = group // head_count
    lane = lax.broadcasted_iota(jnp.int32, (length, group), 1)
    in_lower = lax.rem(lane, head_dim) < head_dim // 2

    def turned(values):
        partner = jnp.where(
            in_lower,
            pltpu.roll(values, group - head_dim // 2, 1),
            pltpu.roll(values, head_dim // 2, 1),
        )
        return values * cosine[...] + partner * sine_part[...]

    offset = (
        lax.broadcasted_iota(jnp.int32, (length, length), 0)
        - lax.broadcasted_iota(jnp.int32, (length, length), 1)
    ).astype(jnp.float32)

    def log_sigmoid(logit):
        value = jnp.full((8, 128), logit, jnp.float32)
        return (jnp.minimum(value, 0.0) - jnp.log1p(jnp.exp(-jnp.abs(value))))[:1, :1]

    decays = [
        jnp.exp(
            jnp.where(
                offset >= 0,
                log_sigmoid(ahead[slot * head_count + h]) * offset,
                -log_sigmoid(behind[slot * head_count + h]) * offset,
            )
        )
        for h in range(head_count)
    ]
    here = [(lane >= h * head_dim) & (lane < (h + 1) * head_dim) for h in range(head_count)]
    for plane in range(2):
        queries = turned(projected[0, plane])
        key_heads = (turned(projected[1, plane]) * head_dim ** (-0.5)).astype(jnp.bfloat16)
        valued = projected[2, plane]
        result = jnp.zeros((length, group), jnp.float32)
        for h in range(head_count):
            scores = lax.dot_general(
                jnp.where(here[h], queries, 0.0).astype(jnp.bfloat16),
                key_heads,
                (((1,), (1,)), ((), ())),
                preferred_element_type=jnp.float32,
            )
            result = result + jnp.dot(
                (scores * decays[h]).astype(jnp.bfloat16),
                jnp.where(here[h], valued, 0.0).astype(jnp.bfloat16),
                preferred_element_type=jnp.float32,
            )
        center = jnp.zeros((length, group), jnp.float32)
        for h in range(head_count):
            mean = jnp.sum(jnp.where(here[h], result, 0.0), axis=1, keepdims=True) / head_dim
            center = jnp.where(here[h], mean, center)
        centered = result - center
        squared = centered * centered
        factor = jnp.zeros((length, group), jnp.float32)
        for h in range(head_count):
            spread_h = jnp.sum(jnp.where(here[h], squared, 0.0), axis=1, keepdims=True) / head_dim
            factor = jnp.where(here[h], lax.rsqrt(spread_h + group_eps), factor)
        gates = projected[3, plane]
        mixed[plane] = (gates / (1.0 + jnp.exp(-gates)) * (centered * factor)).astype(jnp.bfloat16)

    ready(6)
    settle(1)

    def fill(rows_in, weight, partial, side):
        for x in range(row // 2):
            block = x * 2 + side
            for plane in range(2):
                term = jnp.dot(rows_in[plane], weight[block], preferred_element_type=jnp.float32)
                partial[side, x, plane] = term.astype(jnp.bfloat16)

    steps = reducer(first_partial, first_core, first_row, 0) + [
        moved(first_partial.at[core, column, plane], first_line.at[plane], {"fs": line_peer}, 0, 3 + plane)
        for plane in range(2)
    ]
    fill(mixed, merge, first_partial, 1 - core)
    steps[0].start()
    fill(mixed, merge, first_partial, core)
    add_core(first_partial, first_core, steps, (0, 1))
    pump(2, others[0])
    for plane in range(2):
        total = add_row(first_partial, first_core, first_row, steps, plane, plane)
        first_partial[core, column, plane] = total.astype(jnp.bfloat16)
        steps[3 + plane].start()
    ready(4)
    for i in range(pieces):
        for there in others:
            post(4 + i, there).start()

    second = [share_mid(step) for step in range(6)]
    pump(2, others[1])
    pump(2, others[2])
    pump(3, others[0])
    for plane in range(2):
        steps[3 + plane].wait_recv()
        total = gathered[plane, seat].astype(jnp.float32) + (
            first_partial[core, column, plane].astype(jnp.float32)
            + first_line[plane].astype(jnp.float32)
        )
        gathered_mid[plane, seat] = total.astype(jnp.bfloat16)
        second[plane].start()
        second[2 + plane].start()
        pump(3, others[1 + plane])
    queue = [(4 + i, block) for i in range(pieces) for block in others]

    def pump_next(count):
        for _ in range(count):
            pump(*queue.pop(0))

    for plane in range(2):
        shared_mid(plane).wait_recv()
        second[4 + plane].start()
        pump_next(len(others))
    for plane in range(2):
        shared_mid(2 + plane).wait_recv()
        shared_mid(4 + plane).wait_recv()
        normalize(gathered_mid, middle_gain, plane)
    ready(7)
    ready(8)
    settle(2)
    settle(3)
    tile = 256
    for plane in range(2):
        for begin in range(0, hidden_half, tile):
            columns = slice(begin, min(begin + tile, hidden_half))
            gate_act, up_act = [
                jnp.dot(
                    normed[plane],
                    weight[:, :, columns].reshape(width, -1),
                    preferred_element_type=jnp.float32,
                )
                for weight in (gate, up)
            ]
            hidden[plane, :, columns] = (gate_act / (1.0 + jnp.exp(-gate_act)) * up_act).astype(
                jnp.bfloat16
            )
        if plane == 0:
            pump_next(len(others))

    ready(9)
    ends = [
        reducer(last_partial.at[i], last_core.at[i], last_row.at[i], 1 + i)
        + [
            moved(
                last_partial.at[i, core, column, 1 - slot],
                last_line.at[i],
                {"fs": line_peer},
                1 + i,
                3,
            )
        ]
        for i in range(pieces)
    ]

    def pass_line(i):
        total = add_row(
            last_partial.at[i], last_core.at[i], last_row.at[i], ends[i], 0, 1 - slot
        )
        last_partial[i, core, column, 1 - slot] = total.astype(jnp.bfloat16)
        ends[i][3].start()

    written = [
        pltpu.make_async_copy(
            finished.at[:, i * piece_width : (i + 1) * piece_width],
            out.at[:, i * piece_width : (i + 1) * piece_width],
            out_sem.at[i],
        )
        for i in range(pieces)
    ]

    def finish(i):
        span = slice(i * piece_width, (i + 1) * piece_width)
        total = gathered_mid[slot, seat, :, span].astype(jnp.float32) + add_row(
            last_partial.at[i], last_core.at[i], last_row.at[i], ends[i], 1, slot
        )
        ends[i][3].wait_recv()
        finished[:, span] = (total + last_line[i].astype(jnp.float32)).astype(jnp.bfloat16)
        written[i].start()

    for i in range(pieces):
        if i == 2:
            pump_next(len(queue))
        settle(4 + i)
        fill(hidden, down.at[i], last_partial.at[i], 1 - core)
        ends[i][0].start()
        fill(hidden, down.at[i], last_partial.at[i], core)
        add_core(last_partial.at[i], last_core.at[i], ends[i], (1 - slot, slot))
        if i:
            pass_line(i - 1)
        if i > 1:
            finish(i - 2)
    pass_line(pieces - 1)
    for i in range(max(0, pieces - 2), pieces):
        finish(i)

    for copy in written:
        copy.wait()
    for copy in first + second + steps:
        copy.wait_send()
    for group_steps in ends:
        for copy in group_steps:
            copy.wait_send()
    for k in range(4 + pieces):
        for there in others:
            post(k, there).wait_send()
            across(k, there, half).wait_send()


def paired_call(
    sizes, flat, input_gain, middle_gain, decays, tables, quads, merge_weight, gate_weight, up_weight, down_weight
):
    line, row = sizes["fs"], sizes["tp"]
    bf16 = jnp.bfloat16
    length, part_width = flat.shape
    depth, ret_width = quads[0].shape
    hidden_half, group = gate_weight.shape[1] // 2, ret_width // 2
    pieces = 4
    piece_width = down_weight.shape[1] // pieces
    kinds = 4 + pieces
    anywhere = pl.BlockSpec(memory_space=pl.ANY)
    in_smem = pl.BlockSpec(memory_space=pltpu.SMEM)

    def sums(lead, columns, last):
        return [
            pltpu.VMEM(lead + (2, row // 2, 2, length, columns), bf16),
            pltpu.VMEM(lead + (row // 2, 2, length, columns), bf16),
            pltpu.VMEM(lead + (2, length, columns), bf16),
            pltpu.VMEM(lead + last + (length, columns), bf16),
        ]

    dma = pltpu.SemaphoreType.DMA
    return pl.pallas_call(
        functools.partial(paired_kernel, sizes),
        out_shape=jax.ShapeDtypeStruct(flat.shape, bf16),
        in_specs=[anywhere] * 3 + [in_smem] * 2 + [anywhere] * 10,
        out_specs=anywhere,
        scratch_shapes=[
            pltpu.VMEM((1, row * part_width), jnp.float32),
            pltpu.VMEM((1, row * part_width), jnp.float32),
            pltpu.VMEM(tables[0].shape, jnp.float32),
            pltpu.VMEM(tables[1].shape, jnp.float32),
            pltpu.VMEM(flat.shape, bf16),
            pltpu.VMEM((2, depth, 4 * group), bf16),
            pltpu.VMEM(merge_weight.shape, bf16),
            pltpu.VMEM(gate_weight.shape, bf16),
            pltpu.VMEM(up_weight.shape, bf16),
            pltpu.VMEM(down_weight.shape, bf16),
            pltpu.VMEM((line, depth, 4 * group), bf16),
            pltpu.VMEM((line, merge_weight.shape[0] // 2, part_width), bf16),
            pltpu.VMEM((line, depth, hidden_half), bf16),
            pltpu.VMEM((line, depth, hidden_half), bf16),
            pltpu.VMEM((pieces, line, hidden_half, piece_width), bf16),
            pltpu.VMEM((2, row, length, part_width), bf16),
            pltpu.VMEM((2, row, length, part_width), bf16),
            pltpu.VMEM((2, length, row * part_width), bf16),
            pltpu.VMEM((4, 2, length, group), jnp.float32),
            pltpu.VMEM((2, length, group), bf16),
            pltpu.VMEM((2, length, hidden_half), bf16),
        ]
        + sums((), part_width, (2,))
        + sums((pieces,), piece_width, ())
        + [
            dma((25 + pieces,)),
            dma((kinds, line)),
            dma((kinds, line)),
            dma((kinds, line)),
            dma((kinds, line)),
            dma((2, 7)),
            dma((2, 7)),
            dma((1 + pieces, 5)),
            dma((1 + pieces, 5)),
            dma((pieces,)),
        ],
        compiler_params=pltpu.CompilerParams(
            collective_id=0, has_side_effects=True, vmem_limit_bytes=60 << 20
        ),
    )(
        flat,
        input_gain[None, :],
        middle_gain[None, :],
        *decays,
        *tables,
        *quads,
        merge_weight,
        gate_weight,
        up_weight,
        down_weight,
    )


def on_device(
    sizes,
    tokens,
    input_gain,
    query_weight,
    key_weight,
    value_weight,
    output_gate_matrix,
    forward_decay,
    backward_decay,
    merge_weight,
    middle_gain,
    gate_weight,
    up_weight,
    down_weight,
):
    seq_count, length, part_width = tokens.shape
    flat = tokens.reshape(seq_count * length, part_width)
    quads = (query_weight, key_weight, value_weight, output_gate_matrix)
    paired = (
        sizes["grp"] == 2
        and sizes["fs"] == sizes["tp"] == 4
        and seq_count == 1
        and query_weight.shape[1] % 256 == 0
        and forward_decay.shape[0] % 2 == 0
        and gate_weight.shape[1] % 256 == 0
        and down_weight.shape[1] == part_width
        and part_width % 256 == 0
    )
    if paired:
        head_count = forward_decay.shape[0] // 2
        head_dim = query_weight.shape[1] // (2 * head_count)
        layer_out = paired_call(
            sizes,
            flat,
            input_gain,
            middle_gain,
            (forward_decay, backward_decay),
            turn_tables(length, head_dim, head_count),
            quads,
            merge_weight,
            gate_weight,
            up_weight,
            down_weight,
        )
        return layer_out.reshape(seq_count, length, part_width)
    joined = jnp.concatenate(quads, axis=1)
    shards = (joined, merge_weight, gate_weight, up_weight, down_weight)
    line, copies, row = sizes["fs"], sizes["grp"], sizes["tp"]
    down_width = down_weight.shape[1]
    parts = down_width // 256 if line == row and down_width % 256 == 0 else 1
    down_piece = jax.ShapeDtypeStruct((down_weight.shape[0], down_width // parts), jnp.bfloat16)
    landing = shards[:4] + (down_piece,) * parts
    count = len(landing)
    width, ret_width, hidden_width = row * part_width, query_weight.shape[1], gate_weight.shape[1]
    head_count = forward_decay.shape[0]
    tables = turn_tables(length, ret_width // head_count, head_count)
    in_vmem = pl.BlockSpec(memory_space=pltpu.VMEM)
    in_smem = pl.BlockSpec(memory_space=pltpu.SMEM)
    bf16 = jnp.bfloat16
    layer_out = pl.pallas_call(
        functools.partial(layer_kernel, sizes),
        out_shape=jax.ShapeDtypeStruct(flat.shape, bf16),
        in_specs=[in_vmem] * 3
        + [in_smem] * 2
        + [in_vmem] * 2
        + [pl.BlockSpec(memory_space=pl.ANY)] * len(shards),
        out_specs=in_vmem,
        scratch_shapes=[pltpu.VMEM((line,) + w.shape, w.dtype) for w in landing]
        + [
            pltpu.VMEM((row, length, part_width), bf16),
            pltpu.VMEM((row, length, part_width), bf16),
            pltpu.VMEM((length, width), bf16),
            pltpu.VMEM((4, length, ret_width), jnp.float32),
            pltpu.VMEM((length, ret_width), bf16),
            pltpu.VMEM((length, hidden_width), bf16),
            pltpu.VMEM((row, length, part_width), bf16),
            pltpu.VMEM((row - 1, length, part_width), bf16),
            pltpu.SemaphoreType.DMA((count,)),
            pltpu.SemaphoreType.DMA((count, 2, line)),
            pltpu.SemaphoreType.DMA((count, 2, line)),
            pltpu.SemaphoreType.DMA((count, 2, line, copies - 1)),
            pltpu.SemaphoreType.DMA((count, 2, line, copies - 1)),
            pltpu.SemaphoreType.DMA((3 + parts, row - 1)),
            pltpu.SemaphoreType.DMA((3 + parts, row - 1)),
            pltpu.SemaphoreType.DMA,
            pltpu.VMEM((parts, row, length, part_width // parts), bf16),
            pltpu.VMEM((parts, row - 1, length, part_width // parts), bf16),
        ],
        compiler_params=pltpu.CompilerParams(
            collective_id=0, has_side_effects=True, vmem_limit_bytes=58 << 20
        ),
    )(
        flat,
        input_gain[None, :],
        middle_gain[None, :],
        jax.nn.log_sigmoid(forward_decay),
        jax.nn.log_sigmoid(backward_decay),
        *tables,
        *shards,
    )
    return layer_out.reshape(seq_count, length, part_width)


def solution(mesh):
    placed = (
        P(("grp", "fs"), None, "tp"),
        P(),
        P("fs", "tp"),
        P("fs", "tp"),
        P("fs", "tp"),
        P("fs", "tp"),
        P("tp"),
        P("tp"),
        P("tp", "fs"),
        P(),
        P("fs", "tp"),
        P("fs", "tp"),
        P("tp", "fs"),
    )
    return jax.shard_map(
        functools.partial(on_device, dict(mesh.shape)),
        mesh=mesh,
        in_specs=placed,
        out_specs=P(("grp", "fs"), None, "tp"),
        check_vma=False,
    )
```

```python
import functools

import jax
import jax.numpy as jnp
import numpy as np
from jax import lax
from jax.experimental import pallas as pl
from jax.experimental.pallas import tpu as pltpu
from jax.sharding import PartitionSpec as P

norm_eps = 1e-06
group_eps = 1e-05
rope_base = 10000.0


def turn_tables(length, head_dim, head_count):
    half_dim = head_dim // 2
    inverse = rope_base ** (-np.arange(half_dim) / half_dim)
    angles = np.arange(length)[:, None] * inverse[None, :]
    cosine, sine_part = np.cos(angles), np.sin(angles)
    return (
        np.tile(np.concatenate([cosine, cosine], axis=1), (1, head_count)).astype(np.float32),
        np.tile(np.concatenate([-sine_part, sine_part], axis=1), (1, head_count)).astype(np.float32),
    )


MESH = pl.DeviceIdType.MESH


def layer_kernel(
    sizes,
    tokens,
    input_gain,
    middle_gain,
    rate_ahead,
    rate_behind,
    cosine,
    sine_part,
    joined_shard,
    merge_shard,
    gate_shard,
    up_shard,
    down_shard,
    out,
    joined,
    merge,
    gate,
    up,
    *rest,
):
    line, copies, row = sizes["fs"], sizes["grp"], sizes["tp"]
    parts = len(rest) - 18
    downs, partial_ends, received_ends = rest[:parts], rest[-2], rest[-1]
    (
        gathered,
        gathered_mid,
        normed,
        projected,
        mixed,
        hidden,
        partial,
        received,
        own_sem,
        line_send,
        line_recv,
        pair_send,
        pair_recv,
        row_send,
        row_recv,
        self_sem,
    ) = rest[parts:-2]
    piece_width = downs[0].shape[2]
    shards = (joined_shard, merge_shard, gate_shard, up_shard) + tuple(
        down_shard if parts == 1 else down_shard.at[:, pl.ds(i * piece_width, piece_width)]
        for i in range(parts)
    )
    slots = (joined, merge, gate, up) + tuple(downs)
    count = len(slots)
    length, part_width = tokens.shape
    width = row * part_width
    seat = lax.axis_index("tp")
    place = lax.axis_index("fs")
    half = lax.axis_index("grp")

    barrier = pltpu.get_barrier_semaphore()
    for shift in (1, -1):
        there = place + shift

        @pl.when((there >= 0) & (there < line))
        def _():
            pl.semaphore_signal(barrier, inc=1, device_id={"fs": there}, device_id_type=MESH)

    for other in range(1, copies):
        pl.semaphore_signal(
            barrier,
            inc=1,
            device_id={"grp": lax.rem(half + other, copies)},
            device_id_type=MESH,
        )
    for other in range(1, row):
        pl.semaphore_signal(
            barrier,
            inc=1,
            device_id={"tp": lax.rem(seat + other, row)},
            device_id_type=MESH,
        )
    own = [pltpu.make_async_copy(shards[k], slots[k].at[place], own_sem.at[k]) for k in range(count)]
    for copy in own:
        copy.start()
    neighbours = (place > 0).astype(jnp.int32) + (place < line - 1).astype(jnp.int32)
    mine = pltpu.make_async_copy(tokens, gathered.at[seat], self_sem)
    mine.start()
    pl.semaphore_wait(barrier, neighbours + copies - 1 + row - 1)

    def piece(k, block, part):
        rows = slots[k].shape[1] // copies
        return slots[k].at[block, pl.ds(pl.multiple_of(part * rows, rows), rows), :]

    def hop(k, way, step):
        shift = 1 if way == 0 else -1
        block = place - shift * step
        return pltpu.make_async_remote_copy(
            src_ref=piece(k, block, half),
            dst_ref=piece(k, block, half),
            send_sem=line_send.at[k, way, step],
            recv_sem=line_recv.at[k, way, step],
            device_id={"fs": place + shift},
            device_id_type=MESH,
        )

    def arrival(k, way, step):
        shift = 1 if way == 0 else -1
        block = place - shift * step
        return pltpu.make_async_remote_copy(
            src_ref=piece(k, block, half),
            dst_ref=piece(k, block, half),
            send_sem=line_send.at[k, way, step - 1],
            recv_sem=line_recv.at[k, way, step - 1],
            device_id={"fs": place - shift},
            device_id_type=MESH,
        )

    def across(k, way, step, other):
        shift = 1 if way == 0 else -1
        block = place - shift * step
        return pltpu.make_async_remote_copy(
            src_ref=piece(k, block, half),
            dst_ref=piece(k, block, half),
            send_sem=pair_send.at[k, way, step - 1, other - 1],
            recv_sem=pair_recv.at[k, way, step - 1, other - 1],
            device_id={"grp": lax.rem(half + other, copies)},
            device_id_type=MESH,
        )

    def landed(k, way, step, other):
        shift = 1 if way == 0 else -1
        block = place - shift * step
        source = lax.rem(half + copies - other, copies)
        return pltpu.make_async_remote_copy(
            src_ref=piece(k, block, source),
            dst_ref=piece(k, block, source),
            send_sem=pair_send.at[k, way, step - 1, other - 1],
            recv_sem=pair_recv.at[k, way, step - 1, other - 1],
            device_id={"grp": source},
            device_id_type=MESH,
        )

    def has(way, step):
        return place >= step if way == 0 else place + step < line

    def goes(way):
        return place < line - 1 if way == 0 else place > 0

    def launch(k):
        own[k].wait()
        for way in range(2):

            @pl.when(goes(way))
            def _():
                hop(k, way, 0).start()

    def pump(k):
        for step in range(1, line):
            for way in range(2):

                @pl.when(has(way, step))
                def _():
                    arrival(k, way, step).wait_recv()
                    for other in range(1, copies):
                        across(k, way, step, other).start()

                @pl.when(has(way, step) & goes(way))
                def _():
                    hop(k, way, step).start()

    def settle(k):
        for step in range(1, line):
            for way in range(2):

                @pl.when(has(way, step))
                def _():
                    for other in range(1, copies):
                        landed(k, way, step, other).wait_recv()

    def drain(k):
        for way in range(2):
            for step in range(line):

                @pl.when((has(way, step) if step else True) & goes(way))
                def _():
                    hop(k, way, step).wait_send()

                if step:

                    @pl.when(has(way, step))
                    def _():
                        for other in range(1, copies):
                            across(k, way, step, other).wait_send()

    def spread(source, target, stage):
        return [
            pltpu.make_async_remote_copy(
                src_ref=source,
                dst_ref=target.at[seat],
                send_sem=row_send.at[stage, other - 1],
                recv_sem=row_recv.at[stage, other - 1],
                device_id={"tp": lax.rem(seat + other, row)},
                device_id_type=MESH,
            )
            for other in range(1, row)
        ]

    def spread_in(target, stage):
        sources = [lax.rem(seat + row - other, row) for other in range(1, row)]
        return [
            pltpu.make_async_remote_copy(
                src_ref=target.at[source],
                dst_ref=target.at[source],
                send_sem=row_send.at[stage, other],
                recv_sem=row_recv.at[stage, other],
                device_id={"tp": source},
                device_id_type=MESH,
            )
            for other, source in enumerate(sources)
        ]

    def scatter(source, target, stage, other):
        there = lax.rem(seat + other, row)
        return pltpu.make_async_remote_copy(
            src_ref=source.at[there],
            dst_ref=target.at[other - 1],
            send_sem=row_send.at[stage, other - 1],
            recv_sem=row_recv.at[stage, other - 1],
            device_id={"tp": there},
            device_id_type=MESH,
        )

    def normalize(source, gain_vector):
        total = jnp.zeros((length, 1), jnp.float32)
        for t in range(row):
            widened = source[t].astype(jnp.float32)
            total = total + jnp.sum(widened * widened, axis=1, keepdims=True)
        scale = lax.rsqrt(total / width + norm_eps)
        for t in range(row):
            span = slice(t * part_width, (t + 1) * part_width)
            scaled = source[t].astype(jnp.float32) * scale * gain_vector[:, span]
            normed[:, span] = scaled.astype(jnp.bfloat16)

    def times(weight, columns):
        block = weight[:, :, columns]
        return jnp.dot(
            normed[...], block.reshape(-1, block.shape[2]), preferred_element_type=jnp.float32
        )

    def shares(rows_in, weight, target):
        step = weight.shape[2]
        for block in range(line):
            term = jnp.dot(rows_in[...], weight[block], preferred_element_type=jnp.float32)
            begin = block * step
            inner = begin % part_width
            target[begin // part_width, :, inner : inner + step] = term.astype(jnp.bfloat16)

    def finish(i):
        settle(4 + i)
        if parts == 1:
            shares(hidden, downs[i], partial_ends.at[i])
        else:
            for j in range(row):
                blocks = [jnp.dot(
                    hidden[...], downs[i][j * line // row + c], preferred_element_type=jnp.float32
                ) for c in range(max(1, line // row))]
                for c, term in enumerate(blocks):
                    partial_ends[i, j, :, c * piece_width : (c + 1) * piece_width] = term.astype(
                        jnp.bfloat16
                    )
        for other in range(1, row):
            scatter(partial_ends.at[i], received_ends.at[i], 3 + i, other).start()

    def collect(i):
        span = slice(None) if parts == 1 else slice(i * piece_width, (i + 1) * piece_width)
        total = gathered_mid[seat, :, span].astype(jnp.float32)
        total = total + partial_ends[i, seat].astype(jnp.float32)
        for other in range(1, row):
            scatter(partial_ends.at[i], received_ends.at[i], 3 + i, other).wait_recv()
            total = total + received_ends[i, other - 1].astype(jnp.float32)
        out[:, span] = total.astype(jnp.bfloat16)

    launch(0)
    first = spread(tokens, gathered, 0)
    for copy in first:
        copy.start()
    launch(1)
    mine.wait()
    for copy in spread_in(gathered, 0):
        copy.wait_recv()
    normalize(gathered, input_gain)

    pump(0)
    launch(2)
    settle(0)
    ret_width = projected.shape[2]
    for t in range(4):
        projected[t] = (
            times(joined, slice(t * ret_width, (t + 1) * ret_width))
            .astype(jnp.bfloat16)
            .astype(jnp.float32)
        )
    pump(1)
    launch(3)

    head_count = rate_ahead.shape[0]
    head_dim = ret_width // head_count
    lane = lax.broadcasted_iota(jnp.int32, (length, ret_width), 1)
    in_lower = lax.rem(lane, head_dim) < head_dim // 2

    def turned(values):
        partner = jnp.where(
            in_lower,
            pltpu.roll(values, ret_width - head_dim // 2, 1),
            pltpu.roll(values, head_dim // 2, 1),
        )
        return values * cosine[...] + partner * sine_part[...]

    queries = turned(projected[0])
    key_heads = (turned(projected[1]) * head_dim ** (-0.5)).astype(jnp.bfloat16)
    valued = projected[2]
    offset = (
        lax.broadcasted_iota(jnp.int32, (length, length), 0)
        - lax.broadcasted_iota(jnp.int32, (length, length), 1)
    ).astype(jnp.float32)
    result = jnp.zeros((length, ret_width), jnp.float32)
    for h in range(head_count):
        here = (lane >= h * head_dim) & (lane < (h + 1) * head_dim)
        scores = lax.dot_general(
            jnp.where(here, queries, 0.0).astype(jnp.bfloat16),
            key_heads,
            (((1,), (1,)), ((), ())),
            preferred_element_type=jnp.float32,
        )
        decay = jnp.exp(jnp.where(offset >= 0, rate_ahead[h] * offset, -rate_behind[h] * offset))
        result = result + jnp.dot(
            (scores * decay).astype(jnp.bfloat16),
            jnp.where(here, valued, 0.0).astype(jnp.bfloat16),
            preferred_element_type=jnp.float32,
        )
    center = jnp.zeros((length, ret_width), jnp.float32)
    for h in range(head_count):
        here = (lane >= h * head_dim) & (lane < (h + 1) * head_dim)
        mean = jnp.sum(jnp.where(here, result, 0.0), axis=1, keepdims=True) / head_dim
        center = jnp.where(here, mean, center)
    centered = result - center
    squared = centered * centered
    factor = jnp.zeros((length, ret_width), jnp.float32)
    for h in range(head_count):
        here = (lane >= h * head_dim) & (lane < (h + 1) * head_dim)
        spread_h = jnp.sum(jnp.where(here, squared, 0.0), axis=1, keepdims=True) / head_dim
        factor = jnp.where(here, lax.rsqrt(spread_h + group_eps), factor)
    gates = projected[3]
    mixed[...] = (gates / (1.0 + jnp.exp(-gates)) * (centered * factor)).astype(jnp.bfloat16)

    settle(1)
    shares(mixed, merge, partial)
    for other in range(1, row):
        scatter(partial, received, 1, other).start()
    pump(2)
    total = tokens[...].astype(jnp.float32) + partial[seat].astype(jnp.float32)
    for other in range(1, row):
        scatter(partial, received, 1, other).wait_recv()
        total = total + received[other - 1].astype(jnp.float32)
    gathered_mid[seat] = total.astype(jnp.bfloat16)
    second = spread(gathered_mid.at[seat], gathered_mid, 2)
    for copy in second:
        copy.start()
    pump(3)
    launch(4)
    if parts > 1:
        launch(5)
    for copy in spread_in(gathered_mid, 2):
        copy.wait_recv()
    normalize(gathered_mid, middle_gain)
    settle(2)
    settle(3)
    hidden_width = hidden.shape[1]
    tile = 256 if hidden_width % 256 == 0 else 128

    @pl.loop(0, hidden_width // tile)
    def _(index):
        columns = pl.ds(pl.multiple_of(index * tile, tile), tile)
        gate_act = times(gate, columns)
        up_act = times(up, columns)
        hidden[:, columns] = (gate_act / (1.0 + jnp.exp(-gate_act)) * up_act).astype(jnp.bfloat16)

    for i in range(parts):
        pump(4 + i)
        if i + 2 < parts:
            launch(6 + i)
        if i:
            finish(i - 1)
    finish(parts - 1)
    for i in range(parts):
        collect(i)
    for copy in first + second:
        copy.wait_send()
    for other in range(1, row):
        scatter(partial, received, 1, other).wait_send()
        for i in range(parts):
            scatter(partial_ends.at[i], received_ends.at[i], 3 + i, other).wait_send()
    for k in range(count):
        drain(k)


def paired_kernel(
    sizes,
    tokens,
    input_gain_in,
    middle_gain_in,
    ahead,
    behind,
    cosine_in,
    sine_in,
    query_shard,
    key_shard,
    value_shard,
    output_gate_shard,
    merge_shard,
    gate_shard,
    up_shard,
    down_shard,
    out,
    input_gain,
    middle_gain,
    cosine,
    sine_part,
    finished,
    joined_out,
    merge_out,
    gate_out,
    up_out,
    down_out,
    joined,
    merge,
    gate,
    up,
    down,
    gathered,
    gathered_mid,
    normed,
    projected,
    mixed,
    hidden,
    first_partial,
    first_core,
    first_row,
    first_line,
    last_partial,
    last_core,
    last_row,
    last_line,
    own_sem,
    line_send,
    line_recv,
    pair_send,
    pair_recv,
    share_send,
    share_recv,
    sum_send,
    sum_recv,
    out_sem,
):
    line, row = sizes["fs"], sizes["tp"]
    pieces = down.shape[0]
    piece_width = down.shape[3]
    length, part_width = tokens.shape
    width = row * part_width
    seat = lax.axis_index("tp")
    place = lax.axis_index("fs")
    half = lax.axis_index("grp")
    core, column = lax.rem(seat, 2), seat // 2
    slot = lax.rem(place, 2)
    core_peer = seat + 1 - 2 * core
    row_peer = lax.rem(seat + 2, row)
    far_peer = lax.rem(core_peer + 2, row)
    line_peer = place + 1 - 2 * slot
    sign = 1 - 2 * (place // (line // 2))
    others = [lax.rem(place + sign * step + line, line) for step in range(1, line)]
    facing = jnp.where(place < line // 2, line // 2, line // 2 - 1)
    crossing = [facing + sign * step for step in range(line // 2)]
    sources = [facing, line_peer] + crossing[1:]

    barrier = pltpu.get_barrier_semaphore()
    for there in others:
        pl.semaphore_signal(barrier, inc=1, device_id={"fs": there}, device_id_type=MESH)
    pl.semaphore_signal(barrier, inc=1, device_id={"grp": 1 - half}, device_id_type=MESH)
    for there in (core_peer, row_peer):
        pl.semaphore_signal(barrier, inc=1, device_id={"tp": there}, device_id_type=MESH)

    group = joined_out.shape[2] // 4
    quads = (query_shard, key_shard, value_shard, output_gate_shard)
    merge_rows = merge.shape[1]
    hidden_half = gate.shape[2]

    def cut(ref, axis, part, size):
        window = pl.ds(pl.multiple_of(part * size, size), size)
        return ref.at[window] if axis == 0 else ref.at[:, window]

    loads = [
        [
            (quad.at[:, p * group : (p + 1) * group], joined_out.at[p, :, i * group : (i + 1) * group])
            for p in range(2)
            for i, quad in enumerate(quads)
        ],
        [(merge_shard, merge_out)],
        [(gate_shard, gate_out)],
        [(up_shard, up_out)],
        [(down_shard, down_out)],
        [
            (cut(quad, 1, slot, group), joined.at[place, :, i * group : (i + 1) * group])
            for i, quad in enumerate(quads)
        ],
        [(cut(merge_shard, 0, slot, merge_rows), merge.at[place])],
        [(cut(gate_shard, 1, slot, hidden_half), gate.at[place])],
        [(cut(up_shard, 1, slot, hidden_half), up.at[place])],
        [
            (
                cut(down_shard, 0, slot, hidden_half).at[:, i * piece_width : (i + 1) * piece_width],
                down.at[i, place],
            )
            for i in range(pieces)
        ],
        [(tokens, gathered.at[slot, seat])],
        [
            (input_gain_in, input_gain),
            (middle_gain_in, middle_gain),
            (cosine_in, cosine),
            (sine_in, sine_part),
        ],
    ]
    own, index = [], 0
    for pairs in loads:
        own.append([])
        for source, target in pairs:
            own[-1].append(pltpu.make_async_copy(source, target, own_sem.at[index]))
            index += 1

    for copies in (own[-2], *own[:-2], own[-1]):
        for copy in copies:
            copy.start()

    pl.semaphore_wait(barrier, line - 1 + 1 + 2)

    def ready(k):
        for copy in own[k]:
            copy.wait()

    first_down = 6

    def outgoing(k, parity):
        if k == 0:
            size = joined.shape[1] // 2
            return joined_out.at[parity, pl.ds(pl.multiple_of(half * size, size), size)]
        if k == 1:
            size = merge_rows // 2
            return cut(merge_out, 0, parity * 2 + half, size)
        if k < first_down:
            source = (gate_out, up_out)[(k - 2) // 2]
            size = source.shape[0] // 4
            return cut(source, 0, half * 2 + k % 2, size).at[
                :, pl.ds(pl.multiple_of(parity * hidden_half, hidden_half), hidden_half)
            ]
        size = hidden_half // 2
        begin = (k - first_down) * piece_width
        return cut(down_out, 0, parity * 2 + half, size).at[:, begin : begin + piece_width]

    def landing(k, block, part):
        if 2 <= k < first_down:
            target = (gate, up)[(k - 2) // 2]
            size, part = target.shape[1] // 4, part * 2 + k % 2
        else:
            target = (joined, merge)[k] if k < 2 else down.at[k - first_down]
            size = target.shape[1] // 2
        return target.at[block, pl.ds(pl.multiple_of(part * size, size), size)]

    def post(k, there):
        return pltpu.make_async_remote_copy(
            src_ref=outgoing(k, lax.rem(there, 2)),
            dst_ref=landing(k, place, half),
            send_sem=line_send.at[k, there],
            recv_sem=line_recv.at[k, place],
            device_id={"fs": there},
            device_id_type=MESH,
        )

    def arrival(k, block):
        return pltpu.make_async_remote_copy(
            src_ref=landing(k, block, half),
            dst_ref=landing(k, block, half),
            send_sem=line_send.at[k, block],
            recv_sem=line_recv.at[k, block],
            device_id={"fs": block},
            device_id_type=MESH,
        )

    def across(k, block, part):
        return pltpu.make_async_remote_copy(
            src_ref=landing(k, block, part),
            dst_ref=landing(k, block, part),
            send_sem=pair_send.at[k, block],
            recv_sem=pair_recv.at[k, block],
            device_id={"grp": 1 - half},
            device_id_type=MESH,
        )

    def launch(k):
        for there in others:
            post(k, there).start()

    def pump(k, block):
        arrival(k, block).wait_recv()
        across(k, block, half).start()

    def settle(k):
        for block in sources:
            across(k, block, 1 - half).wait_recv()

    def handed(target, stage, step):
        plane = slot if step in (0, 1, 2, 3) else 1 - slot
        holder = seat if step in (0, 1, 2, 4, 5) else row_peer
        place_in = target.at[plane, holder]
        peer = {"tp": core_peer}
        if step in (1, 5):
            peer = {"tp": row_peer}
        if step == 2:
            peer = {"fs": line_peer}
        return pltpu.make_async_remote_copy(
            src_ref=place_in,
            dst_ref=place_in,
            send_sem=share_send.at[stage, step],
            recv_sem=share_recv.at[stage, step],
            device_id=peer,
            device_id_type=MESH,
        )

    def received(target, stage, step):
        plane = slot if step in (0, 1, 3) else 1 - slot
        holder = (core_peer, row_peer, seat, far_peer, core_peer, row_peer, far_peer)[step]
        place_in = target.at[plane, holder]
        return pltpu.make_async_remote_copy(
            src_ref=place_in,
            dst_ref=place_in,
            send_sem=share_send.at[stage, step],
            recv_sem=share_recv.at[stage, step],
            device_id={"tp": core_peer},
            device_id_type=MESH,
        )

    def normalize(source, gain_vector, plane):
        total = jnp.zeros((length, 1), jnp.float32)
        for t in range(row):
            widened = source[plane, t].astype(jnp.float32)
            total = total + jnp.sum(widened * widened, axis=1, keepdims=True)
        scale = lax.rsqrt(total / width + norm_eps)
        for t in range(row):
            span = slice(t * part_width, (t + 1) * part_width)
            scaled = source[plane, t].astype(jnp.float32) * scale * gain_vector[:, span]
            normed[plane, :, span] = scaled.astype(jnp.bfloat16)

    def hand_over(target, stage):
        return [handed(target, stage, step) for step in range(7)]

    def moved(source, target, peer, stage, step):
        return pltpu.make_async_remote_copy(
            src_ref=source,
            dst_ref=target,
            send_sem=sum_send.at[stage, step],
            recv_sem=sum_recv.at[stage, step],
            device_id=peer,
            device_id_type=MESH,
        )

    def share_mid(step):
        plane, kind = step % 2, step // 2
        spot = gathered_mid.at[plane, row_peer if kind == 2 else seat]
        return pltpu.make_async_remote_copy(
            src_ref=spot,
            dst_ref=spot,
            send_sem=share_send.at[1, step],
            recv_sem=share_recv.at[1, step],
            device_id={"tp": core_peer if kind else row_peer},
            device_id_type=MESH,
        )

    def shared_mid(step):
        plane, kind = step % 2, step // 2
        spot = gathered_mid.at[plane, (row_peer, core_peer, far_peer)[kind]]
        return pltpu.make_async_remote_copy(
            src_ref=spot,
            dst_ref=spot,
            send_sem=share_send.at[1, step],
            recv_sem=share_recv.at[1, step],
            device_id={"tp": core_peer},
            device_id_type=MESH,
        )

    def spot(by_row, ahead_part, behind_part):
        return (ahead_part, behind_part) if by_row else (behind_part, ahead_part)

    def chosen(by_row):
        return spot(by_row, column, slot)

    def reducer(partial, core_in, row_in, stage, order, by_row):
        mine = chosen(by_row)[0]
        peer = {"tp": row_peer} if by_row else {"fs": line_peer}
        return [moved(partial.at[1 - core], core_in, {"tp": core_peer}, stage, 0)] + [
            moved(
                partial.at[(core, *spot(by_row, 1 - mine, part))],
                row_in.at[step],
                peer,
                stage,
                1 + step,
            )
            for step, part in enumerate(order)
        ]

    def add_core(partial, core_in, steps, order, by_row):
        mine = chosen(by_row)[0]
        steps[0].wait_recv()
        for step, part in enumerate(order):
            index = spot(by_row, 1 - mine, part)
            total = partial[(core, *index)].astype(jnp.float32) + core_in[index].astype(jnp.float32)
            partial[(core, *index)] = total.astype(jnp.bfloat16)
            steps[1 + step].start()

    def add_row(partial, core_in, row_in, steps, step, part, by_row):
        index = spot(by_row, chosen(by_row)[0], part)
        steps[1 + step].wait_recv()
        return (
            partial[(core, *index)].astype(jnp.float32)
            + core_in[index].astype(jnp.float32)
            + row_in[step].astype(jnp.float32)
        )

    ready(10)
    first = hand_over(gathered, 0)

    for step in (2, 1, 0):
        first[step].start()
    for load, kinds in enumerate(((0,), (1,), (2, 3), (4, 5))):
        ready(load)
        for k in kinds:
            launch(k)

    received(gathered, 0, 1).wait_recv()
    first[3].start()

    pump(0, sources[0])

    received(gathered, 0, 2).wait_recv()
    first[5].start()
    first[4].start()

    pump(0, sources[1])

    received(gathered, 0, 0).wait_recv()
    received(gathered, 0, 3).wait_recv()

    ready(11)
    normalize(gathered, input_gain, slot)

    pump(0, sources[2])

    received(gathered, 0, 5).wait_recv()
    first[6].start()
    received(gathered, 0, 4).wait_recv()
    received(gathered, 0, 6).wait_recv()

    normalize(gathered, input_gain, 1 - slot)

    ready(5)
    settle(0)

    for block in sources:
        pump(1, block)

    for plane in range(2):
        rows_out = jnp.dot(
            normed[plane], joined[...].reshape(width, 4 * group), preferred_element_type=jnp.float32
        )
        for i in range(4):
            projected[i, plane] = (
                rows_out[:, i * group : (i + 1) * group].astype(jnp.bfloat16).astype(jnp.float32)
            )

    head_count = ahead.shape[0] // 2
    head_dim = group // head_count
    lane = lax.broadcasted_iota(jnp.int32, (length, group), 1)
    in_lower = lax.rem(lane, head_dim) < head_dim // 2

    def turned(values):
        partner = jnp.where(
            in_lower,
            pltpu.roll(values, group - head_dim // 2, 1),
            pltpu.roll(values, head_dim // 2, 1),
        )
        return values * cosine[...] + partner * sine_part[...]

    offset = (
        lax.broadcasted_iota(jnp.int32, (length, length), 0)
        - lax.broadcasted_iota(jnp.int32, (length, length), 1)
    ).astype(jnp.float32)

    def log_sigmoid(logit):
        value = jnp.full((8, 128), logit, jnp.float32)
        return (jnp.minimum(value, 0.0) - jnp.log1p(jnp.exp(-jnp.abs(value))))[:1, :1]

    decays = [
        jnp.exp(
            jnp.where(
                offset >= 0,
                log_sigmoid(ahead[slot * head_count + h]) * offset,
                -log_sigmoid(behind[slot * head_count + h]) * offset,
            )
        )
        for h in range(head_count)
    ]
    here = [(lane >= h * head_dim) & (lane < (h + 1) * head_dim) for h in range(head_count)]
    for plane in range(2):
        queries = turned(projected[0, plane])
        key_heads = (turned(projected[1, plane]) * head_dim ** (-0.5)).astype(jnp.bfloat16)
        valued = projected[2, plane]
        result = jnp.zeros((length, group), jnp.float32)
        for h in range(head_count):
            scores = lax.dot_general(
                jnp.where(here[h], queries, 0.0).astype(jnp.bfloat16),
                key_heads,
                (((1,), (1,)), ((), ())),
                preferred_element_type=jnp.float32,
            )
            result = result + jnp.dot(
                (scores * decays[h]).astype(jnp.bfloat16),
                jnp.where(here[h], valued, 0.0).astype(jnp.bfloat16),
                preferred_element_type=jnp.float32,
            )
        center = jnp.zeros((length, group), jnp.float32)
        for h in range(head_count):
            mean = jnp.sum(jnp.where(here[h], result, 0.0), axis=1, keepdims=True) / head_dim
            center = jnp.where(here[h], mean, center)
        centered = result - center
        squared = centered * centered
        factor = jnp.zeros((length, group), jnp.float32)
        for h in range(head_count):
            spread_h = jnp.sum(jnp.where(here[h], squared, 0.0), axis=1, keepdims=True) / head_dim
            factor = jnp.where(here[h], lax.rsqrt(spread_h + group_eps), factor)
        gates = projected[3, plane]
        mixed[plane] = (gates / (1.0 + jnp.exp(-gates)) * (centered * factor)).astype(jnp.bfloat16)

    ready(6)
    settle(1)

    def fill(rows_in, weight, partial, side):
        for x in range(row // 2):
            block = x * 2 + side
            for plane in range(2):
                term = jnp.dot(rows_in[plane], weight[block], preferred_element_type=jnp.float32)
                partial[side, x, plane] = term.astype(jnp.bfloat16)

    steps = reducer(first_partial, first_core, first_row, 0, (0, 1), True) + [
        moved(first_partial.at[core, column, plane], first_line.at[plane], {"fs": line_peer}, 0, 3 + plane)
        for plane in range(2)
    ]
    fill(mixed, merge, first_partial, 1 - core)
    steps[0].start()
    fill(mixed, merge, first_partial, core)

    add_core(first_partial, first_core, steps, (0, 1), True)

    for block in others:
        pump(2, block)
    pump(3, others[0])
    for plane in range(2):
        total = add_row(first_partial, first_core, first_row, steps, plane, plane, True)
        first_partial[core, column, plane] = total.astype(jnp.bfloat16)
        steps[3 + plane].start()

    ready(4)
    for i in range(pieces):
        for there in others:
            post(first_down + i, there).start()

    second = [share_mid(step) for step in range(6)]

    pump(3, others[1])
    pump(3, others[2])

    for block in others:
        pump(4, block)
    pump(5, others[0])
    for plane in range(2):
        steps[3 + plane].wait_recv()
        total = gathered[plane, seat].astype(jnp.float32) + (
            first_partial[core, column, plane].astype(jnp.float32)
            + first_line[plane].astype(jnp.float32)
        )
        gathered_mid[plane, seat] = total.astype(jnp.bfloat16)
        second[plane].start()
        second[2 + plane].start()
        pump(5, others[1 + plane])
    queue = [(first_down + i, block) for i in range(pieces) for block in [line_peer] + crossing]

    def pump_next(count):
        for _ in range(count):
            pump(*queue.pop(0))

    for plane in range(2):
        shared_mid(plane).wait_recv()
        second[4 + plane].start()
        pump_next(len(others))
    for plane in range(2):
        shared_mid(2 + plane).wait_recv()
        shared_mid(4 + plane).wait_recv()
        normalize(gathered_mid, middle_gain, plane)

    ready(7)
    ready(8)
    for k in range(2, first_down):
        settle(k)
    tile = 256
    for plane in range(2):
        for begin in range(0, hidden_half, tile):
            columns = slice(begin, min(begin + tile, hidden_half))
            gate_act, up_act = [
                jnp.dot(
                    normed[plane],
                    weight[:, :, columns].reshape(width, -1),
                    preferred_element_type=jnp.float32,
                )
                for weight in (gate, up)
            ]
            hidden[plane, :, columns] = (gate_act / (1.0 + jnp.exp(-gate_act)) * up_act).astype(
                jnp.bfloat16
            )
            if plane == 0:
                pump_next(1)

    pump_next(1)

    ready(9)
    by_rows = [i in (0, 2) for i in range(pieces)]
    ends = []
    for i in range(pieces):
        mine, other = chosen(by_rows[i])
        ends.append(
            reducer(
                last_partial.at[i],
                last_core.at[i],
                last_row.at[i],
                1 + i,
                (1 - other, other),
                by_rows[i],
            )
            + [
                moved(
                    last_partial.at[(i, core, *spot(by_rows[i], mine, 1 - other))],
                    last_line.at[i],
                    {"fs": line_peer} if by_rows[i] else {"tp": row_peer},
                    1 + i,
                    3,
                )
            ]
        )

    def last_sum(i, step):
        other = chosen(by_rows[i])[1]
        part = other if step else 1 - other
        return add_row(
            last_partial.at[i], last_core.at[i], last_row.at[i], ends[i], step, part, by_rows[i]
        )

    def pass_line(i):
        total = last_sum(i, 0)
        mine, other = chosen(by_rows[i])
        last_partial[(i, core, *spot(by_rows[i], mine, 1 - other))] = total.astype(jnp.bfloat16)
        ends[i][3].start()

    written = [
        pltpu.make_async_copy(
            finished.at[:, i * piece_width : (i + 1) * piece_width],
            out.at[:, i * piece_width : (i + 1) * piece_width],
            out_sem.at[i],
        )
        for i in range(pieces)
    ]

    def finish(i):
        span = slice(i * piece_width, (i + 1) * piece_width)
        total = gathered_mid[slot, seat, :, span].astype(jnp.float32) + last_sum(i, 1)
        ends[i][3].wait_recv()
        finished[:, span] = (total + last_line[i].astype(jnp.float32)).astype(jnp.bfloat16)
        written[i].start()

    for i in range(pieces):
        settle(first_down + i)
        fill(hidden, down.at[i], last_partial.at[i], 1 - core)
        ends[i][0].start()
        if queue:
            pump_next(1)
        fill(hidden, down.at[i], last_partial.at[i], core)
        if queue:
            pump_next(1)
        other = chosen(by_rows[i])[1]
        add_core(last_partial.at[i], last_core.at[i], ends[i], (1 - other, other), by_rows[i])
        if i > 1:
            pass_line(i - 2)
    for i in range(max(0, pieces - 2), pieces):
        pass_line(i)

    for i in range(pieces):
        finish(i)

    for copy in written:
        copy.wait()
    for copy in first + second + steps:
        copy.wait_send()
    for group_steps in ends:
        for copy in group_steps:
            copy.wait_send()
    for k in range(first_down + pieces):
        for there in others:
            post(k, there).wait_send()
            across(k, there, half).wait_send()


def paired_call(
    sizes, flat, input_gain, middle_gain, decays, tables, quads, merge_weight, gate_weight, up_weight, down_weight
):
    line, row = sizes["fs"], sizes["tp"]
    bf16 = jnp.bfloat16
    length, part_width = flat.shape
    depth, ret_width = quads[0].shape
    hidden_half, group = gate_weight.shape[1] // 2, ret_width // 2
    pieces = 4
    piece_width = down_weight.shape[1] // pieces
    kinds = 6 + pieces
    anywhere = pl.BlockSpec(memory_space=pl.ANY)
    in_smem = pl.BlockSpec(memory_space=pltpu.SMEM)

    def sums(lead, columns, last):
        return [
            pltpu.VMEM(lead + (2, row // 2, 2, length, columns), bf16),
            pltpu.VMEM(lead + (row // 2, 2, length, columns), bf16),
            pltpu.VMEM(lead + (2, length, columns), bf16),
            pltpu.VMEM(lead + last + (length, columns), bf16),
        ]

    dma = pltpu.SemaphoreType.DMA
    return pl.pallas_call(
        functools.partial(paired_kernel, sizes),
        out_shape=jax.ShapeDtypeStruct(flat.shape, bf16),
        in_specs=[anywhere] * 3 + [in_smem] * 2 + [anywhere] * 10,
        out_specs=anywhere,
        scratch_shapes=[
            pltpu.VMEM((1, row * part_width), jnp.float32),
            pltpu.VMEM((1, row * part_width), jnp.float32),
            pltpu.VMEM(tables[0].shape, jnp.float32),
            pltpu.VMEM(tables[1].shape, jnp.float32),
            pltpu.VMEM(flat.shape, bf16),
            pltpu.VMEM((2, depth, 4 * group), bf16),
            pltpu.VMEM(merge_weight.shape, bf16),
            pltpu.VMEM(gate_weight.shape, bf16),
            pltpu.VMEM(up_weight.shape, bf16),
            pltpu.VMEM(down_weight.shape, bf16),
            pltpu.VMEM((line, depth, 4 * group), bf16),
            pltpu.VMEM((line, merge_weight.shape[0] // 2, part_width), bf16),
            pltpu.VMEM((line, depth, hidden_half), bf16),
            pltpu.VMEM((line, depth, hidden_half), bf16),
            pltpu.VMEM((pieces, line, hidden_half, piece_width), bf16),
            pltpu.VMEM((2, row, length, part_width), bf16),
            pltpu.VMEM((2, row, length, part_width), bf16),
            pltpu.VMEM((2, length, row * part_width), bf16),
            pltpu.VMEM((4, 2, length, group), jnp.float32),
            pltpu.VMEM((2, length, group), bf16),
            pltpu.VMEM((2, length, hidden_half), bf16),
        ]
        + sums((), part_width, (2,))
        + sums((pieces,), piece_width, ())
        + [
            dma((25 + pieces,)),
            dma((kinds, line)),
            dma((kinds, line)),
            dma((kinds, line)),
            dma((kinds, line)),
            dma((2, 7)),
            dma((2, 7)),
            dma((1 + pieces, 5)),
            dma((1 + pieces, 5)),
            dma((pieces,)),
        ],
        compiler_params=pltpu.CompilerParams(
            collective_id=0, has_side_effects=True, vmem_limit_bytes=60 << 20
        ),
    )(
        flat,
        input_gain[None, :],
        middle_gain[None, :],
        *decays,
        *tables,
        *quads,
        merge_weight,
        gate_weight,
        up_weight,
        down_weight,
    )


def on_device(
    sizes,
    tokens,
    input_gain,
    query_weight,
    key_weight,
    value_weight,
    output_gate_matrix,
    forward_decay,
    backward_decay,
    merge_weight,
    middle_gain,
    gate_weight,
    up_weight,
    down_weight,
):
    seq_count, length, part_width = tokens.shape
    flat = tokens.reshape(seq_count * length, part_width)
    quads = (query_weight, key_weight, value_weight, output_gate_matrix)
    paired = (
        sizes["grp"] == 2
        and sizes["fs"] == sizes["tp"] == 4
        and seq_count == 1
        and query_weight.shape[1] % 256 == 0
        and forward_decay.shape[0] % 2 == 0
        and gate_weight.shape[1] % 256 == 0
        and down_weight.shape[1] == part_width
        and part_width % 256 == 0
    )
    if paired:
        head_count = forward_decay.shape[0] // 2
        head_dim = query_weight.shape[1] // (2 * head_count)
        layer_out = paired_call(
            sizes,
            flat,
            input_gain,
            middle_gain,
            (forward_decay, backward_decay),
            turn_tables(length, head_dim, head_count),
            quads,
            merge_weight,
            gate_weight,
            up_weight,
            down_weight,
        )
        return layer_out.reshape(seq_count, length, part_width)
    joined = jnp.concatenate(quads, axis=1)
    shards = (joined, merge_weight, gate_weight, up_weight, down_weight)
    line, copies, row = sizes["fs"], sizes["grp"], sizes["tp"]
    down_width = down_weight.shape[1]
    parts = down_width // 256 if line == row and down_width % 256 == 0 else 1
    down_piece = jax.ShapeDtypeStruct((down_weight.shape[0], down_width // parts), jnp.bfloat16)
    landing = shards[:4] + (down_piece,) * parts
    count = len(landing)
    width, ret_width, hidden_width = row * part_width, query_weight.shape[1], gate_weight.shape[1]
    head_count = forward_decay.shape[0]
    tables = turn_tables(length, ret_width // head_count, head_count)
    in_vmem = pl.BlockSpec(memory_space=pltpu.VMEM)
    in_smem = pl.BlockSpec(memory_space=pltpu.SMEM)
    bf16 = jnp.bfloat16
    layer_out = pl.pallas_call(
        functools.partial(layer_kernel, sizes),
        out_shape=jax.ShapeDtypeStruct(flat.shape, bf16),
        in_specs=[in_vmem] * 3
        + [in_smem] * 2
        + [in_vmem] * 2
        + [pl.BlockSpec(memory_space=pl.ANY)] * len(shards),
        out_specs=in_vmem,
        scratch_shapes=[pltpu.VMEM((line,) + w.shape, w.dtype) for w in landing]
        + [
            pltpu.VMEM((row, length, part_width), bf16),
            pltpu.VMEM((row, length, part_width), bf16),
            pltpu.VMEM((length, width), bf16),
            pltpu.VMEM((4, length, ret_width), jnp.float32),
            pltpu.VMEM((length, ret_width), bf16),
            pltpu.VMEM((length, hidden_width), bf16),
            pltpu.VMEM((row, length, part_width), bf16),
            pltpu.VMEM((row - 1, length, part_width), bf16),
            pltpu.SemaphoreType.DMA((count,)),
            pltpu.SemaphoreType.DMA((count, 2, line)),
            pltpu.SemaphoreType.DMA((count, 2, line)),
            pltpu.SemaphoreType.DMA((count, 2, line, copies - 1)),
            pltpu.SemaphoreType.DMA((count, 2, line, copies - 1)),
            pltpu.SemaphoreType.DMA((3 + parts, row - 1)),
            pltpu.SemaphoreType.DMA((3 + parts, row - 1)),
            pltpu.SemaphoreType.DMA,
            pltpu.VMEM((parts, row, length, part_width // parts), bf16),
            pltpu.VMEM((parts, row - 1, length, part_width // parts), bf16),
        ],
        compiler_params=pltpu.CompilerParams(
            collective_id=0, has_side_effects=True, vmem_limit_bytes=58 << 20
        ),
    )(
        flat,
        input_gain[None, :],
        middle_gain[None, :],
        jax.nn.log_sigmoid(forward_decay),
        jax.nn.log_sigmoid(backward_decay),
        *tables,
        *shards,
    )
    return layer_out.reshape(seq_count, length, part_width)


def solution(mesh):
    placed = (
        P(("grp", "fs"), None, "tp"),
        P(),
        P("fs", "tp"),
        P("fs", "tp"),
        P("fs", "tp"),
        P("fs", "tp"),
        P("tp"),
        P("tp"),
        P("tp", "fs"),
        P(),
        P("fs", "tp"),
        P("fs", "tp"),
        P("tp", "fs"),
    )
    return jax.shard_map(
        functools.partial(on_device, dict(mesh.shape)),
        mesh=mesh,
        in_specs=placed,
        out_specs=P(("grp", "fs"), None, "tp"),
        check_vma=False,
    )
```

```python
import functools

import jax
import jax.numpy as jnp
import numpy as np
from jax import lax
from jax.experimental import pallas as pl
from jax.experimental.pallas import tpu as pltpu
from jax.sharding import PartitionSpec as P

norm_eps = 1e-06
group_eps = 1e-05
rope_base = 10000.0


def turn_tables(length, head_dim, head_count):
    half_dim = head_dim // 2
    inverse = rope_base ** (-np.arange(half_dim) / half_dim)
    angles = np.arange(length)[:, None] * inverse[None, :]
    cosine, sine_part = np.cos(angles), np.sin(angles)
    return (
        np.tile(np.concatenate([cosine, cosine], axis=1), (1, head_count)).astype(np.float32),
        np.tile(np.concatenate([-sine_part, sine_part], axis=1), (1, head_count)).astype(np.float32),
    )


MESH = pl.DeviceIdType.MESH


def layer_kernel(
    sizes,
    tokens,
    input_gain,
    middle_gain,
    rate_ahead,
    rate_behind,
    cosine,
    sine_part,
    joined_shard,
    merge_shard,
    gate_shard,
    up_shard,
    down_shard,
    out,
    joined,
    merge,
    gate,
    up,
    *rest,
):
    line, copies, row = sizes["fs"], sizes["grp"], sizes["tp"]
    parts = len(rest) - 18
    downs, partial_ends, received_ends = rest[:parts], rest[-2], rest[-1]
    (
        gathered,
        gathered_mid,
        normed,
        projected,
        mixed,
        hidden,
        partial,
        received,
        own_sem,
        line_send,
        line_recv,
        pair_send,
        pair_recv,
        row_send,
        row_recv,
        self_sem,
    ) = rest[parts:-2]
    piece_width = downs[0].shape[2]
    shards = (joined_shard, merge_shard, gate_shard, up_shard) + tuple(
        down_shard if parts == 1 else down_shard.at[:, pl.ds(i * piece_width, piece_width)]
        for i in range(parts)
    )
    slots = (joined, merge, gate, up) + tuple(downs)
    count = len(slots)
    length, part_width = tokens.shape
    width = row * part_width
    seat = lax.axis_index("tp")
    place = lax.axis_index("fs")
    half = lax.axis_index("grp")

    barrier = pltpu.get_barrier_semaphore()
    for shift in (1, -1):
        there = place + shift

        @pl.when((there >= 0) & (there < line))
        def _():
            pl.semaphore_signal(barrier, inc=1, device_id={"fs": there}, device_id_type=MESH)

    for other in range(1, copies):
        pl.semaphore_signal(
            barrier,
            inc=1,
            device_id={"grp": lax.rem(half + other, copies)},
            device_id_type=MESH,
        )
    for other in range(1, row):
        pl.semaphore_signal(
            barrier,
            inc=1,
            device_id={"tp": lax.rem(seat + other, row)},
            device_id_type=MESH,
        )
    own = [pltpu.make_async_copy(shards[k], slots[k].at[place], own_sem.at[k]) for k in range(count)]
    for copy in own:
        copy.start()
    neighbours = (place > 0).astype(jnp.int32) + (place < line - 1).astype(jnp.int32)
    mine = pltpu.make_async_copy(tokens, gathered.at[seat], self_sem)
    mine.start()
    pl.semaphore_wait(barrier, neighbours + copies - 1 + row - 1)

    def piece(k, block, part):
        rows = slots[k].shape[1] // copies
        return slots[k].at[block, pl.ds(pl.multiple_of(part * rows, rows), rows), :]

    def hop(k, way, step):
        shift = 1 if way == 0 else -1
        block = place - shift * step
        return pltpu.make_async_remote_copy(
            src_ref=piece(k, block, half),
            dst_ref=piece(k, block, half),
            send_sem=line_send.at[k, way, step],
            recv_sem=line_recv.at[k, way, step],
            device_id={"fs": place + shift},
            device_id_type=MESH,
        )

    def arrival(k, way, step):
        shift = 1 if way == 0 else -1
        block = place - shift * step
        return pltpu.make_async_remote_copy(
            src_ref=piece(k, block, half),
            dst_ref=piece(k, block, half),
            send_sem=line_send.at[k, way, step - 1],
            recv_sem=line_recv.at[k, way, step - 1],
            device_id={"fs": place - shift},
            device_id_type=MESH,
        )

    def across(k, way, step, other):
        shift = 1 if way == 0 else -1
        block = place - shift * step
        return pltpu.make_async_remote_copy(
            src_ref=piece(k, block, half),
            dst_ref=piece(k, block, half),
            send_sem=pair_send.at[k, way, step - 1, other - 1],
            recv_sem=pair_recv.at[k, way, step - 1, other - 1],
            device_id={"grp": lax.rem(half + other, copies)},
            device_id_type=MESH,
        )

    def landed(k, way, step, other):
        shift = 1 if way == 0 else -1
        block = place - shift * step
        source = lax.rem(half + copies - other, copies)
        return pltpu.make_async_remote_copy(
            src_ref=piece(k, block, source),
            dst_ref=piece(k, block, source),
            send_sem=pair_send.at[k, way, step - 1, other - 1],
            recv_sem=pair_recv.at[k, way, step - 1, other - 1],
            device_id={"grp": source},
            device_id_type=MESH,
        )

    def has(way, step):
        return place >= step if way == 0 else place + step < line

    def goes(way):
        return place < line - 1 if way == 0 else place > 0

    def launch(k):
        own[k].wait()
        for way in range(2):

            @pl.when(goes(way))
            def _():
                hop(k, way, 0).start()

    def pump(k):
        for step in range(1, line):
            for way in range(2):

                @pl.when(has(way, step))
                def _():
                    arrival(k, way, step).wait_recv()
                    for other in range(1, copies):
                        across(k, way, step, other).start()

                @pl.when(has(way, step) & goes(way))
                def _():
                    hop(k, way, step).start()

    def settle(k):
        for step in range(1, line):
            for way in range(2):

                @pl.when(has(way, step))
                def _():
                    for other in range(1, copies):
                        landed(k, way, step, other).wait_recv()

    def drain(k):
        for way in range(2):
            for step in range(line):

                @pl.when((has(way, step) if step else True) & goes(way))
                def _():
                    hop(k, way, step).wait_send()

                if step:

                    @pl.when(has(way, step))
                    def _():
                        for other in range(1, copies):
                            across(k, way, step, other).wait_send()

    def spread(source, target, stage):
        return [
            pltpu.make_async_remote_copy(
                src_ref=source,
                dst_ref=target.at[seat],
                send_sem=row_send.at[stage, other - 1],
                recv_sem=row_recv.at[stage, other - 1],
                device_id={"tp": lax.rem(seat + other, row)},
                device_id_type=MESH,
            )
            for other in range(1, row)
        ]

    def spread_in(target, stage):
        sources = [lax.rem(seat + row - other, row) for other in range(1, row)]
        return [
            pltpu.make_async_remote_copy(
                src_ref=target.at[source],
                dst_ref=target.at[source],
                send_sem=row_send.at[stage, other],
                recv_sem=row_recv.at[stage, other],
                device_id={"tp": source},
                device_id_type=MESH,
            )
            for other, source in enumerate(sources)
        ]

    def scatter(source, target, stage, other):
        there = lax.rem(seat + other, row)
        return pltpu.make_async_remote_copy(
            src_ref=source.at[there],
            dst_ref=target.at[other - 1],
            send_sem=row_send.at[stage, other - 1],
            recv_sem=row_recv.at[stage, other - 1],
            device_id={"tp": there},
            device_id_type=MESH,
        )

    def normalize(source, gain_vector):
        total = jnp.zeros((length, 1), jnp.float32)
        for t in range(row):
            widened = source[t].astype(jnp.float32)
            total = total + jnp.sum(widened * widened, axis=1, keepdims=True)
        scale = lax.rsqrt(total / width + norm_eps)
        for t in range(row):
            span = slice(t * part_width, (t + 1) * part_width)
            scaled = source[t].astype(jnp.float32) * scale * gain_vector[:, span]
            normed[:, span] = scaled.astype(jnp.bfloat16)

    def times(weight, columns):
        block = weight[:, :, columns]
        return jnp.dot(
            normed[...], block.reshape(-1, block.shape[2]), preferred_element_type=jnp.float32
        )

    def shares(rows_in, weight, target):
        step = weight.shape[2]
        for block in range(line):
            term = jnp.dot(rows_in[...], weight[block], preferred_element_type=jnp.float32)
            begin = block * step
            inner = begin % part_width
            target[begin // part_width, :, inner : inner + step] = term.astype(jnp.bfloat16)

    def finish(i):
        settle(4 + i)
        if parts == 1:
            shares(hidden, downs[i], partial_ends.at[i])
        else:
            for j in range(row):
                blocks = [jnp.dot(
                    hidden[...], downs[i][j * line // row + c], preferred_element_type=jnp.float32
                ) for c in range(max(1, line // row))]
                for c, term in enumerate(blocks):
                    partial_ends[i, j, :, c * piece_width : (c + 1) * piece_width] = term.astype(
                        jnp.bfloat16
                    )
        for other in range(1, row):
            scatter(partial_ends.at[i], received_ends.at[i], 3 + i, other).start()

    def collect(i):
        span = slice(None) if parts == 1 else slice(i * piece_width, (i + 1) * piece_width)
        total = gathered_mid[seat, :, span].astype(jnp.float32)
        total = total + partial_ends[i, seat].astype(jnp.float32)
        for other in range(1, row):
            scatter(partial_ends.at[i], received_ends.at[i], 3 + i, other).wait_recv()
            total = total + received_ends[i, other - 1].astype(jnp.float32)
        out[:, span] = total.astype(jnp.bfloat16)

    launch(0)
    first = spread(tokens, gathered, 0)
    for copy in first:
        copy.start()
    launch(1)
    mine.wait()
    for copy in spread_in(gathered, 0):
        copy.wait_recv()
    normalize(gathered, input_gain)

    pump(0)
    launch(2)
    settle(0)
    ret_width = projected.shape[2]
    for t in range(4):
        projected[t] = (
            times(joined, slice(t * ret_width, (t + 1) * ret_width))
            .astype(jnp.bfloat16)
            .astype(jnp.float32)
        )
    pump(1)
    launch(3)

    head_count = rate_ahead.shape[0]
    head_dim = ret_width // head_count
    lane = lax.broadcasted_iota(jnp.int32, (length, ret_width), 1)
    in_lower = lax.rem(lane, head_dim) < head_dim // 2

    def turned(values):
        partner = jnp.where(
            in_lower,
            pltpu.roll(values, ret_width - head_dim // 2, 1),
            pltpu.roll(values, head_dim // 2, 1),
        )
        return values * cosine[...] + partner * sine_part[...]

    queries = turned(projected[0])
    key_heads = (turned(projected[1]) * head_dim ** (-0.5)).astype(jnp.bfloat16)
    valued = projected[2]
    offset = (
        lax.broadcasted_iota(jnp.int32, (length, length), 0)
        - lax.broadcasted_iota(jnp.int32, (length, length), 1)
    ).astype(jnp.float32)
    result = jnp.zeros((length, ret_width), jnp.float32)
    for h in range(head_count):
        here = (lane >= h * head_dim) & (lane < (h + 1) * head_dim)
        scores = lax.dot_general(
            jnp.where(here, queries, 0.0).astype(jnp.bfloat16),
            key_heads,
            (((1,), (1,)), ((), ())),
            preferred_element_type=jnp.float32,
        )
        decay = jnp.exp(jnp.where(offset >= 0, rate_ahead[h] * offset, -rate_behind[h] * offset))
        result = result + jnp.dot(
            (scores * decay).astype(jnp.bfloat16),
            jnp.where(here, valued, 0.0).astype(jnp.bfloat16),
            preferred_element_type=jnp.float32,
        )
    center = jnp.zeros((length, ret_width), jnp.float32)
    for h in range(head_count):
        here = (lane >= h * head_dim) & (lane < (h + 1) * head_dim)
        mean = jnp.sum(jnp.where(here, result, 0.0), axis=1, keepdims=True) / head_dim
        center = jnp.where(here, mean, center)
    centered = result - center
    squared = centered * centered
    factor = jnp.zeros((length, ret_width), jnp.float32)
    for h in range(head_count):
        here = (lane >= h * head_dim) & (lane < (h + 1) * head_dim)
        spread_h = jnp.sum(jnp.where(here, squared, 0.0), axis=1, keepdims=True) / head_dim
        factor = jnp.where(here, lax.rsqrt(spread_h + group_eps), factor)
    gates = projected[3]
    mixed[...] = (gates / (1.0 + jnp.exp(-gates)) * (centered * factor)).astype(jnp.bfloat16)

    settle(1)
    shares(mixed, merge, partial)
    for other in range(1, row):
        scatter(partial, received, 1, other).start()
    pump(2)
    total = tokens[...].astype(jnp.float32) + partial[seat].astype(jnp.float32)
    for other in range(1, row):
        scatter(partial, received, 1, other).wait_recv()
        total = total + received[other - 1].astype(jnp.float32)
    gathered_mid[seat] = total.astype(jnp.bfloat16)
    second = spread(gathered_mid.at[seat], gathered_mid, 2)
    for copy in second:
        copy.start()
    pump(3)
    launch(4)
    if parts > 1:
        launch(5)
    for copy in spread_in(gathered_mid, 2):
        copy.wait_recv()
    normalize(gathered_mid, middle_gain)
    settle(2)
    settle(3)
    hidden_width = hidden.shape[1]
    tile = 256 if hidden_width % 256 == 0 else 128

    @pl.loop(0, hidden_width // tile)
    def _(index):
        columns = pl.ds(pl.multiple_of(index * tile, tile), tile)
        gate_act = times(gate, columns)
        up_act = times(up, columns)
        hidden[:, columns] = (gate_act / (1.0 + jnp.exp(-gate_act)) * up_act).astype(jnp.bfloat16)

    for i in range(parts):
        pump(4 + i)
        if i + 2 < parts:
            launch(6 + i)
        if i:
            finish(i - 1)
    finish(parts - 1)
    for i in range(parts):
        collect(i)
    for copy in first + second:
        copy.wait_send()
    for other in range(1, row):
        scatter(partial, received, 1, other).wait_send()
        for i in range(parts):
            scatter(partial_ends.at[i], received_ends.at[i], 3 + i, other).wait_send()
    for k in range(count):
        drain(k)


def paired_kernel(
    sizes,
    tokens,
    input_gain_in,
    middle_gain_in,
    ahead,
    behind,
    cosine_in,
    sine_in,
    query_shard,
    key_shard,
    value_shard,
    output_gate_shard,
    merge_shard,
    gate_shard,
    up_shard,
    down_shard,
    out,
    input_gain,
    middle_gain,
    cosine,
    sine_part,
    finished,
    joined_out,
    merge_out,
    gate_out,
    up_out,
    down_out,
    joined,
    merge,
    gate,
    up,
    down,
    gathered,
    gathered_mid,
    normed,
    projected,
    mixed,
    hidden,
    first_partial,
    first_core,
    first_row,
    first_line,
    last_partial,
    last_core,
    last_row,
    last_line,
    own_sem,
    line_send,
    line_recv,
    pair_send,
    pair_recv,
    share_send,
    share_recv,
    sum_send,
    sum_recv,
    out_sem,
):
    line, row = sizes["fs"], sizes["tp"]
    pieces = down.shape[0]
    piece_width = down.shape[3]
    length, part_width = tokens.shape
    width = row * part_width
    seat = lax.axis_index("tp")
    place = lax.axis_index("fs")
    half = lax.axis_index("grp")
    core, column = lax.rem(seat, 2), seat // 2
    slot = lax.rem(place, 2)
    core_peer = seat + 1 - 2 * core
    row_peer = lax.rem(seat + 2, row)
    far_peer = lax.rem(core_peer + 2, row)
    line_peer = place + 1 - 2 * slot
    sign = 1 - 2 * (place // (line // 2))
    others = [lax.rem(place + sign * step + line, line) for step in range(1, line)]
    facing = jnp.where(place < line // 2, line // 2, line // 2 - 1)
    crossing = [facing + sign * step for step in range(line // 2)]
    sources = [facing, line_peer] + crossing[1:]

    barrier = pltpu.get_barrier_semaphore()
    for there in others:
        pl.semaphore_signal(barrier, inc=1, device_id={"fs": there}, device_id_type=MESH)
    pl.semaphore_signal(barrier, inc=1, device_id={"grp": 1 - half}, device_id_type=MESH)
    for there in (core_peer, row_peer):
        pl.semaphore_signal(barrier, inc=1, device_id={"tp": there}, device_id_type=MESH)

    group = joined_out.shape[2] // 4
    quads = (query_shard, key_shard, value_shard, output_gate_shard)
    merge_rows = merge.shape[1]
    hidden_half = gate.shape[2]

    def cut(ref, axis, part, size):
        window = pl.ds(pl.multiple_of(part * size, size), size)
        return ref.at[window] if axis == 0 else ref.at[:, window]

    loads = [
        [
            (quad.at[:, p * group : (p + 1) * group], joined_out.at[p, :, i * group : (i + 1) * group])
            for p in range(2)
            for i, quad in enumerate(quads)
        ],
        [(merge_shard, merge_out)],
        [(gate_shard, gate_out)],
        [(up_shard, up_out)],
        [(down_shard, down_out)],
        [
            (cut(quad, 1, slot, group), joined.at[place, :, i * group : (i + 1) * group])
            for i, quad in enumerate(quads)
        ],
        [(cut(merge_shard, 0, slot, merge_rows), merge.at[place])],
        [(cut(gate_shard, 1, slot, hidden_half), gate.at[place])],
        [(cut(up_shard, 1, slot, hidden_half), up.at[place])],
        [
            (
                cut(down_shard, 0, slot, hidden_half).at[:, i * piece_width : (i + 1) * piece_width],
                down.at[i, place],
            )
            for i in range(pieces)
        ],
        [(tokens, gathered.at[slot, seat])],
        [
            (input_gain_in, input_gain),
            (middle_gain_in, middle_gain),
            (cosine_in, cosine),
            (sine_in, sine_part),
        ],
    ]
    own, index = [], 0
    for pairs in loads:
        own.append([])
        for source, target in pairs:
            own[-1].append(pltpu.make_async_copy(source, target, own_sem.at[index]))
            index += 1
    for copies in (own[-2], *own[:-2], own[-1]):
        for copy in copies:
            copy.start()
    pl.semaphore_wait(barrier, line - 1 + 1 + 2)

    def ready(k):
        for copy in own[k]:
            copy.wait()

    first_down = 6

    def outgoing(k, parity):
        if k == 0:
            size = joined.shape[1] // 2
            return joined_out.at[parity, pl.ds(pl.multiple_of(half * size, size), size)]
        if k == 1:
            size = merge_rows // 2
            return cut(merge_out, 0, parity * 2 + half, size)
        if k < first_down:
            source = (gate_out, up_out)[(k - 2) // 2]
            size = source.shape[0] // 4
            return cut(source, 0, half * 2 + k % 2, size).at[
                :, pl.ds(pl.multiple_of(parity * hidden_half, hidden_half), hidden_half)
            ]
        size = hidden_half // 2
        begin = (k - first_down) * piece_width
        return cut(down_out, 0, parity * 2 + half, size).at[:, begin : begin + piece_width]

    def landing(k, block, part):
        if 2 <= k < first_down:
            target = (gate, up)[(k - 2) // 2]
            size, part = target.shape[1] // 4, part * 2 + k % 2
        else:
            target = (joined, merge)[k] if k < 2 else down.at[k - first_down]
            size = target.shape[1] // 2
        return target.at[block, pl.ds(pl.multiple_of(part * size, size), size)]

    def post(k, there):
        return pltpu.make_async_remote_copy(
            src_ref=outgoing(k, lax.rem(there, 2)),
            dst_ref=landing(k, place, half),
            send_sem=line_send.at[k, there],
            recv_sem=line_recv.at[k, place],
            device_id={"fs": there},
            device_id_type=MESH,
        )

    def arrival(k, block):
        return pltpu.make_async_remote_copy(
            src_ref=landing(k, block, half),
            dst_ref=landing(k, block, half),
            send_sem=line_send.at[k, block],
            recv_sem=line_recv.at[k, block],
            device_id={"fs": block},
            device_id_type=MESH,
        )

    def across(k, block, part):
        return pltpu.make_async_remote_copy(
            src_ref=landing(k, block, part),
            dst_ref=landing(k, block, part),
            send_sem=pair_send.at[k, block],
            recv_sem=pair_recv.at[k, block],
            device_id={"grp": 1 - half},
            device_id_type=MESH,
        )

    def launch(k):
        for there in others:
            post(k, there).start()

    def pump(k, block):
        arrival(k, block).wait_recv()
        across(k, block, half).start()

    def settle(k):
        for block in sources:
            across(k, block, 1 - half).wait_recv()

    def handed(target, stage, step):
        plane = slot if step in (0, 1, 2, 3) else 1 - slot
        holder = seat if step in (0, 1, 2, 4, 5) else row_peer
        place_in = target.at[plane, holder]
        peer = {"tp": core_peer}
        if step in (1, 5):
            peer = {"tp": row_peer}
        if step == 2:
            peer = {"fs": line_peer}
        return pltpu.make_async_remote_copy(
            src_ref=place_in,
            dst_ref=place_in,
            send_sem=share_send.at[stage, step],
            recv_sem=share_recv.at[stage, step],
            device_id=peer,
            device_id_type=MESH,
        )

    def received(target, stage, step):
        plane = slot if step in (0, 1, 3) else 1 - slot
        holder = (core_peer, row_peer, seat, far_peer, core_peer, row_peer, far_peer)[step]
        place_in = target.at[plane, holder]
        return pltpu.make_async_remote_copy(
            src_ref=place_in,
            dst_ref=place_in,
            send_sem=share_send.at[stage, step],
            recv_sem=share_recv.at[stage, step],
            device_id={"tp": core_peer},
            device_id_type=MESH,
        )

    def normalize(source, gain_vector, plane):
        total = jnp.zeros((length, 1), jnp.float32)
        for t in range(row):
            widened = source[plane, t].astype(jnp.float32)
            total = total + jnp.sum(widened * widened, axis=1, keepdims=True)
        scale = lax.rsqrt(total / width + norm_eps)
        for t in range(row):
            span = slice(t * part_width, (t + 1) * part_width)
            scaled = source[plane, t].astype(jnp.float32) * scale * gain_vector[:, span]
            normed[plane, :, span] = scaled.astype(jnp.bfloat16)

    def hand_over(target, stage):
        return [handed(target, stage, step) for step in range(7)]

    def moved(source, target, peer, stage, step):
        return pltpu.make_async_remote_copy(
            src_ref=source,
            dst_ref=target,
            send_sem=sum_send.at[stage, step],
            recv_sem=sum_recv.at[stage, step],
            device_id=peer,
            device_id_type=MESH,
        )

    def share_mid(step):
        plane, kind = step % 2, step // 2
        spot = gathered_mid.at[plane, row_peer if kind == 2 else seat]
        return pltpu.make_async_remote_copy(
            src_ref=spot,
            dst_ref=spot,
            send_sem=share_send.at[1, step],
            recv_sem=share_recv.at[1, step],
            device_id={"tp": core_peer if kind else row_peer},
            device_id_type=MESH,
        )

    def shared_mid(step):
        plane, kind = step % 2, step // 2
        spot = gathered_mid.at[plane, (row_peer, core_peer, far_peer)[kind]]
        return pltpu.make_async_remote_copy(
            src_ref=spot,
            dst_ref=spot,
            send_sem=share_send.at[1, step],
            recv_sem=share_recv.at[1, step],
            device_id={"tp": core_peer},
            device_id_type=MESH,
        )

    def spot(by_row, ahead_part, behind_part):
        return (ahead_part, behind_part) if by_row else (behind_part, ahead_part)

    def chosen(by_row):
        return spot(by_row, column, slot)

    def reducer(partial, core_in, row_in, stage, order, by_row):
        mine = chosen(by_row)[0]
        peer = {"tp": row_peer} if by_row else {"fs": line_peer}
        return [moved(partial.at[1 - core], core_in, {"tp": core_peer}, stage, 0)] + [
            moved(
                partial.at[(core, *spot(by_row, 1 - mine, part))],
                row_in.at[step],
                peer,
                stage,
                1 + step,
            )
            for step, part in enumerate(order)
        ]

    def add_core(partial, core_in, steps, order, by_row):
        mine = chosen(by_row)[0]
        steps[0].wait_recv()
        for step, part in enumerate(order):
            index = spot(by_row, 1 - mine, part)
            total = partial[(core, *index)].astype(jnp.float32) + core_in[index].astype(jnp.float32)
            partial[(core, *index)] = total.astype(jnp.bfloat16)
            steps[1 + step].start()

    def add_row(partial, core_in, row_in, steps, step, part, by_row):
        index = spot(by_row, chosen(by_row)[0], part)
        steps[1 + step].wait_recv()
        return (
            partial[(core, *index)].astype(jnp.float32)
            + core_in[index].astype(jnp.float32)
            + row_in[step].astype(jnp.float32)
        )

    ready(10)
    first = hand_over(gathered, 0)
    for step in (2, 1, 0):
        first[step].start()
    for load, kinds in enumerate(((0,), (1,), (2, 3), (4, 5))):
        ready(load)
        for k in kinds:
            launch(k)
    received(gathered, 0, 1).wait_recv()
    first[3].start()
    pump(0, sources[0])
    received(gathered, 0, 2).wait_recv()
    first[5].start()
    first[4].start()
    pump(0, sources[1])
    received(gathered, 0, 0).wait_recv()
    received(gathered, 0, 3).wait_recv()
    ready(11)
    normalize(gathered, input_gain, slot)
    pump(0, sources[2])
    received(gathered, 0, 5).wait_recv()
    first[6].start()
    received(gathered, 0, 4).wait_recv()
    received(gathered, 0, 6).wait_recv()
    normalize(gathered, input_gain, 1 - slot)
    ready(5)
    settle(0)
    for block in sources:
        pump(1, block)
    for plane in range(2):
        rows_out = jnp.dot(
            normed[plane], joined[...].reshape(width, 4 * group), preferred_element_type=jnp.float32
        )
        for i in range(4):
            projected[i, plane] = (
                rows_out[:, i * group : (i + 1) * group].astype(jnp.bfloat16).astype(jnp.float32)
            )

    head_count = ahead.shape[0] // 2
    head_dim = group // head_count
    lane = lax.broadcasted_iota(jnp.int32, (length, group), 1)
    in_lower = lax.rem(lane, head_dim) < head_dim // 2

    def turned(values):
        partner = jnp.where(
            in_lower,
            pltpu.roll(values, group - head_dim // 2, 1),
            pltpu.roll(values, head_dim // 2, 1),
        )
        return values * cosine[...] + partner * sine_part[...]

    offset = (
        lax.broadcasted_iota(jnp.int32, (length, length), 0)
        - lax.broadcasted_iota(jnp.int32, (length, length), 1)
    ).astype(jnp.float32)

    def log_sigmoid(logit):
        value = jnp.full((8, 128), logit, jnp.float32)
        return (jnp.minimum(value, 0.0) - jnp.log1p(jnp.exp(-jnp.abs(value))))[:1, :1]

    decays = [
        jnp.exp(
            jnp.where(
                offset >= 0,
                log_sigmoid(ahead[slot * head_count + h]) * offset,
                -log_sigmoid(behind[slot * head_count + h]) * offset,
            )
        )
        for h in range(head_count)
    ]
    here = [(lane >= h * head_dim) & (lane < (h + 1) * head_dim) for h in range(head_count)]
    for plane in range(2):
        queries = turned(projected[0, plane])
        key_heads = (turned(projected[1, plane]) * head_dim ** (-0.5)).astype(jnp.bfloat16)
        valued = projected[2, plane]
        result = jnp.zeros((length, group), jnp.float32)
        for h in range(head_count):
            scores = lax.dot_general(
                jnp.where(here[h], queries, 0.0).astype(jnp.bfloat16),
                key_heads,
                (((1,), (1,)), ((), ())),
                preferred_element_type=jnp.float32,
            )
            result = result + jnp.dot(
                (scores * decays[h]).astype(jnp.bfloat16),
                jnp.where(here[h], valued, 0.0).astype(jnp.bfloat16),
                preferred_element_type=jnp.float32,
            )
        center = jnp.zeros((length, group), jnp.float32)
        for h in range(head_count):
            mean = jnp.sum(jnp.where(here[h], result, 0.0), axis=1, keepdims=True) / head_dim
            center = jnp.where(here[h], mean, center)
        centered = result - center
        squared = centered * centered
        factor = jnp.zeros((length, group), jnp.float32)
        for h in range(head_count):
            spread_h = jnp.sum(jnp.where(here[h], squared, 0.0), axis=1, keepdims=True) / head_dim
            factor = jnp.where(here[h], lax.rsqrt(spread_h + group_eps), factor)
        gates = projected[3, plane]
        mixed[plane] = (gates / (1.0 + jnp.exp(-gates)) * (centered * factor)).astype(jnp.bfloat16)

    ready(6)
    settle(1)

    def fill(rows_in, weight, partial, side):
        for x in range(row // 2):
            block = x * 2 + side
            for plane in range(2):
                term = jnp.dot(rows_in[plane], weight[block], preferred_element_type=jnp.float32)
                partial[side, x, plane] = term.astype(jnp.bfloat16)

    steps = reducer(first_partial, first_core, first_row, 0, (0, 1), True) + [
        moved(first_partial.at[core, column, plane], first_line.at[plane], {"fs": line_peer}, 0, 3 + plane)
        for plane in range(2)
    ]
    fill(mixed, merge, first_partial, 1 - core)
    steps[0].start()
    fill(mixed, merge, first_partial, core)
    add_core(first_partial, first_core, steps, (0, 1), True)
    for block in others:
        pump(2, block)
    pump(3, others[0])
    for plane in range(2):
        total = add_row(first_partial, first_core, first_row, steps, plane, plane, True)
        first_partial[core, column, plane] = total.astype(jnp.bfloat16)
        steps[3 + plane].start()
    ready(4)
    for i in range(pieces):
        for there in others:
            post(first_down + i, there).start()

    second = [share_mid(step) for step in range(6)]
    pump(3, others[1])
    pump(3, others[2])
    for block in others:
        pump(4, block)
    pump(5, others[0])
    for plane in range(2):
        steps[3 + plane].wait_recv()
        total = gathered[plane, seat].astype(jnp.float32) + (
            first_partial[core, column, plane].astype(jnp.float32)
            + first_line[plane].astype(jnp.float32)
        )
        gathered_mid[plane, seat] = total.astype(jnp.bfloat16)
        second[plane].start()
        second[2 + plane].start()
        pump(5, others[1 + plane])
    queue = [(first_down + i, block) for i in range(pieces) for block in [line_peer] + crossing]

    def pump_next(count):
        for _ in range(count):
            pump(*queue.pop(0))

    def product(plane):
        for begin in range(0, hidden_half, tile):
            columns = slice(begin, min(begin + tile, hidden_half))
            gate_act, up_act = [
                jnp.dot(
                    normed[plane],
                    weight[:, :, columns].reshape(width, -1),
                    preferred_element_type=jnp.float32,
                )
                for weight in (gate, up)
            ]
            hidden[plane, :, columns] = (gate_act / (1.0 + jnp.exp(-gate_act)) * up_act).astype(
                jnp.bfloat16
            )
            if plane == 1:
                pump_next(1)

    tile = 256
    shared_mid(0).wait_recv()
    second[4].start()
    pump_next(len(others))
    shared_mid(2).wait_recv()
    shared_mid(4).wait_recv()
    normalize(gathered_mid, middle_gain, 0)
    ready(7)
    ready(8)
    for k in range(2, first_down):
        settle(k)
    product(0)
    shared_mid(1).wait_recv()
    second[5].start()
    pump_next(len(others))
    shared_mid(3).wait_recv()
    shared_mid(5).wait_recv()
    normalize(gathered_mid, middle_gain, 1)
    product(1)
    ready(9)
    by_rows = [i in (0, 2) for i in range(pieces)]
    ends = []
    for i in range(pieces):
        mine, other = chosen(by_rows[i])
        ends.append(
            reducer(
                last_partial.at[i],
                last_core.at[i],
                last_row.at[i],
                1 + i,
                (1 - other, other),
                by_rows[i],
            )
            + [
                moved(
                    last_partial.at[(i, core, *spot(by_rows[i], mine, 1 - other))],
                    last_line.at[i],
                    {"fs": line_peer} if by_rows[i] else {"tp": row_peer},
                    1 + i,
                    3,
                )
            ]
        )

    def last_sum(i, step):
        other = chosen(by_rows[i])[1]
        part = other if step else 1 - other
        return add_row(
            last_partial.at[i], last_core.at[i], last_row.at[i], ends[i], step, part, by_rows[i]
        )

    def pass_line(i):
        total = last_sum(i, 0)
        mine, other = chosen(by_rows[i])
        last_partial[(i, core, *spot(by_rows[i], mine, 1 - other))] = total.astype(jnp.bfloat16)
        ends[i][3].start()

    written = [
        pltpu.make_async_copy(
            finished.at[:, i * piece_width : (i + 1) * piece_width],
            out.at[:, i * piece_width : (i + 1) * piece_width],
            out_sem.at[i],
        )
        for i in range(pieces)
    ]

    def finish(i):
        span = slice(i * piece_width, (i + 1) * piece_width)
        total = gathered_mid[slot, seat, :, span].astype(jnp.float32) + last_sum(i, 1)
        ends[i][3].wait_recv()
        finished[:, span] = (total + last_line[i].astype(jnp.float32)).astype(jnp.bfloat16)
        written[i].start()

    for i in range(pieces):
        settle(first_down + i)
        fill(hidden, down.at[i], last_partial.at[i], 1 - core)
        ends[i][0].start()
        fill(hidden, down.at[i], last_partial.at[i], core)
        other = chosen(by_rows[i])[1]
        add_core(last_partial.at[i], last_core.at[i], ends[i], (1 - other, other), by_rows[i])
        if queue:
            pump_next(1 if i == 0 else 2)
        if i > 1:
            pass_line(i - 2)
    for i in range(max(0, pieces - 2), pieces):
        pass_line(i)
    for i in range(pieces):
        finish(i)

    for copy in written:
        copy.wait()
    for copy in first + second + steps:
        copy.wait_send()
    for group_steps in ends:
        for copy in group_steps:
            copy.wait_send()
    for k in range(first_down + pieces):
        for there in others:
            post(k, there).wait_send()
            across(k, there, half).wait_send()


def paired_call(
    sizes, flat, input_gain, middle_gain, decays, tables, quads, merge_weight, gate_weight, up_weight, down_weight
):
    line, row = sizes["fs"], sizes["tp"]
    bf16 = jnp.bfloat16
    length, part_width = flat.shape
    depth, ret_width = quads[0].shape
    hidden_half, group = gate_weight.shape[1] // 2, ret_width // 2
    pieces = 4
    piece_width = down_weight.shape[1] // pieces
    kinds = 6 + pieces
    anywhere = pl.BlockSpec(memory_space=pl.ANY)
    in_smem = pl.BlockSpec(memory_space=pltpu.SMEM)

    def sums(lead, columns, last):
        return [
            pltpu.VMEM(lead + (2, row // 2, 2, length, columns), bf16),
            pltpu.VMEM(lead + (row // 2, 2, length, columns), bf16),
            pltpu.VMEM(lead + (2, length, columns), bf16),
            pltpu.VMEM(lead + last + (length, columns), bf16),
        ]

    dma = pltpu.SemaphoreType.DMA
    return pl.pallas_call(
        functools.partial(paired_kernel, sizes),
        out_shape=jax.ShapeDtypeStruct(flat.shape, bf16),
        in_specs=[anywhere] * 3 + [in_smem] * 2 + [anywhere] * 10,
        out_specs=anywhere,
        scratch_shapes=[
            pltpu.VMEM((1, row * part_width), jnp.float32),
            pltpu.VMEM((1, row * part_width), jnp.float32),
            pltpu.VMEM(tables[0].shape, jnp.float32),
            pltpu.VMEM(tables[1].shape, jnp.float32),
            pltpu.VMEM(flat.shape, bf16),
            pltpu.VMEM((2, depth, 4 * group), bf16),
            pltpu.VMEM(merge_weight.shape, bf16),
            pltpu.VMEM(gate_weight.shape, bf16),
            pltpu.VMEM(up_weight.shape, bf16),
            pltpu.VMEM(down_weight.shape, bf16),
            pltpu.VMEM((line, depth, 4 * group), bf16),
            pltpu.VMEM((line, merge_weight.shape[0] // 2, part_width), bf16),
            pltpu.VMEM((line, depth, hidden_half), bf16),
            pltpu.VMEM((line, depth, hidden_half), bf16),
            pltpu.VMEM((pieces, line, hidden_half, piece_width), bf16),
            pltpu.VMEM((2, row, length, part_width), bf16),
            pltpu.VMEM((2, row, length, part_width), bf16),
            pltpu.VMEM((2, length, row * part_width), bf16),
            pltpu.VMEM((4, 2, length, group), jnp.float32),
            pltpu.VMEM((2, length, group), bf16),
            pltpu.VMEM((2, length, hidden_half), bf16),
        ]
        + sums((), part_width, (2,))
        + sums((pieces,), piece_width, ())
        + [
            dma((25 + pieces,)),
            dma((kinds, line)),
            dma((kinds, line)),
            dma((kinds, line)),
            dma((kinds, line)),
            dma((2, 7)),
            dma((2, 7)),
            dma((1 + pieces, 5)),
            dma((1 + pieces, 5)),
            dma((pieces,)),
        ],
        compiler_params=pltpu.CompilerParams(
            collective_id=0, has_side_effects=True, vmem_limit_bytes=60 << 20
        ),
    )(
        flat,
        input_gain[None, :],
        middle_gain[None, :],
        *decays,
        *tables,
        *quads,
        merge_weight,
        gate_weight,
        up_weight,
        down_weight,
    )


def on_device(
    sizes,
    tokens,
    input_gain,
    query_weight,
    key_weight,
    value_weight,
    output_gate_matrix,
    forward_decay,
    backward_decay,
    merge_weight,
    middle_gain,
    gate_weight,
    up_weight,
    down_weight,
):
    seq_count, length, part_width = tokens.shape
    flat = tokens.reshape(seq_count * length, part_width)
    quads = (query_weight, key_weight, value_weight, output_gate_matrix)
    paired = (
        sizes["grp"] == 2
        and sizes["fs"] == sizes["tp"] == 4
        and seq_count == 1
        and query_weight.shape[1] % 256 == 0
        and forward_decay.shape[0] % 2 == 0
        and gate_weight.shape[1] % 256 == 0
        and down_weight.shape[1] == part_width
        and part_width % 256 == 0
    )
    if paired:
        head_count = forward_decay.shape[0] // 2
        head_dim = query_weight.shape[1] // (2 * head_count)
        layer_out = paired_call(
            sizes,
            flat,
            input_gain,
            middle_gain,
            (forward_decay, backward_decay),
            turn_tables(length, head_dim, head_count),
            quads,
            merge_weight,
            gate_weight,
            up_weight,
            down_weight,
        )
        return layer_out.reshape(seq_count, length, part_width)
    joined = jnp.concatenate(quads, axis=1)
    shards = (joined, merge_weight, gate_weight, up_weight, down_weight)
    line, copies, row = sizes["fs"], sizes["grp"], sizes["tp"]
    down_width = down_weight.shape[1]
    parts = down_width // 256 if line == row and down_width % 256 == 0 else 1
    down_piece = jax.ShapeDtypeStruct((down_weight.shape[0], down_width // parts), jnp.bfloat16)
    landing = shards[:4] + (down_piece,) * parts
    count = len(landing)
    width, ret_width, hidden_width = row * part_width, query_weight.shape[1], gate_weight.shape[1]
    head_count = forward_decay.shape[0]
    tables = turn_tables(length, ret_width // head_count, head_count)
    in_vmem = pl.BlockSpec(memory_space=pltpu.VMEM)
    in_smem = pl.BlockSpec(memory_space=pltpu.SMEM)
    bf16 = jnp.bfloat16
    layer_out = pl.pallas_call(
        functools.partial(layer_kernel, sizes),
        out_shape=jax.ShapeDtypeStruct(flat.shape, bf16),
        in_specs=[in_vmem] * 3
        + [in_smem] * 2
        + [in_vmem] * 2
        + [pl.BlockSpec(memory_space=pl.ANY)] * len(shards),
        out_specs=in_vmem,
        scratch_shapes=[pltpu.VMEM((line,) + w.shape, w.dtype) for w in landing]
        + [
            pltpu.VMEM((row, length, part_width), bf16),
            pltpu.VMEM((row, length, part_width), bf16),
            pltpu.VMEM((length, width), bf16),
            pltpu.VMEM((4, length, ret_width), jnp.float32),
            pltpu.VMEM((length, ret_width), bf16),
            pltpu.VMEM((length, hidden_width), bf16),
            pltpu.VMEM((row, length, part_width), bf16),
            pltpu.VMEM((row - 1, length, part_width), bf16),
            pltpu.SemaphoreType.DMA((count,)),
            pltpu.SemaphoreType.DMA((count, 2, line)),
            pltpu.SemaphoreType.DMA((count, 2, line)),
            pltpu.SemaphoreType.DMA((count, 2, line, copies - 1)),
            pltpu.SemaphoreType.DMA((count, 2, line, copies - 1)),
            pltpu.SemaphoreType.DMA((3 + parts, row - 1)),
            pltpu.SemaphoreType.DMA((3 + parts, row - 1)),
            pltpu.SemaphoreType.DMA,
            pltpu.VMEM((parts, row, length, part_width // parts), bf16),
            pltpu.VMEM((parts, row - 1, length, part_width // parts), bf16),
        ],
        compiler_params=pltpu.CompilerParams(
            collective_id=0, has_side_effects=True, vmem_limit_bytes=58 << 20
        ),
    )(
        flat,
        input_gain[None, :],
        middle_gain[None, :],
        jax.nn.log_sigmoid(forward_decay),
        jax.nn.log_sigmoid(backward_decay),
        *tables,
        *shards,
    )
    return layer_out.reshape(seq_count, length, part_width)


def solution(mesh):
    placed = (
        P(("grp", "fs"), None, "tp"),
        P(),
        P("fs", "tp"),
        P("fs", "tp"),
        P("fs", "tp"),
        P("fs", "tp"),
        P("tp"),
        P("tp"),
        P("tp", "fs"),
        P(),
        P("fs", "tp"),
        P("fs", "tp"),
        P("tp", "fs"),
    )
    return jax.shard_map(
        functools.partial(on_device, dict(mesh.shape)),
        mesh=mesh,
        in_specs=placed,
        out_specs=P(("grp", "fs"), None, "tp"),
        check_vma=False,
    )
```

```python
import functools

import jax
import jax.numpy as jnp
import numpy as np
from jax import lax
from jax.experimental import pallas as pl
from jax.experimental.pallas import tpu as pltpu
from jax.sharding import PartitionSpec as P

norm_eps = 1e-06
group_eps = 1e-05
rope_base = 10000.0


def turn_tables(length, head_dim, head_count):
    half_dim = head_dim // 2
    inverse = rope_base ** (-np.arange(half_dim) / half_dim)
    angles = np.arange(length)[:, None] * inverse[None, :]
    cosine, sine_part = np.cos(angles), np.sin(angles)
    return (
        np.tile(np.concatenate([cosine, cosine], axis=1), (1, head_count)).astype(np.float32),
        np.tile(np.concatenate([-sine_part, sine_part], axis=1), (1, head_count)).astype(np.float32),
    )


MESH = pl.DeviceIdType.MESH


def layer_kernel(
    sizes,
    tokens,
    input_gain,
    middle_gain,
    rate_ahead,
    rate_behind,
    cosine,
    sine_part,
    joined_shard,
    merge_shard,
    gate_shard,
    up_shard,
    down_shard,
    out,
    joined,
    merge,
    gate,
    up,
    *rest,
):
    line, copies, row = sizes["fs"], sizes["grp"], sizes["tp"]
    parts = len(rest) - 18
    downs, partial_ends, received_ends = rest[:parts], rest[-2], rest[-1]
    (
        gathered,
        gathered_mid,
        normed,
        projected,
        mixed,
        hidden,
        partial,
        received,
        own_sem,
        line_send,
        line_recv,
        pair_send,
        pair_recv,
        row_send,
        row_recv,
        self_sem,
    ) = rest[parts:-2]
    piece_width = downs[0].shape[2]
    shards = (joined_shard, merge_shard, gate_shard, up_shard) + tuple(
        down_shard if parts == 1 else down_shard.at[:, pl.ds(i * piece_width, piece_width)]
        for i in range(parts)
    )
    slots = (joined, merge, gate, up) + tuple(downs)
    count = len(slots)
    length, part_width = tokens.shape
    width = row * part_width
    seat = lax.axis_index("tp")
    place = lax.axis_index("fs")
    half = lax.axis_index("grp")

    barrier = pltpu.get_barrier_semaphore()
    for shift in (1, -1):
        there = place + shift

        @pl.when((there >= 0) & (there < line))
        def _():
            pl.semaphore_signal(barrier, inc=1, device_id={"fs": there}, device_id_type=MESH)

    for other in range(1, copies):
        pl.semaphore_signal(
            barrier,
            inc=1,
            device_id={"grp": lax.rem(half + other, copies)},
            device_id_type=MESH,
        )
    for other in range(1, row):
        pl.semaphore_signal(
            barrier,
            inc=1,
            device_id={"tp": lax.rem(seat + other, row)},
            device_id_type=MESH,
        )
    own = [pltpu.make_async_copy(shards[k], slots[k].at[place], own_sem.at[k]) for k in range(count)]
    for copy in own:
        copy.start()
    neighbours = (place > 0).astype(jnp.int32) + (place < line - 1).astype(jnp.int32)
    mine = pltpu.make_async_copy(tokens, gathered.at[seat], self_sem)
    mine.start()
    pl.semaphore_wait(barrier, neighbours + copies - 1 + row - 1)

    def piece(k, block, part):
        rows = slots[k].shape[1] // copies
        return slots[k].at[block, pl.ds(pl.multiple_of(part * rows, rows), rows), :]

    def hop(k, way, step):
        shift = 1 if way == 0 else -1
        block = place - shift * step
        return pltpu.make_async_remote_copy(
            src_ref=piece(k, block, half),
            dst_ref=piece(k, block, half),
            send_sem=line_send.at[k, way, step],
            recv_sem=line_recv.at[k, way, step],
            device_id={"fs": place + shift},
            device_id_type=MESH,
        )

    def arrival(k, way, step):
        shift = 1 if way == 0 else -1
        block = place - shift * step
        return pltpu.make_async_remote_copy(
            src_ref=piece(k, block, half),
            dst_ref=piece(k, block, half),
            send_sem=line_send.at[k, way, step - 1],
            recv_sem=line_recv.at[k, way, step - 1],
            device_id={"fs": place - shift},
            device_id_type=MESH,
        )

    def across(k, way, step, other):
        shift = 1 if way == 0 else -1
        block = place - shift * step
        return pltpu.make_async_remote_copy(
            src_ref=piece(k, block, half),
            dst_ref=piece(k, block, half),
            send_sem=pair_send.at[k, way, step - 1, other - 1],
            recv_sem=pair_recv.at[k, way, step - 1, other - 1],
            device_id={"grp": lax.rem(half + other, copies)},
            device_id_type=MESH,
        )

    def landed(k, way, step, other):
        shift = 1 if way == 0 else -1
        block = place - shift * step
        source = lax.rem(half + copies - other, copies)
        return pltpu.make_async_remote_copy(
            src_ref=piece(k, block, source),
            dst_ref=piece(k, block, source),
            send_sem=pair_send.at[k, way, step - 1, other - 1],
            recv_sem=pair_recv.at[k, way, step - 1, other - 1],
            device_id={"grp": source},
            device_id_type=MESH,
        )

    def has(way, step):
        return place >= step if way == 0 else place + step < line

    def goes(way):
        return place < line - 1 if way == 0 else place > 0

    def launch(k):
        own[k].wait()
        for way in range(2):

            @pl.when(goes(way))
            def _():
                hop(k, way, 0).start()

    def pump(k):
        for step in range(1, line):
            for way in range(2):

                @pl.when(has(way, step))
                def _():
                    arrival(k, way, step).wait_recv()
                    for other in range(1, copies):
                        across(k, way, step, other).start()

                @pl.when(has(way, step) & goes(way))
                def _():
                    hop(k, way, step).start()

    def settle(k):
        for step in range(1, line):
            for way in range(2):

                @pl.when(has(way, step))
                def _():
                    for other in range(1, copies):
                        landed(k, way, step, other).wait_recv()

    def drain(k):
        for way in range(2):
            for step in range(line):

                @pl.when((has(way, step) if step else True) & goes(way))
                def _():
                    hop(k, way, step).wait_send()

                if step:

                    @pl.when(has(way, step))
                    def _():
                        for other in range(1, copies):
                            across(k, way, step, other).wait_send()

    def spread(source, target, stage):
        return [
            pltpu.make_async_remote_copy(
                src_ref=source,
                dst_ref=target.at[seat],
                send_sem=row_send.at[stage, other - 1],
                recv_sem=row_recv.at[stage, other - 1],
                device_id={"tp": lax.rem(seat + other, row)},
                device_id_type=MESH,
            )
            for other in range(1, row)
        ]

    def spread_in(target, stage):
        sources = [lax.rem(seat + row - other, row) for other in range(1, row)]
        return [
            pltpu.make_async_remote_copy(
                src_ref=target.at[source],
                dst_ref=target.at[source],
                send_sem=row_send.at[stage, other],
                recv_sem=row_recv.at[stage, other],
                device_id={"tp": source},
                device_id_type=MESH,
            )
            for other, source in enumerate(sources)
        ]

    def scatter(source, target, stage, other):
        there = lax.rem(seat + other, row)
        return pltpu.make_async_remote_copy(
            src_ref=source.at[there],
            dst_ref=target.at[other - 1],
            send_sem=row_send.at[stage, other - 1],
            recv_sem=row_recv.at[stage, other - 1],
            device_id={"tp": there},
            device_id_type=MESH,
        )

    def normalize(source, gain_vector):
        total = jnp.zeros((length, 1), jnp.float32)
        for t in range(row):
            widened = source[t].astype(jnp.float32)
            total = total + jnp.sum(widened * widened, axis=1, keepdims=True)
        scale = lax.rsqrt(total / width + norm_eps)
        for t in range(row):
            span = slice(t * part_width, (t + 1) * part_width)
            scaled = source[t].astype(jnp.float32) * scale * gain_vector[:, span]
            normed[:, span] = scaled.astype(jnp.bfloat16)

    def times(weight, columns):
        block = weight[:, :, columns]
        return jnp.dot(
            normed[...], block.reshape(-1, block.shape[2]), preferred_element_type=jnp.float32
        )

    def shares(rows_in, weight, target):
        step = weight.shape[2]
        for block in range(line):
            term = jnp.dot(rows_in[...], weight[block], preferred_element_type=jnp.float32)
            begin = block * step
            inner = begin % part_width
            target[begin // part_width, :, inner : inner + step] = term.astype(jnp.bfloat16)

    def finish(i):
        settle(4 + i)
        if parts == 1:
            shares(hidden, downs[i], partial_ends.at[i])
        else:
            for j in range(row):
                blocks = [jnp.dot(
                    hidden[...], downs[i][j * line // row + c], preferred_element_type=jnp.float32
                ) for c in range(max(1, line // row))]
                for c, term in enumerate(blocks):
                    partial_ends[i, j, :, c * piece_width : (c + 1) * piece_width] = term.astype(
                        jnp.bfloat16
                    )
        for other in range(1, row):
            scatter(partial_ends.at[i], received_ends.at[i], 3 + i, other).start()

    def collect(i):
        span = slice(None) if parts == 1 else slice(i * piece_width, (i + 1) * piece_width)
        total = gathered_mid[seat, :, span].astype(jnp.float32)
        total = total + partial_ends[i, seat].astype(jnp.float32)
        for other in range(1, row):
            scatter(partial_ends.at[i], received_ends.at[i], 3 + i, other).wait_recv()
            total = total + received_ends[i, other - 1].astype(jnp.float32)
        out[:, span] = total.astype(jnp.bfloat16)

    launch(0)
    first = spread(tokens, gathered, 0)
    for copy in first:
        copy.start()
    launch(1)
    mine.wait()
    for copy in spread_in(gathered, 0):
        copy.wait_recv()
    normalize(gathered, input_gain)

    pump(0)
    launch(2)
    settle(0)
    ret_width = projected.shape[2]
    for t in range(4):
        projected[t] = (
            times(joined, slice(t * ret_width, (t + 1) * ret_width))
            .astype(jnp.bfloat16)
            .astype(jnp.float32)
        )
    pump(1)
    launch(3)

    head_count = rate_ahead.shape[0]
    head_dim = ret_width // head_count
    lane = lax.broadcasted_iota(jnp.int32, (length, ret_width), 1)
    in_lower = lax.rem(lane, head_dim) < head_dim // 2

    def turned(values):
        partner = jnp.where(
            in_lower,
            pltpu.roll(values, ret_width - head_dim // 2, 1),
            pltpu.roll(values, head_dim // 2, 1),
        )
        return values * cosine[...] + partner * sine_part[...]

    queries = turned(projected[0])
    key_heads = (turned(projected[1]) * head_dim ** (-0.5)).astype(jnp.bfloat16)
    valued = projected[2]
    offset = (
        lax.broadcasted_iota(jnp.int32, (length, length), 0)
        - lax.broadcasted_iota(jnp.int32, (length, length), 1)
    ).astype(jnp.float32)
    result = jnp.zeros((length, ret_width), jnp.float32)
    for h in range(head_count):
        here = (lane >= h * head_dim) & (lane < (h + 1) * head_dim)
        scores = lax.dot_general(
            jnp.where(here, queries, 0.0).astype(jnp.bfloat16),
            key_heads,
            (((1,), (1,)), ((), ())),
            preferred_element_type=jnp.float32,
        )
        decay = jnp.exp(jnp.where(offset >= 0, rate_ahead[h] * offset, -rate_behind[h] * offset))
        result = result + jnp.dot(
            (scores * decay).astype(jnp.bfloat16),
            jnp.where(here, valued, 0.0).astype(jnp.bfloat16),
            preferred_element_type=jnp.float32,
        )
    center = jnp.zeros((length, ret_width), jnp.float32)
    for h in range(head_count):
        here = (lane >= h * head_dim) & (lane < (h + 1) * head_dim)
        mean = jnp.sum(jnp.where(here, result, 0.0), axis=1, keepdims=True) / head_dim
        center = jnp.where(here, mean, center)
    centered = result - center
    squared = centered * centered
    factor = jnp.zeros((length, ret_width), jnp.float32)
    for h in range(head_count):
        here = (lane >= h * head_dim) & (lane < (h + 1) * head_dim)
        spread_h = jnp.sum(jnp.where(here, squared, 0.0), axis=1, keepdims=True) / head_dim
        factor = jnp.where(here, lax.rsqrt(spread_h + group_eps), factor)
    gates = projected[3]
    mixed[...] = (gates / (1.0 + jnp.exp(-gates)) * (centered * factor)).astype(jnp.bfloat16)

    settle(1)
    shares(mixed, merge, partial)
    for other in range(1, row):
        scatter(partial, received, 1, other).start()
    pump(2)
    total = tokens[...].astype(jnp.float32) + partial[seat].astype(jnp.float32)
    for other in range(1, row):
        scatter(partial, received, 1, other).wait_recv()
        total = total + received[other - 1].astype(jnp.float32)
    gathered_mid[seat] = total.astype(jnp.bfloat16)
    second = spread(gathered_mid.at[seat], gathered_mid, 2)
    for copy in second:
        copy.start()
    pump(3)
    launch(4)
    if parts > 1:
        launch(5)
    for copy in spread_in(gathered_mid, 2):
        copy.wait_recv()
    normalize(gathered_mid, middle_gain)
    settle(2)
    settle(3)
    hidden_width = hidden.shape[1]
    tile = 256 if hidden_width % 256 == 0 else 128

    @pl.loop(0, hidden_width // tile)
    def _(index):
        columns = pl.ds(pl.multiple_of(index * tile, tile), tile)
        gate_act = times(gate, columns)
        up_act = times(up, columns)
        hidden[:, columns] = (gate_act / (1.0 + jnp.exp(-gate_act)) * up_act).astype(jnp.bfloat16)

    for i in range(parts):
        pump(4 + i)
        if i + 2 < parts:
            launch(6 + i)
        if i:
            finish(i - 1)
    finish(parts - 1)
    for i in range(parts):
        collect(i)
    for copy in first + second:
        copy.wait_send()
    for other in range(1, row):
        scatter(partial, received, 1, other).wait_send()
        for i in range(parts):
            scatter(partial_ends.at[i], received_ends.at[i], 3 + i, other).wait_send()
    for k in range(count):
        drain(k)


def paired_kernel(
    sizes,
    tokens,
    input_gain_in,
    middle_gain_in,
    ahead,
    behind,
    cosine_in,
    sine_in,
    query_shard,
    key_shard,
    value_shard,
    output_gate_shard,
    merge_shard,
    gate_shard,
    up_shard,
    down_shard,
    out,
    input_gain,
    middle_gain,
    cosine,
    sine_part,
    finished,
    joined_out,
    merge_out,
    gate_out,
    up_out,
    down_out,
    joined,
    merge,
    gate,
    up,
    down,
    gathered,
    gathered_mid,
    normed,
    projected,
    mixed,
    hidden,
    first_partial,
    first_core,
    first_row,
    first_line,
    last_partial,
    last_core,
    last_row,
    last_line,
    own_sem,
    line_send,
    line_recv,
    pair_send,
    pair_recv,
    share_send,
    share_recv,
    sum_send,
    sum_recv,
    out_sem,
):
    line, row = sizes["fs"], sizes["tp"]
    pieces = down.shape[0]
    piece_width = down.shape[3]
    length, part_width = tokens.shape
    width = row * part_width
    seat = lax.axis_index("tp")
    place = lax.axis_index("fs")
    half = lax.axis_index("grp")
    core, column = lax.rem(seat, 2), seat // 2
    slot = lax.rem(place, 2)
    core_peer = seat + 1 - 2 * core
    row_peer = lax.rem(seat + 2, row)
    far_peer = lax.rem(core_peer + 2, row)
    line_peer = place + 1 - 2 * slot
    sign = 1 - 2 * (place // (line // 2))
    others = [lax.rem(place + sign * step + line, line) for step in range(1, line)]
    facing = jnp.where(place < line // 2, line // 2, line // 2 - 1)
    crossing = [facing + sign * step for step in range(line // 2)]
    sources = [facing, line_peer] + crossing[1:]

    barrier = pltpu.get_barrier_semaphore()
    for there in others:
        pl.semaphore_signal(barrier, inc=1, device_id={"fs": there}, device_id_type=MESH)
    pl.semaphore_signal(barrier, inc=1, device_id={"grp": 1 - half}, device_id_type=MESH)
    for there in (core_peer, row_peer):
        pl.semaphore_signal(barrier, inc=1, device_id={"tp": there}, device_id_type=MESH)

    group = joined_out.shape[2] // 4
    quads = (query_shard, key_shard, value_shard, output_gate_shard)
    merge_rows = merge.shape[1]
    hidden_half = gate.shape[2]

    def cut(ref, axis, part, size):
        window = pl.ds(pl.multiple_of(part * size, size), size)
        return ref.at[window] if axis == 0 else ref.at[:, window]

    loads = [
        [
            (quad.at[:, p * group : (p + 1) * group], joined_out.at[p, :, i * group : (i + 1) * group])
            for p in range(2)
            for i, quad in enumerate(quads)
        ],
        [(merge_shard, merge_out)],
        [(gate_shard, gate_out)],
        [(up_shard, up_out)],
        [(down_shard, down_out)],
        [
            (cut(quad, 1, slot, group), joined.at[place, :, i * group : (i + 1) * group])
            for i, quad in enumerate(quads)
        ],
        [(cut(merge_shard, 0, slot, merge_rows), merge.at[place])],
        [(cut(gate_shard, 1, slot, hidden_half), gate.at[place])],
        [(cut(up_shard, 1, slot, hidden_half), up.at[place])],
        [
            (
                cut(down_shard, 0, slot, hidden_half).at[:, i * piece_width : (i + 1) * piece_width],
                down.at[i, place],
            )
            for i in range(pieces)
        ],
        [(tokens, gathered.at[slot, seat])],
        [
            (input_gain_in, input_gain),
            (middle_gain_in, middle_gain),
            (cosine_in, cosine),
            (sine_in, sine_part),
        ],
    ]
    own, index = [], 0
    for pairs in loads:
        own.append([])
        for source, target in pairs:
            own[-1].append(pltpu.make_async_copy(source, target, own_sem.at[index]))
            index += 1
    for copies in (own[-2], *own[:-2], own[-1]):
        for copy in copies:
            copy.start()
    pl.semaphore_wait(barrier, line - 1 + 1 + 2)

    def ready(k):
        for copy in own[k]:
            copy.wait()

    first_down = 6

    def outgoing(k, parity):
        if k == 0:
            size = joined.shape[1] // 2
            return joined_out.at[parity, pl.ds(pl.multiple_of(half * size, size), size)]
        if k == 1:
            size = merge_rows // 2
            return cut(merge_out, 0, parity * 2 + half, size)
        if k < first_down:
            source = (gate_out, up_out)[(k - 2) // 2]
            size = source.shape[0] // 4
            return cut(source, 0, half * 2 + k % 2, size).at[
                :, pl.ds(pl.multiple_of(parity * hidden_half, hidden_half), hidden_half)
            ]
        size = hidden_half // 2
        begin = (k - first_down) * piece_width
        return cut(down_out, 0, parity * 2 + half, size).at[:, begin : begin + piece_width]

    def landing(k, block, part):
        if 2 <= k < first_down:
            target = (gate, up)[(k - 2) // 2]
            size, part = target.shape[1] // 4, part * 2 + k % 2
        else:
            target = (joined, merge)[k] if k < 2 else down.at[k - first_down]
            size = target.shape[1] // 2
        return target.at[block, pl.ds(pl.multiple_of(part * size, size), size)]

    def post(k, there):
        return pltpu.make_async_remote_copy(
            src_ref=outgoing(k, lax.rem(there, 2)),
            dst_ref=landing(k, place, half),
            send_sem=line_send.at[k, there],
            recv_sem=line_recv.at[k, place],
            device_id={"fs": there},
            device_id_type=MESH,
        )

    def arrival(k, block):
        return pltpu.make_async_remote_copy(
            src_ref=landing(k, block, half),
            dst_ref=landing(k, block, half),
            send_sem=line_send.at[k, block],
            recv_sem=line_recv.at[k, block],
            device_id={"fs": block},
            device_id_type=MESH,
        )

    def across(k, block, part):
        return pltpu.make_async_remote_copy(
            src_ref=landing(k, block, part),
            dst_ref=landing(k, block, part),
            send_sem=pair_send.at[k, block],
            recv_sem=pair_recv.at[k, block],
            device_id={"grp": 1 - half},
            device_id_type=MESH,
        )

    def launch(k):
        for there in others:
            post(k, there).start()

    def pump(k, block):
        arrival(k, block).wait_recv()
        across(k, block, half).start()

    def settle(k):
        for block in sources:
            across(k, block, 1 - half).wait_recv()

    def handed(target, stage, step):
        plane = slot if step in (0, 1, 2, 3) else 1 - slot
        holder = seat if step in (0, 1, 2, 4, 5) else row_peer
        place_in = target.at[plane, holder]
        peer = {"tp": core_peer}
        if step in (1, 5):
            peer = {"tp": row_peer}
        if step == 2:
            peer = {"fs": line_peer}
        return pltpu.make_async_remote_copy(
            src_ref=place_in,
            dst_ref=place_in,
            send_sem=share_send.at[stage, step],
            recv_sem=share_recv.at[stage, step],
            device_id=peer,
            device_id_type=MESH,
        )

    def received(target, stage, step):
        plane = slot if step in (0, 1, 3) else 1 - slot
        holder = (core_peer, row_peer, seat, far_peer, core_peer, row_peer, far_peer)[step]
        place_in = target.at[plane, holder]
        return pltpu.make_async_remote_copy(
            src_ref=place_in,
            dst_ref=place_in,
            send_sem=share_send.at[stage, step],
            recv_sem=share_recv.at[stage, step],
            device_id={"tp": core_peer},
            device_id_type=MESH,
        )

    def normalize(source, gain_vector, plane):
        total = jnp.zeros((length, 1), jnp.float32)
        for t in range(row):
            widened = source[plane, t].astype(jnp.float32)
            total = total + jnp.sum(widened * widened, axis=1, keepdims=True)
        scale = lax.rsqrt(total / width + norm_eps)
        for t in range(row):
            span = slice(t * part_width, (t + 1) * part_width)
            scaled = source[plane, t].astype(jnp.float32) * scale * gain_vector[:, span]
            normed[plane, :, span] = scaled.astype(jnp.bfloat16)

    def hand_over(target, stage):
        return [handed(target, stage, step) for step in range(7)]

    def moved(source, target, peer, stage, step):
        return pltpu.make_async_remote_copy(
            src_ref=source,
            dst_ref=target,
            send_sem=sum_send.at[stage, step],
            recv_sem=sum_recv.at[stage, step],
            device_id=peer,
            device_id_type=MESH,
        )

    def share_mid(step):
        plane, kind = step % 2, step // 2
        spot = gathered_mid.at[plane, row_peer if kind == 2 else seat]
        return pltpu.make_async_remote_copy(
            src_ref=spot,
            dst_ref=spot,
            send_sem=share_send.at[1, step],
            recv_sem=share_recv.at[1, step],
            device_id={"tp": core_peer if kind else row_peer},
            device_id_type=MESH,
        )

    def shared_mid(step):
        plane, kind = step % 2, step // 2
        spot = gathered_mid.at[plane, (row_peer, core_peer, far_peer)[kind]]
        return pltpu.make_async_remote_copy(
            src_ref=spot,
            dst_ref=spot,
            send_sem=share_send.at[1, step],
            recv_sem=share_recv.at[1, step],
            device_id={"tp": core_peer},
            device_id_type=MESH,
        )

    def spot(by_row, ahead_part, behind_part):
        return (ahead_part, behind_part) if by_row else (behind_part, ahead_part)

    def chosen(by_row):
        return spot(by_row, column, slot)

    def reducer(partial, core_in, row_in, stage, order, by_row):
        mine = chosen(by_row)[0]
        peer = {"tp": row_peer} if by_row else {"fs": line_peer}
        return [moved(partial.at[1 - core], core_in, {"tp": core_peer}, stage, 0)] + [
            moved(
                partial.at[(core, *spot(by_row, 1 - mine, part))],
                row_in.at[step],
                peer,
                stage,
                1 + step,
            )
            for step, part in enumerate(order)
        ]

    def add_core(partial, core_in, steps, order, by_row):
        mine = chosen(by_row)[0]
        steps[0].wait_recv()
        for step, part in enumerate(order):
            index = spot(by_row, 1 - mine, part)
            total = partial[(core, *index)].astype(jnp.float32) + core_in[index].astype(jnp.float32)
            partial[(core, *index)] = total.astype(jnp.bfloat16)
            steps[1 + step].start()

    def add_row(partial, core_in, row_in, steps, step, part, by_row):
        index = spot(by_row, chosen(by_row)[0], part)
        steps[1 + step].wait_recv()
        return (
            partial[(core, *index)].astype(jnp.float32)
            + core_in[index].astype(jnp.float32)
            + row_in[step].astype(jnp.float32)
        )

    ready(10)
    first = hand_over(gathered, 0)
    for step in (2, 1, 0):
        first[step].start()
    for load, kinds in enumerate(((0,), (1,), (2, 3), (4, 5))):
        ready(load)
        for k in kinds:
            launch(k)
    received(gathered, 0, 1).wait_recv()
    first[3].start()
    pump(0, sources[0])
    received(gathered, 0, 2).wait_recv()
    first[5].start()
    first[4].start()
    pump(0, sources[1])
    received(gathered, 0, 0).wait_recv()
    received(gathered, 0, 3).wait_recv()
    ready(11)
    normalize(gathered, input_gain, slot)
    pump(0, sources[2])
    received(gathered, 0, 5).wait_recv()
    first[6].start()
    received(gathered, 0, 4).wait_recv()
    received(gathered, 0, 6).wait_recv()
    normalize(gathered, input_gain, 1 - slot)
    ready(5)
    settle(0)
    for block in sources:
        pump(1, block)
    for plane in range(2):
        rows_out = jnp.dot(
            normed[plane], joined[...].reshape(width, 4 * group), preferred_element_type=jnp.float32
        )
        for i in range(4):
            projected[i, plane] = (
                rows_out[:, i * group : (i + 1) * group].astype(jnp.bfloat16).astype(jnp.float32)
            )

    head_count = ahead.shape[0] // 2
    head_dim = group // head_count
    lane = lax.broadcasted_iota(jnp.int32, (length, group), 1)
    in_lower = lax.rem(lane, head_dim) < head_dim // 2

    def turned(values):
        partner = jnp.where(
            in_lower,
            pltpu.roll(values, group - head_dim // 2, 1),
            pltpu.roll(values, head_dim // 2, 1),
        )
        return values * cosine[...] + partner * sine_part[...]

    offset = (
        lax.broadcasted_iota(jnp.int32, (length, length), 0)
        - lax.broadcasted_iota(jnp.int32, (length, length), 1)
    ).astype(jnp.float32)

    def log_sigmoid(logit):
        value = jnp.full((8, 128), logit, jnp.float32)
        return (jnp.minimum(value, 0.0) - jnp.log1p(jnp.exp(-jnp.abs(value))))[:1, :1]

    decays = [
        jnp.exp(
            jnp.where(
                offset >= 0,
                log_sigmoid(ahead[slot * head_count + h]) * offset,
                -log_sigmoid(behind[slot * head_count + h]) * offset,
            )
        )
        for h in range(head_count)
    ]
    here = [(lane >= h * head_dim) & (lane < (h + 1) * head_dim) for h in range(head_count)]
    for plane in range(2):
        queries = turned(projected[0, plane])
        key_heads = (turned(projected[1, plane]) * head_dim ** (-0.5)).astype(jnp.bfloat16)
        valued = projected[2, plane]
        result = jnp.zeros((length, group), jnp.float32)
        for h in range(head_count):
            scores = lax.dot_general(
                jnp.where(here[h], queries, 0.0).astype(jnp.bfloat16),
                key_heads,
                (((1,), (1,)), ((), ())),
                preferred_element_type=jnp.float32,
            )
            result = result + jnp.dot(
                (scores * decays[h]).astype(jnp.bfloat16),
                jnp.where(here[h], valued, 0.0).astype(jnp.bfloat16),
                preferred_element_type=jnp.float32,
            )
        center = jnp.zeros((length, group), jnp.float32)
        for h in range(head_count):
            mean = jnp.sum(jnp.where(here[h], result, 0.0), axis=1, keepdims=True) / head_dim
            center = jnp.where(here[h], mean, center)
        centered = result - center
        squared = centered * centered
        factor = jnp.zeros((length, group), jnp.float32)
        for h in range(head_count):
            spread_h = jnp.sum(jnp.where(here[h], squared, 0.0), axis=1, keepdims=True) / head_dim
            factor = jnp.where(here[h], lax.rsqrt(spread_h + group_eps), factor)
        gates = projected[3, plane]
        mixed[plane] = (gates / (1.0 + jnp.exp(-gates)) * (centered * factor)).astype(jnp.bfloat16)

    ready(6)
    settle(1)

    def fill(rows_in, weight, partial, side):
        for x in range(row // 2):
            block = x * 2 + side
            for plane in range(2):
                term = jnp.dot(rows_in[plane], weight[block], preferred_element_type=jnp.float32)
                partial[side, x, plane] = term.astype(jnp.bfloat16)

    steps = reducer(first_partial, first_core, first_row, 0, (0, 1), True) + [
        moved(first_partial.at[core, column, plane], first_line.at[plane], {"fs": line_peer}, 0, 3 + plane)
        for plane in range(2)
    ]
    fill(mixed, merge, first_partial, 1 - core)
    steps[0].start()
    fill(mixed, merge, first_partial, core)
    add_core(first_partial, first_core, steps, (0, 1), True)
    for block in others:
        pump(2, block)
    pump(3, others[0])
    for plane in range(2):
        total = add_row(first_partial, first_core, first_row, steps, plane, plane, True)
        first_partial[core, column, plane] = total.astype(jnp.bfloat16)
        steps[3 + plane].start()
    ready(4)
    for i in range(pieces):
        for there in others:
            post(first_down + i, there).start()

    second = [share_mid(step) for step in range(6)]
    pump(3, others[1])
    pump(3, others[2])
    for block in others:
        pump(4, block)
    pump(5, others[0])
    for plane in range(2):
        steps[3 + plane].wait_recv()
        total = gathered[plane, seat].astype(jnp.float32) + (
            first_partial[core, column, plane].astype(jnp.float32)
            + first_line[plane].astype(jnp.float32)
        )
        gathered_mid[plane, seat] = total.astype(jnp.bfloat16)
        second[plane].start()
        second[2 + plane].start()
        pump(5, others[1 + plane])
    queue = [(first_down + i, block) for i in range(pieces) for block in [line_peer] + crossing]

    def pump_next(count):
        for _ in range(count):
            pump(*queue.pop(0))

    def product(plane):
        for begin in range(0, hidden_half, tile):
            columns = slice(begin, min(begin + tile, hidden_half))
            gate_act, up_act = [
                jnp.dot(
                    normed[plane],
                    weight[:, :, columns].reshape(width, -1),
                    preferred_element_type=jnp.float32,
                )
                for weight in (gate, up)
            ]
            hidden[plane, :, columns] = (gate_act / (1.0 + jnp.exp(-gate_act)) * up_act).astype(
                jnp.bfloat16
            )
            if plane == 1:
                pump_next(1)

    tile = 256
    shared_mid(0).wait_recv()
    second[4].start()
    pump_next(len(others))
    shared_mid(2).wait_recv()
    shared_mid(4).wait_recv()
    normalize(gathered_mid, middle_gain, 0)
    ready(7)
    ready(8)
    for k in range(2, first_down):
        settle(k)
    product(0)
    shared_mid(1).wait_recv()
    second[5].start()
    pump_next(len(others))
    shared_mid(3).wait_recv()
    shared_mid(5).wait_recv()
    normalize(gathered_mid, middle_gain, 1)
    product(1)
    ready(9)
    by_rows = [i in (0, 2) for i in range(pieces)]
    ends = []
    for i in range(pieces):
        mine, other = chosen(by_rows[i])
        ends.append(
            reducer(
                last_partial.at[i],
                last_core.at[i],
                last_row.at[i],
                1 + i,
                (1 - other, other),
                by_rows[i],
            )
            + [
                moved(
                    last_partial.at[(i, core, *spot(by_rows[i], mine, 1 - other))],
                    last_line.at[i],
                    {"fs": line_peer} if by_rows[i] else {"tp": row_peer},
                    1 + i,
                    3,
                )
            ]
        )

    def last_sum(i, step):
        other = chosen(by_rows[i])[1]
        part = other if step else 1 - other
        return add_row(
            last_partial.at[i], last_core.at[i], last_row.at[i], ends[i], step, part, by_rows[i]
        )

    def pass_line(i):
        total = last_sum(i, 0)
        mine, other = chosen(by_rows[i])
        last_partial[(i, core, *spot(by_rows[i], mine, 1 - other))] = total.astype(jnp.bfloat16)
        ends[i][3].start()

    written = [
        pltpu.make_async_copy(
            finished.at[:, i * piece_width : (i + 1) * piece_width],
            out.at[:, i * piece_width : (i + 1) * piece_width],
            out_sem.at[i],
        )
        for i in range(pieces)
    ]

    def finish(i):
        span = slice(i * piece_width, (i + 1) * piece_width)
        total = gathered_mid[slot, seat, :, span].astype(jnp.float32) + last_sum(i, 1)
        ends[i][3].wait_recv()
        finished[:, span] = (total + last_line[i].astype(jnp.float32)).astype(jnp.bfloat16)
        written[i].start()

    for i in range(pieces):
        settle(first_down + i)
        fill(hidden, down.at[i], last_partial.at[i], 1 - core)
        ends[i][0].start()
        fill(hidden, down.at[i], last_partial.at[i], core)
        other = chosen(by_rows[i])[1]
        add_core(last_partial.at[i], last_core.at[i], ends[i], (1 - other, other), by_rows[i])
        if queue:
            pump_next(1 if i == 0 else 2)
        if i > 1:
            pass_line(i - 2)
    pass_line(pieces - 2)
    for i in range(pieces - 2):
        finish(i)
    pass_line(pieces - 1)
    for i in range(pieces - 2, pieces):
        finish(i)

    for copy in written:
        copy.wait()
    for copy in first + second + steps:
        copy.wait_send()
    for group_steps in ends:
        for copy in group_steps:
            copy.wait_send()
    for k in range(first_down + pieces):
        for there in others:
            post(k, there).wait_send()
            across(k, there, half).wait_send()


def paired_call(
    sizes, flat, input_gain, middle_gain, decays, tables, quads, merge_weight, gate_weight, up_weight, down_weight
):
    line, row = sizes["fs"], sizes["tp"]
    bf16 = jnp.bfloat16
    length, part_width = flat.shape
    depth, ret_width = quads[0].shape
    hidden_half, group = gate_weight.shape[1] // 2, ret_width // 2
    pieces = 4
    piece_width = down_weight.shape[1] // pieces
    kinds = 6 + pieces
    anywhere = pl.BlockSpec(memory_space=pl.ANY)
    in_smem = pl.BlockSpec(memory_space=pltpu.SMEM)

    def sums(lead, columns, last):
        return [
            pltpu.VMEM(lead + (2, row // 2, 2, length, columns), bf16),
            pltpu.VMEM(lead + (row // 2, 2, length, columns), bf16),
            pltpu.VMEM(lead + (2, length, columns), bf16),
            pltpu.VMEM(lead + last + (length, columns), bf16),
        ]

    dma = pltpu.SemaphoreType.DMA
    return pl.pallas_call(
        functools.partial(paired_kernel, sizes),
        out_shape=jax.ShapeDtypeStruct(flat.shape, bf16),
        in_specs=[anywhere] * 3 + [in_smem] * 2 + [anywhere] * 10,
        out_specs=anywhere,
        scratch_shapes=[
            pltpu.VMEM((1, row * part_width), jnp.float32),
            pltpu.VMEM((1, row * part_width), jnp.float32),
            pltpu.VMEM(tables[0].shape, jnp.float32),
            pltpu.VMEM(tables[1].shape, jnp.float32),
            pltpu.VMEM(flat.shape, bf16),
            pltpu.VMEM((2, depth, 4 * group), bf16),
            pltpu.VMEM(merge_weight.shape, bf16),
            pltpu.VMEM(gate_weight.shape, bf16),
            pltpu.VMEM(up_weight.shape, bf16),
            pltpu.VMEM(down_weight.shape, bf16),
            pltpu.VMEM((line, depth, 4 * group), bf16),
            pltpu.VMEM((line, merge_weight.shape[0] // 2, part_width), bf16),
            pltpu.VMEM((line, depth, hidden_half), bf16),
            pltpu.VMEM((line, depth, hidden_half), bf16),
            pltpu.VMEM((pieces, line, hidden_half, piece_width), bf16),
            pltpu.VMEM((2, row, length, part_width), bf16),
            pltpu.VMEM((2, row, length, part_width), bf16),
            pltpu.VMEM((2, length, row * part_width), bf16),
            pltpu.VMEM((4, 2, length, group), jnp.float32),
            pltpu.VMEM((2, length, group), bf16),
            pltpu.VMEM((2, length, hidden_half), bf16),
        ]
        + sums((), part_width, (2,))
        + sums((pieces,), piece_width, ())
        + [
            dma((25 + pieces,)),
            dma((kinds, line)),
            dma((kinds, line)),
            dma((kinds, line)),
            dma((kinds, line)),
            dma((2, 7)),
            dma((2, 7)),
            dma((1 + pieces, 5)),
            dma((1 + pieces, 5)),
            dma((pieces,)),
        ],
        compiler_params=pltpu.CompilerParams(
            collective_id=0, has_side_effects=True, vmem_limit_bytes=60 << 20
        ),
    )(
        flat,
        input_gain[None, :],
        middle_gain[None, :],
        *decays,
        *tables,
        *quads,
        merge_weight,
        gate_weight,
        up_weight,
        down_weight,
    )


def on_device(
    sizes,
    tokens,
    input_gain,
    query_weight,
    key_weight,
    value_weight,
    output_gate_matrix,
    forward_decay,
    backward_decay,
    merge_weight,
    middle_gain,
    gate_weight,
    up_weight,
    down_weight,
):
    seq_count, length, part_width = tokens.shape
    flat = tokens.reshape(seq_count * length, part_width)
    quads = (query_weight, key_weight, value_weight, output_gate_matrix)
    paired = (
        sizes["grp"] == 2
        and sizes["fs"] == sizes["tp"] == 4
        and seq_count == 1
        and query_weight.shape[1] % 256 == 0
        and forward_decay.shape[0] % 2 == 0
        and gate_weight.shape[1] % 256 == 0
        and down_weight.shape[1] == part_width
        and part_width % 256 == 0
    )
    if paired:
        head_count = forward_decay.shape[0] // 2
        head_dim = query_weight.shape[1] // (2 * head_count)
        layer_out = paired_call(
            sizes,
            flat,
            input_gain,
            middle_gain,
            (forward_decay, backward_decay),
            turn_tables(length, head_dim, head_count),
            quads,
            merge_weight,
            gate_weight,
            up_weight,
            down_weight,
        )
        return layer_out.reshape(seq_count, length, part_width)
    joined = jnp.concatenate(quads, axis=1)
    shards = (joined, merge_weight, gate_weight, up_weight, down_weight)
    line, copies, row = sizes["fs"], sizes["grp"], sizes["tp"]
    down_width = down_weight.shape[1]
    parts = down_width // 256 if line == row and down_width % 256 == 0 else 1
    down_piece = jax.ShapeDtypeStruct((down_weight.shape[0], down_width // parts), jnp.bfloat16)
    landing = shards[:4] + (down_piece,) * parts
    count = len(landing)
    width, ret_width, hidden_width = row * part_width, query_weight.shape[1], gate_weight.shape[1]
    head_count = forward_decay.shape[0]
    tables = turn_tables(length, ret_width // head_count, head_count)
    in_vmem = pl.BlockSpec(memory_space=pltpu.VMEM)
    in_smem = pl.BlockSpec(memory_space=pltpu.SMEM)
    bf16 = jnp.bfloat16
    layer_out = pl.pallas_call(
        functools.partial(layer_kernel, sizes),
        out_shape=jax.ShapeDtypeStruct(flat.shape, bf16),
        in_specs=[in_vmem] * 3
        + [in_smem] * 2
        + [in_vmem] * 2
        + [pl.BlockSpec(memory_space=pl.ANY)] * len(shards),
        out_specs=in_vmem,
        scratch_shapes=[pltpu.VMEM((line,) + w.shape, w.dtype) for w in landing]
        + [
            pltpu.VMEM((row, length, part_width), bf16),
            pltpu.VMEM((row, length, part_width), bf16),
            pltpu.VMEM((length, width), bf16),
            pltpu.VMEM((4, length, ret_width), jnp.float32),
            pltpu.VMEM((length, ret_width), bf16),
            pltpu.VMEM((length, hidden_width), bf16),
            pltpu.VMEM((row, length, part_width), bf16),
            pltpu.VMEM((row - 1, length, part_width), bf16),
            pltpu.SemaphoreType.DMA((count,)),
            pltpu.SemaphoreType.DMA((count, 2, line)),
            pltpu.SemaphoreType.DMA((count, 2, line)),
            pltpu.SemaphoreType.DMA((count, 2, line, copies - 1)),
            pltpu.SemaphoreType.DMA((count, 2, line, copies - 1)),
            pltpu.SemaphoreType.DMA((3 + parts, row - 1)),
            pltpu.SemaphoreType.DMA((3 + parts, row - 1)),
            pltpu.SemaphoreType.DMA,
            pltpu.VMEM((parts, row, length, part_width // parts), bf16),
            pltpu.VMEM((parts, row - 1, length, part_width // parts), bf16),
        ],
        compiler_params=pltpu.CompilerParams(
            collective_id=0, has_side_effects=True, vmem_limit_bytes=58 << 20
        ),
    )(
        flat,
        input_gain[None, :],
        middle_gain[None, :],
        jax.nn.log_sigmoid(forward_decay),
        jax.nn.log_sigmoid(backward_decay),
        *tables,
        *shards,
    )
    return layer_out.reshape(seq_count, length, part_width)


def solution(mesh):
    placed = (
        P(("grp", "fs"), None, "tp"),
        P(),
        P("fs", "tp"),
        P("fs", "tp"),
        P("fs", "tp"),
        P("fs", "tp"),
        P("tp"),
        P("tp"),
        P("tp", "fs"),
        P(),
        P("fs", "tp"),
        P("fs", "tp"),
        P("tp", "fs"),
    )
    return jax.shard_map(
        functools.partial(on_device, dict(mesh.shape)),
        mesh=mesh,
        in_specs=placed,
        out_specs=P(("grp", "fs"), None, "tp"),
        check_vma=False,
    )
```
